256 devices in a mesh: st: 64 (over z, y, core), tp: 4 (over x).
Axes of the slice: x: 4, y: 4, z: 8, core: 2. Of those that a mesh axis runs over, the one named last changes fastest.
Arguments:
- tokens: bfloat16 [65536, 2048], P('st', 'tp'), may hold values from -6 to 6
- token_gain: float32 [2048], replicated, may hold values from 0.1 to 1.9
- inner_weight: bfloat16 [2048, 2048], P(None, 'tp'), may hold values from -0.125 to 0.125
- gating_weight: bfloat16 [2048, 2048], P(None, 'tp'), may hold values from -0.125 to 0.125
- filter_taps: float32 [31, 2048], P(None, 'tp'), may hold values from -2.4 to 2.4
- channel_gain: float32 [2048], P('tp'), may hold values from 0.1 to 1.9
- retrieval_gate: float32 [2048], P('tp'), may hold values from -2 to 2
- passage_store: bfloat16 [1024, 64, 2048], P('st'), may hold values from -6 to 6
- passage_gain: float32 [2048], replicated, may hold values from 0.1 to 1.9
- keys_weight: bfloat16 [2048, 1024], P(None, 'tp'), may hold values from -0.125 to 0.125
- values_weight: bfloat16 [2048, 1024], P(None, 'tp'), may hold values from -0.125 to 0.125
- owners: int32 [1024, 2], P('st'), may hold values from 0 to 63, all different within a row; in each aligned block of 16 rows (0 to 15, 16 to 31, ...) no two rows name the same one
- local_slots: int32 [1024, 2], P('st'), may hold values from 0 to 15
Outputs:
- mixed: bfloat16 [65536, 2048], P('st', 'tp')
The draws below stay inside these ranges and needn't reach their ends.
Inputs may be any that keep to these rules, and one draw needn't show every extreme that they name: In the rows of one index of st no owner is named by more than 1 row, a bound that some block reaches; a row names 2 different owners, and every owner is named somewhere.
All inputs are finite; a program needn't handle non-finite values.
Results may differ from the reference program's by a relative error of at most 0.0059.
Values may be sent and summed in bfloat16 or wider, within the bound.
No kernel may reach another device: no remote copies, remote signals or barrier semaphores. Data moves between devices by JAX's collectives and lax.ppermute only.
A program may use at most 128 MiB of HBM per device.

```python
import math
import jax
import jax.numpy as jnp
import numpy as np
from jax import lax

D = 2048
HEAD = 256
Q_HEADS = 8
KV_HEADS = 4
CONV = 31
LENGTH = 512
BLOCK = 64
PB = 2
PROWS = 64
PASS_DEV = 16
BLOCKS_DEV = 16
CAP = 1
TOKENS = 65536
BLOCKS = 1024
PASSAGES = 1024
N_ST = 64


def draw_filter_taps(key, part):
    first, second = jax.random.split(jax.random.fold_in(key, 11))
    base = jnp.clip(jax.random.normal(first, (CONV, D), jnp.float32), -4.0, 4.0) / math.sqrt(CONV)
    levels = jax.random.uniform(second, (D // HEAD,), jnp.float32, -1.2, 1.2)
    spread = jnp.repeat(jnp.exp(levels), HEAD)
    return base * spread[None, :]


def place_ends(result, rng, least, largest):
    place = [jax.random.randint(jax.random.fold_in(rng, axis), (), 0, length) for axis, length in enumerate(result.shape)]
    main_axis = result.shape.index(max(result.shape))
    beside = place[:main_axis] + [(place[main_axis] + 1) % result.shape[main_axis]] + place[main_axis + 1:]
    return result.at[tuple(place)].set(least).at[tuple(beside)].set(largest)


def steps_of(stream_key, shape, shards, least, high):
    loudness = 1.0
    for position, shards_of in shards:
        steps = jax.random.uniform(jax.random.fold_in(jax.random.fold_in(stream_key, 6), position), (shards_of,), jnp.float32, least / len(shards), high / len(shards))
        loudness = loudness * jnp.repeat(jnp.exp(steps), shape[position] // shards_of).reshape((-1,) + (1,) * (len(shape) - 1 - position))
    return loudness


def routed_block(key, own, number, rows, amount, top, reach, skew):
    sequence = jax.random.permutation(key, amount)
    heavy_load, common = load_shares(amount, rows * top, reach, skew, True), load_shares(amount, rows * top, reach, skew, False)
    places = jnp.arange(amount)

    def named(lengths, turn):
        used = int((lengths > 0).sum())
        fixed = max(1, used // 4)
        passed = fixed + (places - fixed + turn * (used - fixed)) % max(1, amount - fixed)
        return jnp.zeros((amount,), jnp.int32).at[sequence[jnp.where(places < fixed, places, passed)]].set(jnp.asarray(lengths, jnp.int32))

    lengths = jnp.where(number % 4 == 0, named(heavy_load, number // 4), named(common, number - number // 4 - 1))
    mixed = jax.random.permutation(jax.random.fold_in(own, 3), amount)
    giver, sink = mixed[0:amount // 2 * 2:2], mixed[1:amount // 2 * 2:2]
    slack = jnp.minimum(lengths[giver] - 1, reach - lengths[sink]) // 2
    slack = jnp.where((giver == sequence[0]) | (sink == sequence[0]) | (lengths[sink] == 0), 0, jnp.maximum(slack, 0))
    passed = jax.random.randint(jax.random.fold_in(own, 4), (amount // 2,), 0, 1 << 20) % (slack + 1)
    lengths = lengths.at[giver].add(-passed).at[sink].add(passed)
    labels = jnp.searchsorted(jnp.cumsum(lengths), jnp.arange(rows * top), side="right").astype(jnp.int32)
    grid = labels.reshape(top, rows).T
    grid = grid[jax.random.permutation(jax.random.fold_in(own, 1), rows)]
    turn = jax.random.randint(jax.random.fold_in(own, 2), (rows, 1), 0, top)
    return jnp.take_along_axis(grid, (jnp.arange(top)[None, :] + turn) % top, axis=1)


def load_shares(amount, total, bound, skew, full):
    portions = [(1 << 20) // math.isqrt(standing ** skew) + 1 for standing in range(1, amount + 1)]
    largest = bound if full else min(bound, max(-(-total // amount), total * portions[0] // sum(portions)))
    least = 1 if total - largest >= amount - 1 else 0
    holding, surplus = [largest] + [least] * (amount - 1), total - largest - least * (amount - 1)
    while surplus > 0:
        candidates = [i for i in range(1, amount) if holding[i] < largest] or [i for i in range(1, amount) if holding[i] < bound]
        mass, remaining = sum([portions[i] for i in candidates]), surplus
        for i in candidates:
            extra = min(bound - holding[i], max(1, remaining * portions[i] // mass), surplus)
            holding[i] = holding[i] + extra
            surplus = surplus - extra
    return np.array(holding)


def centred(own_key, extent, width, limit, cuts=(), held_as=jnp.bfloat16):
    values = width * jax.random.normal(own_key, extent, jnp.float32)
    if cuts:
        values = values * steps_of(own_key, extent, cuts, -0.22, 0.18)
    return jnp.clip(values, -limit, limit).astype(held_as)


def setup_inputs(seed: int = 0) -> dict:
    arg_keys = jax.random.split(jax.random.key(seed), 14)
    tokens = centred(arg_keys[0], (TOKENS, D), 1.0, 6.0, ((0, 64), (1, 4)))
    token_gain = jnp.clip(1.0 + 0.18 * jax.random.normal(arg_keys[1], (D,), jnp.float32), 0.1, 1.9)
    inner_weight = centred(arg_keys[2], (D, D), D ** -0.5, 0.125, ((1, 4),))
    gating_weight = centred(arg_keys[3], (D, D), D ** -0.5, 0.125, ((1, 4),))
    filter_taps = draw_filter_taps(jax.random.fold_in(arg_keys[13], 71), 0)
    channel_gain = jnp.clip(1.0 + 0.18 * jax.random.normal(arg_keys[5], (D,), jnp.float32), 0.1, 1.9)
    retrieval_gate = jnp.clip(jax.random.uniform(arg_keys[6], (D,), jnp.float32, -2.0, 2.0) * steps_of(arg_keys[6], (D,), ((0, 4),), -0.4, 0.0), -2.0, 2.0)
    passage_store = centred(arg_keys[7], (PASSAGES, PROWS, D), 1.0, 6.0, ((0, 64),))
    passage_gain = jnp.clip(1.0 + 0.18 * jax.random.normal(arg_keys[8], (D,), jnp.float32), 0.1, 1.9)
    keys_weight = centred(arg_keys[9], (D, KV_HEADS * HEAD), D ** -0.5, 0.125, ((1, 4),))
    values_weight = centred(arg_keys[10], (D, KV_HEADS * HEAD), D ** -0.5, 0.125, ((1, 4),))
    owners_keys = jax.random.split(jax.random.fold_in(arg_keys[11], 1), BLOCKS // BLOCKS_DEV)
    owners_turns = jax.random.permutation(jax.random.fold_in(arg_keys[11], 3), BLOCKS // BLOCKS_DEV)
    owners = jax.vmap(lambda own, number: routed_block(jax.random.fold_in(arg_keys[11], 2), own, number, BLOCKS_DEV, N_ST, PB, CAP, 2))(owners_keys, owners_turns).reshape((BLOCKS, PB))
    local_slots = place_ends(jax.random.randint(arg_keys[12], (BLOCKS, PB), 0, PASS_DEV), jax.random.fold_in(arg_keys[12], 1), 0, PASS_DEV - 1).astype(jnp.int32)
    return {"tokens": tokens, "token_gain": token_gain, "inner_weight": inner_weight, "gating_weight": gating_weight, "filter_taps": filter_taps, "channel_gain": channel_gain, "retrieval_gate": retrieval_gate, "passage_store": passage_store, "passage_gain": passage_gain, "keys_weight": keys_weight, "values_weight": values_weight, "owners": owners, "local_slots": local_slots}


EPSILON = 1e-06
EPSILON_NORM = 1e-05

def project_passages(rows, passage_gain, keys_weight, values_weight):
    flat_rows = rows.reshape(-1, rows.shape[-1]).astype(jnp.float32)
    inverse = lax.rsqrt(lax.optimization_barrier(jnp.mean(flat_rows * flat_rows, axis=1, keepdims=True)) + EPSILON)
    normed = (flat_rows * inverse * passage_gain).astype(jnp.bfloat16)
    key_rows = jnp.dot(normed, keys_weight, preferred_element_type=jnp.float32).astype(jnp.bfloat16)
    value_rows = jnp.dot(normed, values_weight, preferred_element_type=jnp.float32).astype(jnp.bfloat16)
    return (key_rows, value_rows)

def reference(tokens, token_gain, inner_weight, gating_weight, filter_taps, channel_gain, retrieval_gate, passage_store, passage_gain, keys_weight, values_weight, owners, local_slots):
    wide_tokens = tokens.astype(jnp.float32)
    inverse = lax.rsqrt(lax.optimization_barrier(jnp.mean(wide_tokens * wide_tokens, axis=1, keepdims=True)) + EPSILON)
    scaled = (wide_tokens * token_gain).astype(jnp.bfloat16)
    inner_proj = jnp.dot(scaled, inner_weight, preferred_element_type=jnp.float32) * inverse
    gating = jnp.dot(scaled, gating_weight, preferred_element_type=jnp.float32) * inverse
    gated = (inner_proj * jax.nn.sigmoid(gating)).astype(jnp.bfloat16)
    sequences = gated.reshape(-1, LENGTH, D)
    padded = jnp.pad(sequences, ((0, 0), (CONV - 1, 0), (0, 0)))
    convolved = jnp.zeros(sequences.shape, jnp.float32)
    for offset in range(CONV):
        convolved = convolved + padded[:, offset:offset + LENGTH].astype(jnp.float32) * filter_taps[offset]
    convolved = convolved.reshape(-1, D)
    average = lax.optimization_barrier(jnp.mean(convolved, axis=1, keepdims=True))
    variance = lax.optimization_barrier(jnp.mean(convolved * convolved, axis=1, keepdims=True)) - average * average
    conv_out = jax.nn.silu((convolved - average) * lax.rsqrt(variance + EPSILON_NORM) * channel_gain)
    queries = conv_out.astype(jnp.bfloat16)
    key_rows, value_rows = project_passages(passage_store, passage_gain, keys_weight, values_weight)
    key_rows = key_rows.reshape(PASSAGES, PROWS, KV_HEADS, HEAD)
    value_rows = value_rows.reshape(PASSAGES, PROWS, KV_HEADS, HEAD)
    passage_ids = (owners * PASS_DEV + local_slots).reshape(-1).astype(jnp.int32)
    block_keys = key_rows[passage_ids].reshape(BLOCKS, PB * PROWS, KV_HEADS, HEAD)
    block_values = value_rows[passage_ids].reshape(BLOCKS, PB * PROWS, KV_HEADS, HEAD)
    query_blocks = queries.reshape(BLOCKS, BLOCK, KV_HEADS, Q_HEADS // KV_HEADS, HEAD)
    scores = jnp.einsum('btkgd,bskd->bkgts', query_blocks.astype(jnp.float32), block_keys.astype(jnp.float32)) / math.sqrt(HEAD)
    attention_weights = jax.nn.softmax(scores, axis=-1).astype(jnp.bfloat16)
    attended = jnp.einsum('bkgts,bskd->btkgd', attention_weights.astype(jnp.float32), block_values.astype(jnp.float32)).reshape(-1, D)
    return (conv_out + jax.nn.sigmoid(retrieval_gate) * attended).astype(jnp.bfloat16)
```

```python
import math

import jax
import jax.numpy as jnp
from jax import lax
from jax.experimental import pallas as pl
from jax.experimental.pallas import tpu as pltpu
from jax.sharding import Mesh
from jax.sharding import PartitionSpec as P

D = 2048
HEAD = 256
CONV = 31
LENGTH = 512
BLOCK = 64
PB = 2
PROWS = 64
EPSILON = 1e-06
EPSILON_NORM = 1e-05
ST = ("z", "y", "c")
LEAD = 32
ROWS_CHUNK = 64


def ring(size, step):
    return [(i, (i + step) % size) for i in range(size)]


def whole(shape):
    return pl.BlockSpec(shape, lambda *_: (0,) * len(shape))


def project_kernel(rows_ref, gain_ref, keys_ref, values_ref, out_ref):
    rows = rows_ref[...].astype(jnp.float32)
    inverse = lax.rsqrt(jnp.mean(rows * rows, axis=1, keepdims=True) + EPSILON)
    normed = (rows * inverse * gain_ref[...]).astype(jnp.bfloat16)
    out_ref[:, :HEAD] = jnp.dot(normed, keys_ref[...], preferred_element_type=jnp.float32).astype(
        jnp.bfloat16
    )
    out_ref[:, HEAD:] = jnp.dot(
        normed, values_ref[...], preferred_element_type=jnp.float32
    ).astype(jnp.bfloat16)


def project_passages(store, gain, keys_weight, values_weight):
    rows = store.reshape(-1, D)
    count = rows.shape[0]
    tile = 256
    return pl.pallas_call(
        project_kernel,
        grid=(count // tile,),
        in_specs=[
            pl.BlockSpec((tile, D), lambda i: (i, 0)),
            whole((1, D)),
            whole((D, HEAD)),
            whole((D, HEAD)),
        ],
        out_specs=pl.BlockSpec((tile, 2 * HEAD), lambda i: (i, 0)),
        out_shape=jax.ShapeDtypeStruct((count, 2 * HEAD), jnp.bfloat16),
        cost_estimate=pl.CostEstimate(
            flops=4 * count * D * HEAD, transcendentals=0, bytes_accessed=7 << 20
        ),
        name="project_passages",
    )(rows, gain.reshape(1, D), keys_weight, values_weight)


def token_kernel(
    me_ref,
    own_ref,
    left_ref,
    right_ref,
    far0_ref,
    far1_ref,
    gain_ref,
    inner_ref,
    gating_ref,
    taps_ref,
    out_ref,
    stats_ref,
    padded_ref,
):
    me = me_ref[0]
    first = pl.program_id(0) == 0
    width = own_ref.shape[1]
    squares = jnp.zeros((LENGTH, 1), jnp.float32)
    inner = jnp.zeros((LENGTH, width), jnp.float32)
    gating = jnp.zeros((LENGTH, width), jnp.float32)
    for offset in range(4):
        at = lax.rem(me + offset, 4)
        if offset == 0:
            piece = own_ref[...].astype(jnp.float32)
        elif offset == 1:
            piece = right_ref[...].astype(jnp.float32)
        elif offset == 3:
            piece = left_ref[...].astype(jnp.float32)
        else:
            piece = jnp.where(
                first, far0_ref[...].astype(jnp.float32), far1_ref[...].astype(jnp.float32)
            )
        squares = squares + jnp.sum(piece * piece, axis=1, keepdims=True)
        scaled = (piece * gain_ref[at]).astype(jnp.bfloat16)
        inner = inner + jnp.dot(scaled, inner_ref[at], preferred_element_type=jnp.float32)
        gating = gating + jnp.dot(scaled, gating_ref[at], preferred_element_type=jnp.float32)
    inverse = lax.rsqrt(squares / D + EPSILON)
    gated = (inner * inverse * jax.nn.sigmoid(gating * inverse)).astype(jnp.bfloat16)
    padded_ref[:LEAD, :] = jnp.zeros((LEAD, width), jnp.float32)
    padded_ref[LEAD:, :] = gated.astype(jnp.float32)
    shift = LEAD - CONV + 1

    def step(n):
        base = n * ROWS_CHUNK
        sums = jnp.zeros((ROWS_CHUNK, 128), jnp.float32)
        square_sums = jnp.zeros((ROWS_CHUNK, 128), jnp.float32)
        for lane in range(0, width, 128):
            total = jnp.zeros((ROWS_CHUNK, 128), jnp.float32)
            for s in range(8):
                part = None
                for j in range(LEAD // 8 + 1):
                    tap = 8 * j + s - shift
                    if tap < 0 or tap >= CONV:
                        continue
                    height = ROWS_CHUNK + (8 if s else 0)
                    term = (
                        padded_ref[pl.ds(base + 8 * j, height), lane : lane + 128]
                        * taps_ref[tap : tap + 1, lane : lane + 128]
                    )
                    part = term if part is None else part + term
                total = total + part[s : s + ROWS_CHUNK]
            out_ref[pl.ds(base, ROWS_CHUNK), lane : lane + 128] = total
            sums = sums + total
            square_sums = square_sums + total * total
        return sums, square_sums

    for n in range(LENGTH // 128):
        pair = [step(2 * n + h) for h in range(2)]
        sums = jnp.concatenate([pair[0][0], pair[1][0]], axis=0)
        square_sums = jnp.concatenate([pair[0][1], pair[1][1]], axis=0)
        stats_ref[0, n : n + 1, :] = jnp.sum(sums.T, axis=0, keepdims=True)
        stats_ref[1, n : n + 1, :] = jnp.sum(square_sums.T, axis=0, keepdims=True)


def token_path(me, own, left, right, far0, far1, gain, inner_weight, gating_weight, taps):
    rows, width = own.shape
    grid_spec = pltpu.PrefetchScalarGridSpec(
        num_scalar_prefetch=1,
        grid=(rows // LENGTH,),
        in_specs=[pl.BlockSpec((LENGTH, width), lambda i, m: (i, 0))] * 3
        + [
            whole((LENGTH, width)),
            whole((LENGTH, width)),
            whole((4, 1, width)),
            whole((4, width, width)),
            whole((4, width, width)),
            whole((CONV, width)),
        ],
        out_specs=[
            pl.BlockSpec((LENGTH, width), lambda i, m: (i, 0)),
            pl.BlockSpec((None, 2, LENGTH // 128, 128), lambda i, m: (i, 0, 0, 0)),
        ],
        scratch_shapes=[pltpu.VMEM((LEAD + LENGTH, width), jnp.float32)],
    )
    return pl.pallas_call(
        token_kernel,
        grid_spec=grid_spec,
        out_shape=[
            jax.ShapeDtypeStruct((rows, width), jnp.float32),
            jax.ShapeDtypeStruct((rows // LENGTH, 2, LENGTH // 128, 128), jnp.float32),
        ],
        cost_estimate=pl.CostEstimate(
            flops=4 * rows * D * width, transcendentals=rows * width, bytes_accessed=10 << 20
        ),
        name="token_path",
    )(
        me,
        own,
        left,
        right,
        far0,
        far1,
        gain.reshape(4, 1, width),
        inner_weight.reshape(4, width, width),
        gating_weight.reshape(4, width, width),
        taps,
    )


def attend_kernel(
    where_ref, conv_ref, stats_ref, gain_ref, gate_ref, arrived_ref, out_ref, held_ref, sems
):
    turn = pl.program_id(0)
    count = where_ref.shape[0]

    @pl.when(turn == 0)
    def _():
        for n in range(count):
            pltpu.make_async_copy(
                arrived_ref.at[where_ref[n]], held_ref.at[n], sems.at[n]
            ).start()

    width = conv_ref.shape[1]
    average = stats_ref[0, pl.ds(turn, 1), :] / D
    variance = stats_ref[1, pl.ds(turn, 1), :] / D - average * average
    spread = lax.rsqrt(variance + EPSILON_NORM)
    average = jnp.broadcast_to(average, (128, 128)).T
    spread = jnp.broadcast_to(spread, (128, 128)).T
    pieces = []
    for lane in range(0, width, 128):
        scaled = (
            (conv_ref[:, lane : lane + 128] - average) * spread * gain_ref[:, lane : lane + 128]
        )
        pieces.append(scaled * jax.nn.sigmoid(scaled))
    conv_out = jnp.concatenate(pieces, axis=1)
    queries = conv_out.astype(jnp.bfloat16)
    weight = jax.nn.sigmoid(gate_ref[...])
    for b in range(2):
        keys, values = [], []
        for p in range(PB):
            n = (turn * 2 + b) * PB + p
            pltpu.make_async_copy(arrived_ref.at[0], held_ref.at[n], sems.at[n]).wait()
            keys.append(held_ref[n, :, :HEAD])
            values.append(held_ref[n, :, HEAD:])
        keys = jnp.concatenate(keys, axis=0)
        values = jnp.concatenate(values, axis=0)
        rows = slice(b * BLOCK, (b + 1) * BLOCK)
        heads = jnp.concatenate([queries[rows, :HEAD], queries[rows, HEAD:]], axis=0)
        scores = lax.dot_general(
            heads, keys, (((1,), (1,)), ((), ())), preferred_element_type=jnp.float32
        ) / math.sqrt(HEAD)
        raised = jnp.exp(scores - jnp.max(scores, axis=1, keepdims=True))
        shares = (raised / jnp.sum(raised, axis=1, keepdims=True)).astype(jnp.bfloat16)
        attended = jnp.dot(shares, values, preferred_element_type=jnp.float32)
        attended = jnp.concatenate([attended[:BLOCK], attended[BLOCK:]], axis=1)
        out_ref[rows, :] = (conv_out[rows] + weight * attended).astype(jnp.bfloat16)


def attend(where, convolved, stats, channel_gain, retrieval_gate, arrived):
    rows, width = convolved.shape
    count = where.shape[0]
    grid_spec = pltpu.PrefetchScalarGridSpec(
        num_scalar_prefetch=1,
        grid=(rows // 128,),
        in_specs=[
            pl.BlockSpec((128, width), lambda i, w: (i, 0)),
            whole((2, rows // 128, 128)),
            whole((1, width)),
            whole((1, width)),
            pl.BlockSpec(memory_space=pl.ANY),
        ],
        out_specs=pl.BlockSpec((128, width), lambda i, w: (i, 0)),
        scratch_shapes=[
            pltpu.VMEM((count, PROWS, 2 * HEAD), jnp.bfloat16),
            pltpu.SemaphoreType.DMA((count,)),
        ],
    )
    return pl.pallas_call(
        attend_kernel,
        grid_spec=grid_spec,
        out_shape=jax.ShapeDtypeStruct((rows, width), jnp.bfloat16),
        cost_estimate=pl.CostEstimate(
            flops=4 * rows * 2 * PB * PROWS * HEAD,
            transcendentals=2 * rows * width,
            bytes_accessed=5 << 20,
        ),
        name="attend",
    )(
        where,
        convolved,
        stats,
        channel_gain.reshape(1, width),
        retrieval_gate.reshape(1, width),
        arrived,
    )


def body(
    tokens,
    token_gain,
    inner_weight,
    gating_weight,
    filter_taps,
    channel_gain,
    retrieval_gate,
    passage_store,
    passage_gain,
    keys_weight,
    values_weight,
    owners,
    local_slots,
):
    st = lax.axis_size(ST)
    me = lax.axis_index("tp").astype(jnp.int32).reshape(1)
    left = lax.ppermute(tokens, "tp", ring(4, 1))
    right = lax.ppermute(tokens, "tp", ring(4, -1))
    far0 = lax.ppermute(left[:LENGTH], "tp", ring(4, 1))
    far1 = lax.ppermute(right[LENGTH:], "tp", ring(4, -1))

    asked = owners.reshape(-1)
    slots = local_slots.reshape(-1)
    wanted = jnp.sum(
        jnp.where(asked[:, None] == jnp.arange(st, dtype=jnp.int32)[None, :], slots[:, None], 0),
        axis=0,
    )
    sent = lax.all_to_all(wanted[:, None], ST, split_axis=0, concat_axis=0, tiled=True)
    own = project_passages(passage_store, passage_gain, keys_weight, values_weight)
    own = own.reshape(-1, PROWS, 2 * HEAD)
    arrived = lax.all_to_all(own[sent[:, 0]], ST, split_axis=0, concat_axis=0, tiled=True)

    convolved, stats = token_path(
        me, tokens, left, right, far0, far1, token_gain, inner_weight, gating_weight, filter_taps
    )
    stats = lax.psum(stats, "tp")
    stats = stats.transpose(1, 0, 2, 3).reshape(2, -1, 128)
    return attend(asked, convolved, stats, channel_gain, retrieval_gate, arrived)


def solution(mesh):
    st, tp = mesh.devices.shape
    fine = Mesh(mesh.devices.reshape(st // 8, 4, 2, tp), ST + ("tp",))
    placed = (
        P(ST, "tp"),
        P(),
        P(None, "tp"),
        P(None, "tp"),
        P(None, "tp"),
        P("tp"),
        P("tp"),
        P(ST, None, None),
        P(),
        P(None, "tp"),
        P(None, "tp"),
        P(ST, None),
        P(ST, None),
    )
    return jax.shard_map(
        body, mesh=fine, in_specs=placed, out_specs=P(ST, "tp"), check_vma=False
    )
```

```python
import math

import jax
import jax.numpy as jnp
from jax import lax
from jax.experimental import pallas as pl
from jax.experimental.pallas import tpu as pltpu
from jax.sharding import Mesh
from jax.sharding import PartitionSpec as P

D = 2048
HEAD = 256
CONV = 31
LENGTH = 512
BLOCK = 64
PB = 2
PROWS = 64
EPSILON = 1e-06
EPSILON_NORM = 1e-05
ST = ("z", "y", "c")
LEAD = 32
ROWS_CHUNK = 64
GROUPS = ((0, -1, 1), (-2, 2), (-3, 3), (4,))


def ring(size, step):
    return [(i, (i + step) % size) for i in range(size)]


def whole(shape):
    return pl.BlockSpec(shape, lambda *_: (0,) * len(shape))


def project_kernel(rows_ref, gain_ref, keys_ref, values_ref, out_ref):
    rows = rows_ref[...].astype(jnp.float32)
    inverse = lax.rsqrt(jnp.mean(rows * rows, axis=1, keepdims=True) + EPSILON)
    normed = (rows * inverse * gain_ref[...]).astype(jnp.bfloat16)
    out_ref[:, :HEAD] = jnp.dot(normed, keys_ref[...], preferred_element_type=jnp.float32).astype(
        jnp.bfloat16
    )
    out_ref[:, HEAD:] = jnp.dot(
        normed, values_ref[...], preferred_element_type=jnp.float32
    ).astype(jnp.bfloat16)


def project_passages(store, gain, keys_weight, values_weight):
    rows = store.reshape(-1, D)
    count = rows.shape[0]
    tile = 256
    return pl.pallas_call(
        project_kernel,
        grid=(count // tile,),
        in_specs=[
            pl.BlockSpec((tile, D), lambda i: (i, 0)),
            whole((1, D)),
            whole((D, HEAD)),
            whole((D, HEAD)),
        ],
        out_specs=pl.BlockSpec((tile, 2 * HEAD), lambda i: (i, 0)),
        out_shape=jax.ShapeDtypeStruct((count, 2 * HEAD), jnp.bfloat16),
        cost_estimate=pl.CostEstimate(
            flops=4 * count * D * HEAD, transcendentals=0, bytes_accessed=7 << 20
        ),
        name="project_passages",
    )(rows, gain.reshape(1, D), keys_weight, values_weight)


def token_kernel(
    me_ref,
    own_ref,
    left_ref,
    right_ref,
    far0_ref,
    far1_ref,
    gain_ref,
    inner_ref,
    gating_ref,
    taps_ref,
    out_ref,
    stats_ref,
    padded_ref,
):
    me = me_ref[0]
    first = pl.program_id(0) == 0
    width = own_ref.shape[1]
    squares = jnp.zeros((LENGTH, 1), jnp.float32)
    inner = jnp.zeros((LENGTH, width), jnp.float32)
    gating = jnp.zeros((LENGTH, width), jnp.float32)
    for offset in range(4):
        at = lax.rem(me + offset, 4)
        if offset == 0:
            piece = own_ref[...].astype(jnp.float32)
        elif offset == 1:
            piece = right_ref[...].astype(jnp.float32)
        elif offset == 3:
            piece = left_ref[...].astype(jnp.float32)
        else:
            piece = jnp.where(
                first, far0_ref[...].astype(jnp.float32), far1_ref[...].astype(jnp.float32)
            )
        squares = squares + jnp.sum(piece * piece, axis=1, keepdims=True)
        scaled = (piece * gain_ref[at]).astype(jnp.bfloat16)
        inner = inner + jnp.dot(scaled, inner_ref[at], preferred_element_type=jnp.float32)
        gating = gating + jnp.dot(scaled, gating_ref[at], preferred_element_type=jnp.float32)
    inverse = lax.rsqrt(squares / D + EPSILON)
    gated = (inner * inverse * jax.nn.sigmoid(gating * inverse)).astype(jnp.bfloat16)
    padded_ref[:LEAD, :] = jnp.zeros((LEAD, width), jnp.float32)
    padded_ref[LEAD:, :] = gated.astype(jnp.float32)
    shift = LEAD - CONV + 1

    def step(n):
        base = n * ROWS_CHUNK
        sums = jnp.zeros((ROWS_CHUNK, 128), jnp.float32)
        square_sums = jnp.zeros((ROWS_CHUNK, 128), jnp.float32)
        for lane in range(0, width, 128):
            total = jnp.zeros((ROWS_CHUNK, 128), jnp.float32)
            for s in range(8):
                part = None
                for j in range(LEAD // 8 + 1):
                    tap = 8 * j + s - shift
                    if tap < 0 or tap >= CONV:
                        continue
                    height = ROWS_CHUNK + (8 if s else 0)
                    term = (
                        padded_ref[pl.ds(base + 8 * j, height), lane : lane + 128]
                        * taps_ref[tap : tap + 1, lane : lane + 128]
                    )
                    part = term if part is None else part + term
                total = total + part[s : s + ROWS_CHUNK]
            out_ref[pl.ds(base, ROWS_CHUNK), lane : lane + 128] = total
            sums = sums + total
            square_sums = square_sums + total * total
        return sums, square_sums

    for n in range(LENGTH // 128):
        pair = [step(2 * n + h) for h in range(2)]
        sums = jnp.concatenate([pair[0][0], pair[1][0]], axis=0)
        square_sums = jnp.concatenate([pair[0][1], pair[1][1]], axis=0)
        stats_ref[0, n : n + 1, :] = jnp.sum(sums.T, axis=0, keepdims=True)
        stats_ref[1, n : n + 1, :] = jnp.sum(square_sums.T, axis=0, keepdims=True)


def token_path(me, own, left, right, far0, far1, gain, inner_weight, gating_weight, taps):
    rows, width = own.shape
    grid_spec = pltpu.PrefetchScalarGridSpec(
        num_scalar_prefetch=1,
        grid=(rows // LENGTH,),
        in_specs=[pl.BlockSpec((LENGTH, width), lambda i, m: (i, 0))] * 3
        + [
            whole((LENGTH, width)),
            whole((LENGTH, width)),
            whole((4, 1, width)),
            whole((4, width, width)),
            whole((4, width, width)),
            whole((CONV, width)),
        ],
        out_specs=[
            pl.BlockSpec((LENGTH, width), lambda i, m: (i, 0)),
            pl.BlockSpec((None, 2, LENGTH // 128, 128), lambda i, m: (i, 0, 0, 0)),
        ],
        scratch_shapes=[pltpu.VMEM((LEAD + LENGTH, width), jnp.float32)],
    )
    return pl.pallas_call(
        token_kernel,
        grid_spec=grid_spec,
        out_shape=[
            jax.ShapeDtypeStruct((rows, width), jnp.float32),
            jax.ShapeDtypeStruct((rows // LENGTH, 2, LENGTH // 128, 128), jnp.float32),
        ],
        cost_estimate=pl.CostEstimate(
            flops=4 * rows * D * width, transcendentals=rows * width, bytes_accessed=10 << 20
        ),
        name="token_path",
    )(
        me,
        own,
        left,
        right,
        far0,
        far1,
        gain.reshape(4, 1, width),
        inner_weight.reshape(4, width, width),
        gating_weight.reshape(4, width, width),
        taps,
    )


def finish_kernel(conv_ref, stats_ref, gain_ref, out_ref):
    width = conv_ref.shape[1]
    turn = pl.program_id(0)
    for n in range(conv_ref.shape[0] // 128):
        at = turn * (conv_ref.shape[0] // 128) + n
        rows = slice(n * 128, (n + 1) * 128)
        average = stats_ref[0, pl.ds(at, 1), :] / D
        variance = stats_ref[1, pl.ds(at, 1), :] / D - average * average
        spread = lax.rsqrt(variance + EPSILON_NORM)
        average = jnp.broadcast_to(average, (128, 128)).T
        spread = jnp.broadcast_to(spread, (128, 128)).T
        for lane in range(0, width, 128):
            part = slice(lane, lane + 128)
            scaled = (conv_ref[rows, part] - average) * spread * gain_ref[:, part]
            out_ref[rows, part] = scaled * jax.nn.sigmoid(scaled)


def finish(convolved, stats, channel_gain):
    rows, width = convolved.shape
    tile = 512
    return pl.pallas_call(
        finish_kernel,
        grid=(rows // tile,),
        in_specs=[
            pl.BlockSpec((tile, width), lambda i: (i, 0)),
            whole((2, rows // 128, 128)),
            whole((1, width)),
        ],
        out_specs=pl.BlockSpec((tile, width), lambda i: (i, 0)),
        out_shape=jax.ShapeDtypeStruct((rows, width), jnp.float32),
        cost_estimate=pl.CostEstimate(
            flops=8 * rows * width, transcendentals=rows * width, bytes_accessed=4 << 20
        ),
        name="finish",
    )(convolved, stats, channel_gain.reshape(1, width))


def attend_kernel(plane_ref, where_ref, conv_ref, gate_ref, *refs):
    groups, (out_ref, held_ref, sems) = refs[:4], refs[4:]
    turn = pl.program_id(0)
    count = where_ref.shape[0]
    here = plane_ref[0]

    @pl.when(turn == 0)
    def _():
        for n in range(count):
            owner = where_ref[n]
            away = lax.rem(owner // 8 - here + 8, 8)
            column = lax.rem(owner, 8)
            for group, steps in enumerate(GROUPS):
                for k, distance in enumerate(steps):

                    @pl.when(away == distance % 8)
                    def _():
                        pltpu.make_async_copy(
                            groups[group].at[column * len(steps) + k], held_ref.at[n], sems.at[n]
                        ).start()

    blocks = conv_ref.shape[0] // BLOCK
    weight = jax.nn.sigmoid(gate_ref[...])
    queries = conv_ref[...].astype(jnp.bfloat16)
    for n in range(blocks * PB):
        at = turn * blocks * PB + n
        pltpu.make_async_copy(groups[0].at[0], held_ref.at[at], sems.at[at]).wait()
    scores = []
    for b in range(blocks):
        held = held_ref[pl.ds((turn * blocks + b) * PB, PB)].reshape(PB * PROWS, 2 * HEAD)
        rows = slice(b * BLOCK, (b + 1) * BLOCK)
        heads = jnp.concatenate([queries[rows, :HEAD], queries[rows, HEAD:]], axis=0)
        scores.append(
            lax.dot_general(
                heads,
                held[:, :HEAD],
                (((1,), (1,)), ((), ())),
                preferred_element_type=jnp.float32,
            )
            / math.sqrt(HEAD)
        )
    shares = []
    for b in range(blocks):
        raised = jnp.exp(scores[b] - jnp.max(scores[b], axis=1, keepdims=True))
        shares.append((raised / jnp.sum(raised, axis=1, keepdims=True)).astype(jnp.bfloat16))
    for b in range(blocks):
        held = held_ref[pl.ds((turn * blocks + b) * PB, PB)].reshape(PB * PROWS, 2 * HEAD)
        attended = jnp.dot(shares[b], held[:, HEAD:], preferred_element_type=jnp.float32)
        attended = jnp.concatenate([attended[:BLOCK], attended[BLOCK:]], axis=1)
        rows = slice(b * BLOCK, (b + 1) * BLOCK)
        out_ref[rows, :] = (conv_ref[rows, :] + weight * attended).astype(jnp.bfloat16)


def attend(plane, where, conv_out, retrieval_gate, groups):
    rows, width = conv_out.shape
    count = where.shape[0]
    tile = 512
    grid_spec = pltpu.PrefetchScalarGridSpec(
        num_scalar_prefetch=2,
        grid=(rows // tile,),
        in_specs=[
            pl.BlockSpec((tile, width), lambda i, *_: (i, 0)),
            whole((1, width)),
        ]
        + [pl.BlockSpec(memory_space=pl.ANY)] * len(groups),
        out_specs=pl.BlockSpec((tile, width), lambda i, *_: (i, 0)),
        scratch_shapes=[
            pltpu.VMEM((count, PROWS, 2 * HEAD), jnp.bfloat16),
            pltpu.SemaphoreType.DMA((count,)),
        ],
    )
    return pl.pallas_call(
        attend_kernel,
        grid_spec=grid_spec,
        out_shape=jax.ShapeDtypeStruct((rows, width), jnp.bfloat16),
        cost_estimate=pl.CostEstimate(
            flops=4 * rows * 2 * PB * PROWS * HEAD,
            transcendentals=rows * 2 * PB * PROWS,
            bytes_accessed=5 << 20,
        ),
        name="attend",
    )(plane, where, conv_out, retrieval_gate.reshape(1, width), *groups)


def pick_kernel(plane_ref, table_ref, own_ref, below_ref, above_ref, *refs):
    outs, sems = refs[:-1], refs[-1]
    here = plane_ref[0]

    def slot(reader_plane, reader, owner_plane):
        at = lax.rem(here + reader_plane + 8, 8) * 8 + reader
        return table_ref[at * 8 + lax.rem(here + owner_plane + 8, 8)]

    half = PROWS // 2
    for reader in range(8):
        for step in (1, 2):
            for side, source in ((1, below_ref), (-1, above_ref)):
                n = 2 * step - (1 if side == 1 else 0)
                taken = slot(side * step, reader, -side)
                pltpu.make_async_copy(
                    source.at[taken], outs[n].at[reader], sems.at[n]
                ).start()
        for n, side, source, at in ((5, 1, below_ref, 0), (6, -1, above_ref, half)):
            taken = slot(3 * side, reader, -side)
            pltpu.make_async_copy(
                source.at[taken, pl.ds(at, half)], outs[n].at[reader], sems.at[n]
            ).start()
    for reader in range(8):
        for k, source in enumerate((own_ref, below_ref, above_ref)):
            taken = slot(0, reader, (0, -1, 1)[k])
            pltpu.make_async_copy(
                source.at[taken], outs[0].at[reader * 3 + k], sems.at[0]
            ).start()
    for n, out in enumerate(outs):
        pltpu.make_async_copy(out, out, sems.at[n]).wait()


def pick(plane, table, own, below, above):
    shapes = [(24, PROWS)] + [(8, PROWS)] * 4 + [(8, PROWS // 2)] * 2
    grid_spec = pltpu.PrefetchScalarGridSpec(
        num_scalar_prefetch=2,
        grid=(1,),
        in_specs=[pl.BlockSpec(memory_space=pl.ANY)] * 3,
        out_specs=[pl.BlockSpec(memory_space=pl.ANY)] * len(shapes),
        scratch_shapes=[pltpu.SemaphoreType.DMA((len(shapes),))],
    )
    return pl.pallas_call(
        pick_kernel,
        grid_spec=grid_spec,
        out_shape=[
            jax.ShapeDtypeStruct((*shape, 2 * HEAD), jnp.bfloat16) for shape in shapes
        ],
        cost_estimate=pl.CostEstimate(flops=0, transcendentals=0, bytes_accessed=8 << 20),
        name="pick",
    )(plane, table, own, below, above)


def shift(value, axis, step):
    return lax.ppermute(value, axis, ring(lax.axis_size(axis), step))


def exchange(value, axes):
    return lax.all_to_all(value, axes, split_axis=0, concat_axis=0, tiled=True)


def layer(
    tokens,
    token_gain,
    inner_weight,
    gating_weight,
    filter_taps,
    channel_gain,
    retrieval_gate,
    passage_store,
    passage_gain,
    keys_weight,
    values_weight,
    owners,
    local_slots,
):
    me = lax.axis_index("tp").astype(jnp.int32).reshape(1)
    plane = lax.axis_index("z").astype(jnp.int32).reshape(1)
    left = shift(tokens, "tp", 1)
    right = shift(tokens, "tp", -1)
    far0 = shift(left[:LENGTH], "tp", 1)
    far1 = shift(right[LENGTH:], "tp", -1)

    own = project_passages(passage_store, passage_gain, keys_weight, values_weight)
    own = own.reshape(-1, PROWS, 2 * HEAD)
    below = shift(own, "z", 1)
    above = shift(own, "z", -1)

    asked = owners.reshape(-1)
    slots = local_slots.reshape(-1)
    wanted = jnp.sum(
        jnp.where(asked[:, None] == jnp.arange(64, dtype=jnp.int32)[None, :], slots[:, None], 0),
        axis=0,
    )
    wanted = jnp.broadcast_to(wanted.reshape(1, 8, 8).transpose(0, 2, 1), (8, 8, 8))
    table = exchange(wanted.reshape(64, 8), ST)

    near, up1, down1, up2, down2, up3, down3 = pick(
        plane, table.reshape(-1), own, below, above
    )
    up3 = shift(up3, "z", 3)
    down3 = shift(down3, "z", -3)
    up1 = shift(up1, "z", 1)
    down1 = shift(down1, "z", -1)
    up2 = shift(up2, "z", 2)
    down2 = shift(down2, "z", -2)
    side = ("y", "c")
    groups = [
        exchange(near.reshape(8, 3 * PROWS, -1), side),
        exchange(jnp.concatenate([up1, down1], axis=1), side),
        exchange(jnp.concatenate([up2, down2], axis=1), side),
        exchange(jnp.concatenate([up3, down3], axis=1), side),
    ]
    groups = [group.reshape(-1, PROWS, 2 * HEAD) for group in groups]

    convolved, stats = token_path(
        me,
        tokens,
        left,
        right,
        far0,
        far1,
        token_gain,
        inner_weight,
        gating_weight,
        filter_taps,
    )
    stats = lax.psum(stats, "tp")
    stats = stats.transpose(1, 0, 2, 3).reshape(2, -1, 128)
    conv_out = finish(convolved, stats, channel_gain)
    return attend(plane, asked, conv_out, retrieval_gate, groups)


def solution(mesh):
    st, tp = mesh.devices.shape
    fine = Mesh(mesh.devices.reshape(st // 8, 4, 2, tp), ST + ("tp",))
    placed = (
        P(ST, "tp"),
        P(),
        P(None, "tp"),
        P(None, "tp"),
        P(None, "tp"),
        P("tp"),
        P("tp"),
        P(ST, None, None),
        P(),
        P(None, "tp"),
        P(None, "tp"),
        P(ST, None),
        P(ST, None),
    )
    return jax.shard_map(layer, mesh=fine, in_specs=placed, out_specs=P(ST, "tp"), check_vma=False)
```

```python
import math

import jax
import jax.numpy as jnp
from jax import lax
from jax.experimental import pallas as pl
from jax.experimental.pallas import tpu as pltpu
from jax.sharding import Mesh
from jax.sharding import PartitionSpec as P

D = 2048
HEAD = 256
CONV = 31
LENGTH = 512
BLOCK = 64
PB = 2
PROWS = 64
EPSILON = 1e-06
EPSILON_NORM = 1e-05
ST = ("z", "y", "c")
LEAD = 32
ROWS_CHUNK = 64


def ring(size, step):
    return [(i, (i + step) % size) for i in range(size)]


def whole(shape):
    return pl.BlockSpec(shape, lambda *_: (0,) * len(shape))


def project_kernel(rows_ref, gain_ref, keys_ref, values_ref, out_ref):
    rows = rows_ref[...].astype(jnp.float32)
    inverse = lax.rsqrt(jnp.mean(rows * rows, axis=1, keepdims=True) + EPSILON)
    normed = (rows * inverse * gain_ref[...]).astype(jnp.bfloat16)
    out_ref[:, :HEAD] = jnp.dot(normed, keys_ref[...], preferred_element_type=jnp.float32).astype(
        jnp.bfloat16
    )
    out_ref[:, HEAD:] = jnp.dot(
        normed, values_ref[...], preferred_element_type=jnp.float32
    ).astype(jnp.bfloat16)


def project_passages(store, gain, keys_weight, values_weight):
    rows = store.reshape(-1, D)
    count = rows.shape[0]
    tile = 256
    return pl.pallas_call(
        project_kernel,
        grid=(count // tile,),
        in_specs=[
            pl.BlockSpec((tile, D), lambda i: (i, 0)),
            whole((1, D)),
            whole((D, HEAD)),
            whole((D, HEAD)),
        ],
        out_specs=pl.BlockSpec((tile, 2 * HEAD), lambda i: (i, 0)),
        out_shape=jax.ShapeDtypeStruct((count, 2 * HEAD), jnp.bfloat16),
        cost_estimate=pl.CostEstimate(
            flops=4 * count * D * HEAD, transcendentals=0, bytes_accessed=7 << 20
        ),
        name="project_passages",
    )(rows, gain.reshape(1, D), keys_weight, values_weight)


def token_kernel(
    me_ref,
    own_ref,
    left_ref,
    right_ref,
    far0_ref,
    far1_ref,
    gain_ref,
    inner_ref,
    gating_ref,
    taps_ref,
    out_ref,
    stats_ref,
    padded_ref,
):
    me = me_ref[0]
    first = pl.program_id(0) == 0
    width = own_ref.shape[1]
    squares = jnp.zeros((LENGTH, 1), jnp.float32)
    inner = jnp.zeros((LENGTH, width), jnp.float32)
    gating = jnp.zeros((LENGTH, width), jnp.float32)
    for offset in range(4):
        at = lax.rem(me + offset, 4)
        if offset == 0:
            piece = own_ref[...].astype(jnp.float32)
        elif offset == 1:
            piece = right_ref[...].astype(jnp.float32)
        elif offset == 3:
            piece = left_ref[...].astype(jnp.float32)
        else:
            piece = jnp.where(
                first, far0_ref[...].astype(jnp.float32), far1_ref[...].astype(jnp.float32)
            )
        squares = squares + jnp.sum(piece * piece, axis=1, keepdims=True)
        scaled = (piece * gain_ref[at]).astype(jnp.bfloat16)
        inner = inner + jnp.dot(scaled, inner_ref[at], preferred_element_type=jnp.float32)
        gating = gating + jnp.dot(scaled, gating_ref[at], preferred_element_type=jnp.float32)
    inverse = lax.rsqrt(squares / D + EPSILON)
    gated = (inner * inverse * jax.nn.sigmoid(gating * inverse)).astype(jnp.bfloat16)
    padded_ref[:LEAD, :] = jnp.zeros((LEAD, width), jnp.float32)
    padded_ref[LEAD:, :] = gated.astype(jnp.float32)
    shift = LEAD - CONV + 1

    def step(n):
        base = n * ROWS_CHUNK
        sums = jnp.zeros((ROWS_CHUNK, 128), jnp.float32)
        square_sums = jnp.zeros((ROWS_CHUNK, 128), jnp.float32)
        for lane in range(0, width, 128):
            total = jnp.zeros((ROWS_CHUNK, 128), jnp.float32)
            for s in range(8):
                part = None
                for j in range(LEAD // 8 + 1):
                    tap = 8 * j + s - shift
                    if tap < 0 or tap >= CONV:
                        continue
                    height = ROWS_CHUNK + (8 if s else 0)
                    term = (
                        padded_ref[pl.ds(base + 8 * j, height), lane : lane + 128]
                        * taps_ref[tap : tap + 1, lane : lane + 128]
                    )
                    part = term if part is None else part + term
                total = total + part[s : s + ROWS_CHUNK]
            out_ref[pl.ds(base, ROWS_CHUNK), lane : lane + 128] = total
            sums = sums + total
            square_sums = square_sums + total * total
        return sums, square_sums

    for n in range(LENGTH // 128):
        pair = [step(2 * n + h) for h in range(2)]
        sums = jnp.concatenate([pair[0][0], pair[1][0]], axis=0)
        square_sums = jnp.concatenate([pair[0][1], pair[1][1]], axis=0)
        stats_ref[0, n : n + 1, :] = jnp.sum(sums.T, axis=0, keepdims=True)
        stats_ref[1, n : n + 1, :] = jnp.sum(square_sums.T, axis=0, keepdims=True)


def token_path(me, own, left, right, far0, far1, gain, inner_weight, gating_weight, taps):
    rows, width = own.shape
    grid_spec = pltpu.PrefetchScalarGridSpec(
        num_scalar_prefetch=1,
        grid=(rows // LENGTH,),
        in_specs=[pl.BlockSpec((LENGTH, width), lambda i, m: (i, 0))] * 3
        + [
            whole((LENGTH, width)),
            whole((LENGTH, width)),
            whole((4, 1, width)),
            whole((4, width, width)),
            whole((4, width, width)),
            whole((CONV, width)),
        ],
        out_specs=[
            pl.BlockSpec((LENGTH, width), lambda i, m: (i, 0)),
            pl.BlockSpec((None, 2, LENGTH // 128, 128), lambda i, m: (i, 0, 0, 0)),
        ],
        scratch_shapes=[pltpu.VMEM((LEAD + LENGTH, width), jnp.float32)],
    )
    return pl.pallas_call(
        token_kernel,
        grid_spec=grid_spec,
        out_shape=[
            jax.ShapeDtypeStruct((rows, width), jnp.float32),
            jax.ShapeDtypeStruct((rows // LENGTH, 2, LENGTH // 128, 128), jnp.float32),
        ],
        cost_estimate=pl.CostEstimate(
            flops=4 * rows * D * width, transcendentals=rows * width, bytes_accessed=10 << 20
        ),
        name="token_path",
    )(
        me,
        own,
        left,
        right,
        far0,
        far1,
        gain.reshape(4, 1, width),
        inner_weight.reshape(4, width, width),
        gating_weight.reshape(4, width, width),
        taps,
    )


def finish_kernel(conv_ref, stats_ref, gain_ref, out_ref):
    width = conv_ref.shape[1]
    turn = pl.program_id(0)
    for n in range(conv_ref.shape[0] // 128):
        at = turn * (conv_ref.shape[0] // 128) + n
        rows = slice(n * 128, (n + 1) * 128)
        average = stats_ref[0, pl.ds(at, 1), :] / D
        variance = stats_ref[1, pl.ds(at, 1), :] / D - average * average
        spread = lax.rsqrt(variance + EPSILON_NORM)
        average = jnp.broadcast_to(average, (128, 128)).T
        spread = jnp.broadcast_to(spread, (128, 128)).T
        for lane in range(0, width, 128):
            part = slice(lane, lane + 128)
            scaled = (conv_ref[rows, part] - average) * spread * gain_ref[:, part]
            out_ref[rows, part] = scaled * jax.nn.sigmoid(scaled)


def finish(convolved, stats, channel_gain):
    rows, width = convolved.shape
    tile = 512
    return pl.pallas_call(
        finish_kernel,
        grid=(rows // tile,),
        in_specs=[
            pl.BlockSpec((tile, width), lambda i: (i, 0)),
            whole((2, rows // 128, 128)),
            whole((1, width)),
        ],
        out_specs=pl.BlockSpec((tile, width), lambda i: (i, 0)),
        out_shape=jax.ShapeDtypeStruct((rows, width), jnp.float32),
        cost_estimate=pl.CostEstimate(
            flops=8 * rows * width, transcendentals=rows * width, bytes_accessed=4 << 20
        ),
        name="finish",
    )(convolved, stats, channel_gain.reshape(1, width))


def attend_kernel(plane_ref, where_ref, conv_ref, gate_ref, *refs):
    near_ref, far_ref, upper_ref, lower_ref, out_ref, held_ref, sems = refs
    turn = pl.program_id(0)
    count = where_ref.shape[0]
    here = plane_ref[0]
    half = PROWS // 2

    @pl.when(turn == 0)
    def _():
        for n in range(count):
            owner = where_ref[n]
            away = lax.rem(owner // 8 - here + 8, 8)
            column = lax.rem(owner, 8)
            close = (away <= 1) | (away == 7)

            @pl.when(close)
            def _():
                k = jnp.where(away == 7, 1, 2 * away)
                at = pl.multiple_of(k * PROWS, PROWS)
                pltpu.make_async_copy(
                    near_ref.at[column, pl.ds(at, PROWS)], held_ref.at[n], sems.at[n]
                ).start()

            @pl.when(away == 4)
            def _():
                pltpu.make_async_copy(
                    upper_ref.at[column], held_ref.at[n, pl.ds(0, half)], sems.at[n]
                ).start()
                pltpu.make_async_copy(
                    lower_ref.at[column], held_ref.at[n, pl.ds(half, half)], sems.at[n]
                ).start()

            @pl.when(jnp.logical_not(close) & (away != 4))
            def _():
                k = jnp.where(away < 4, 2 * away - 3, 12 - 2 * away)
                at = pl.multiple_of(k * PROWS, PROWS)
                pltpu.make_async_copy(
                    far_ref.at[column, pl.ds(at, PROWS)], held_ref.at[n], sems.at[n]
                ).start()

    blocks = conv_ref.shape[0] // BLOCK
    weight = jax.nn.sigmoid(gate_ref[...])
    queries = conv_ref[...].astype(jnp.bfloat16)
    for n in range(blocks * PB):
        at = turn * blocks * PB + n
        pltpu.make_async_copy(
            far_ref.at[0, pl.ds(0, PROWS)], held_ref.at[at], sems.at[at]
        ).wait()
    scores = []
    for b in range(blocks):
        held = held_ref[pl.ds((turn * blocks + b) * PB, PB)].reshape(PB * PROWS, 2 * HEAD)
        rows = slice(b * BLOCK, (b + 1) * BLOCK)
        heads = jnp.concatenate([queries[rows, :HEAD], queries[rows, HEAD:]], axis=0)
        scores.append(
            lax.dot_general(
                heads,
                held[:, :HEAD],
                (((1,), (1,)), ((), ())),
                preferred_element_type=jnp.float32,
            )
            / math.sqrt(HEAD)
        )
    shares = []
    for b in range(blocks):
        raised = jnp.exp(scores[b] - jnp.max(scores[b], axis=1, keepdims=True))
        shares.append((raised / jnp.sum(raised, axis=1, keepdims=True)).astype(jnp.bfloat16))
    for b in range(blocks):
        held = held_ref[pl.ds((turn * blocks + b) * PB, PB)].reshape(PB * PROWS, 2 * HEAD)
        attended = jnp.dot(shares[b], held[:, HEAD:], preferred_element_type=jnp.float32)
        attended = jnp.concatenate([attended[:BLOCK], attended[BLOCK:]], axis=1)
        rows = slice(b * BLOCK, (b + 1) * BLOCK)
        out_ref[rows, :] = (conv_ref[rows, :] + weight * attended).astype(jnp.bfloat16)


def attend(plane, where, conv_out, retrieval_gate, groups):
    rows, width = conv_out.shape
    count = where.shape[0]
    tile = 512
    grid_spec = pltpu.PrefetchScalarGridSpec(
        num_scalar_prefetch=2,
        grid=(rows // tile,),
        in_specs=[
            pl.BlockSpec((tile, width), lambda i, *_: (i, 0)),
            whole((1, width)),
        ]
        + [pl.BlockSpec(memory_space=pl.ANY)] * len(groups),
        out_specs=pl.BlockSpec((tile, width), lambda i, *_: (i, 0)),
        scratch_shapes=[
            pltpu.VMEM((count, PROWS, 2 * HEAD), jnp.bfloat16),
            pltpu.SemaphoreType.DMA((count,)),
        ],
    )
    return pl.pallas_call(
        attend_kernel,
        grid_spec=grid_spec,
        out_shape=jax.ShapeDtypeStruct((rows, width), jnp.bfloat16),
        cost_estimate=pl.CostEstimate(
            flops=4 * rows * 2 * PB * PROWS * HEAD,
            transcendentals=rows * 2 * PB * PROWS,
            bytes_accessed=5 << 20,
        ),
        name="attend",
    )(plane, where, conv_out, retrieval_gate.reshape(1, width), *groups)


def pick_kernel(plane_ref, table_ref, own_ref, below_ref, above_ref, *refs):
    outs, sems = refs[:-1], refs[-1]
    here = plane_ref[0]
    half = PROWS // 2

    def slot(reader_plane, reader, owner_plane):
        at = lax.rem(here + reader_plane + 8, 8) * 8 + reader
        return table_ref[at, lax.rem(here + owner_plane + 8, 8)]

    for reader in range(8):
        for k, (source, owner_plane) in enumerate(((own_ref, 0), (below_ref, -1), (above_ref, 1))):
            pltpu.make_async_copy(
                source.at[slot(0, reader, owner_plane)],
                outs[0].at[reader, pl.ds(k * PROWS, PROWS)],
                sems.at[0],
            ).start()
        for source, side, at in ((below_ref, 1, 0), (above_ref, -1, half)):
            pltpu.make_async_copy(
                source.at[slot(3 * side, reader, -side), pl.ds(at, half)],
                outs[0].at[reader, pl.ds(3 * PROWS + at, half)],
                sems.at[0],
            ).start()
    for reader in range(8):
        for n, (source, side, steps) in enumerate(
            ((below_ref, 1, 1), (above_ref, -1, 1), (below_ref, 1, 2), (above_ref, -1, 2))
        ):
            pltpu.make_async_copy(
                source.at[slot(side * steps, reader, -side)],
                outs[1 + n].at[reader],
                sems.at[1 + n],
            ).start()
    for n, out in enumerate(outs):
        pltpu.make_async_copy(out, out, sems.at[n]).wait()


def pick(plane, table, own, below, above):
    shapes = [(8, 4 * PROWS)] + [(8, PROWS)] * 4
    return pl.pallas_call(
        pick_kernel,
        in_specs=[pl.BlockSpec(memory_space=pltpu.SMEM)] * 2
        + [pl.BlockSpec(memory_space=pltpu.VMEM)] * 3,
        out_specs=[pl.BlockSpec(memory_space=pl.ANY)] * len(shapes),
        scratch_shapes=[pltpu.SemaphoreType.DMA((len(shapes),))],
        out_shape=[
            jax.ShapeDtypeStruct((*shape, 2 * HEAD), jnp.bfloat16) for shape in shapes
        ],
        cost_estimate=pl.CostEstimate(flops=0, transcendentals=0, bytes_accessed=8 << 20),
        name="pick",
    )(plane, table, own, below, above)


def join_kernel(*refs):
    for n, ref in enumerate(refs[:-1]):
        refs[-1][n * PROWS : (n + 1) * PROWS, :] = ref[...]


def join(parts):
    tile = (None, PROWS, 2 * HEAD)
    count = len(parts)
    return pl.pallas_call(
        join_kernel,
        grid=(8,),
        in_specs=[pl.BlockSpec(tile, lambda i: (i, 0, 0))] * count,
        out_specs=pl.BlockSpec((None, count * PROWS, 2 * HEAD), lambda i: (i, 0, 0)),
        out_shape=jax.ShapeDtypeStruct((8, count * PROWS, 2 * HEAD), jnp.bfloat16),
        cost_estimate=pl.CostEstimate(flops=0, transcendentals=0, bytes_accessed=4 << 20),
        name="join",
    )(*parts)


def shift(value, axis, step):
    return lax.ppermute(value, axis, ring(lax.axis_size(axis), step))


def exchange(value, axes):
    return lax.all_to_all(value, axes, split_axis=0, concat_axis=0, tiled=True)


def layer(
    tokens,
    token_gain,
    inner_weight,
    gating_weight,
    filter_taps,
    channel_gain,
    retrieval_gate,
    passage_store,
    passage_gain,
    keys_weight,
    values_weight,
    owners,
    local_slots,
):
    me = lax.axis_index("tp").astype(jnp.int32).reshape(1)
    plane = lax.axis_index("z").astype(jnp.int32).reshape(1)
    left = shift(tokens, "tp", 1)
    right = shift(tokens, "tp", -1)
    far0 = shift(left[:LENGTH], "tp", 1)
    far1 = shift(right[LENGTH:], "tp", -1)

    own = project_passages(passage_store, passage_gain, keys_weight, values_weight)
    own = own.reshape(-1, PROWS, 2 * HEAD)
    below = shift(own, "z", 1)
    above = shift(own, "z", -1)

    asked = owners.reshape(-1)
    slots = local_slots.reshape(-1)
    wanted = jnp.sum(
        jnp.where(asked[:, None] == jnp.arange(64, dtype=jnp.int32)[None, :], slots[:, None], 0),
        axis=0,
    )
    wanted = jnp.broadcast_to(wanted.reshape(1, 8, 8).transpose(0, 2, 1), (8, 8, 8))
    table = exchange(wanted.reshape(64, 8), ST)

    near, up1, down1, up2, down2 = pick(plane, table, own, below, above)
    side = ("y", "c")
    near = exchange(near, side)
    far = [shift(up1, "z", 1), shift(down1, "z", -1), shift(up2, "z", 2), shift(down2, "z", -2)]
    far = join(far)
    far = exchange(far, side)
    split = 3 * PROWS + PROWS // 2
    upper = shift(near[:, 3 * PROWS : split], "z", 3)
    lower = shift(near[:, split:], "z", -3)

    convolved, stats = token_path(
        me,
        tokens,
        left,
        right,
        far0,
        far1,
        token_gain,
        inner_weight,
        gating_weight,
        filter_taps,
    )
    stats = lax.psum(stats, "tp")
    stats = stats.transpose(1, 0, 2, 3).reshape(2, -1, 128)
    conv_out = finish(convolved, stats, channel_gain)
    return attend(plane, asked, conv_out, retrieval_gate, (near, far, upper, lower))


def solution(mesh):
    st, tp = mesh.devices.shape
    fine = Mesh(mesh.devices.reshape(st // 8, 4, 2, tp), ST + ("tp",))
    placed = (
        P(ST, "tp"),
        P(),
        P(None, "tp"),
        P(None, "tp"),
        P(None, "tp"),
        P("tp"),
        P("tp"),
        P(ST, None, None),
        P(),
        P(None, "tp"),
        P(None, "tp"),
        P(ST, None),
        P(ST, None),
    )
    return jax.shard_map(layer, mesh=fine, in_specs=placed, out_specs=P(ST, "tp"), check_vma=False)
```

```python
import functools
import math

import jax
import jax.numpy as jnp
from jax import lax
from jax.experimental import pallas as pl
from jax.experimental.pallas import tpu as pltpu
from jax.sharding import Mesh
from jax.sharding import PartitionSpec as P

D = 2048
HEAD = 256
CONV = 31
LENGTH = 512
BLOCK = 64
PB = 2
PROWS = 64
EPSILON = 1e-06
EPSILON_NORM = 1e-05
ST = ("z", "y", "c")
LEAD = 32
ROWS_CHUNK = 64


def ring(size, step):
    return [(i, (i + step) % size) for i in range(size)]


def whole(shape):
    return pl.BlockSpec(shape, lambda *_: (0,) * len(shape))


def project_kernel(rows_ref, gain_ref, keys_ref, values_ref, out_ref):
    rows = rows_ref[...].astype(jnp.float32)
    inverse = lax.rsqrt(jnp.mean(rows * rows, axis=1, keepdims=True) + EPSILON)
    normed = (rows * inverse * gain_ref[...]).astype(jnp.bfloat16)
    out_ref[:, :HEAD] = jnp.dot(normed, keys_ref[...], preferred_element_type=jnp.float32).astype(
        jnp.bfloat16
    )
    out_ref[:, HEAD:] = jnp.dot(
        normed, values_ref[...], preferred_element_type=jnp.float32
    ).astype(jnp.bfloat16)


def project_passages(store, gain, keys_weight, values_weight):
    rows = store.reshape(-1, D)
    count = rows.shape[0]
    tile = 256
    return pl.pallas_call(
        project_kernel,
        grid=(count // tile,),
        in_specs=[
            pl.BlockSpec((tile, D), lambda i: (i, 0)),
            whole((1, D)),
            whole((D, HEAD)),
            whole((D, HEAD)),
        ],
        out_specs=pl.BlockSpec((tile, 2 * HEAD), lambda i: (i, 0)),
        out_shape=jax.ShapeDtypeStruct((count, 2 * HEAD), jnp.bfloat16),
        cost_estimate=pl.CostEstimate(
            flops=4 * count * D * HEAD, transcendentals=0, bytes_accessed=7 << 20
        ),
        name="project_passages",
    )(rows, gain.reshape(1, D), keys_weight, values_weight)


def token_kernel(
    me_ref,
    own_ref,
    left_ref,
    right_ref,
    far_ref,
    gain_ref,
    inner_ref,
    gating_ref,
    taps_ref,
    out_ref,
    stats_ref,
    padded_ref,
):
    me = me_ref[0]
    width = own_ref.shape[1]
    squares = jnp.zeros((LENGTH, 1), jnp.float32)
    inner = jnp.zeros((LENGTH, width), jnp.float32)
    gating = jnp.zeros((LENGTH, width), jnp.float32)
    for offset in range(4):
        at = lax.rem(me + offset, 4)
        if offset == 0:
            piece = own_ref[...].astype(jnp.float32)
        elif offset == 1:
            piece = right_ref[...].astype(jnp.float32)
        elif offset == 3:
            piece = left_ref[...].astype(jnp.float32)
        else:
            piece = far_ref[...].astype(jnp.float32)
        squares = squares + jnp.sum(piece * piece, axis=1, keepdims=True)
        scaled = (piece * gain_ref[at]).astype(jnp.bfloat16)
        inner = inner + jnp.dot(scaled, inner_ref[at], preferred_element_type=jnp.float32)
        gating = gating + jnp.dot(scaled, gating_ref[at], preferred_element_type=jnp.float32)
    inverse = lax.rsqrt(squares / D + EPSILON)
    gated = (inner * inverse * jax.nn.sigmoid(gating * inverse)).astype(jnp.bfloat16)
    padded_ref[:LEAD, :] = jnp.zeros((LEAD, width), jnp.float32)
    padded_ref[LEAD:, :] = gated.astype(jnp.float32)
    shift = LEAD - CONV + 1

    def step(n):
        base = n * ROWS_CHUNK
        sums = jnp.zeros((ROWS_CHUNK, 128), jnp.float32)
        square_sums = jnp.zeros((ROWS_CHUNK, 128), jnp.float32)
        for lane in range(0, width, 128):
            total = jnp.zeros((ROWS_CHUNK, 128), jnp.float32)
            for s in range(8):
                part = None
                for j in range(LEAD // 8 + 1):
                    tap = 8 * j + s - shift
                    if tap < 0 or tap >= CONV:
                        continue
                    height = ROWS_CHUNK + (8 if s else 0)
                    term = (
                        padded_ref[pl.ds(base + 8 * j, height), lane : lane + 128]
                        * taps_ref[tap : tap + 1, lane : lane + 128]
                    )
                    part = term if part is None else part + term
                total = total + part[s : s + ROWS_CHUNK]
            out_ref[pl.ds(base, ROWS_CHUNK), lane : lane + 128] = total
            sums = sums + total
            square_sums = square_sums + total * total
        return sums, square_sums

    for n in range(LENGTH // 128):
        pair = [step(2 * n + h) for h in range(2)]
        sums = jnp.concatenate([pair[0][0], pair[1][0]], axis=0)
        square_sums = jnp.concatenate([pair[0][1], pair[1][1]], axis=0)
        stats_ref[0, n : n + 1, :] = jnp.sum(sums.T, axis=0, keepdims=True)
        stats_ref[1, n : n + 1, :] = jnp.sum(square_sums.T, axis=0, keepdims=True)


def token_path(me, own, left, right, far, gain, inner_weight, gating_weight, taps):
    rows, width = own.shape
    grid_spec = pltpu.PrefetchScalarGridSpec(
        num_scalar_prefetch=1,
        grid=(rows // LENGTH,),
        in_specs=[pl.BlockSpec((LENGTH, width), lambda i, m: (i, 0))] * 4
        + [
            whole((4, 1, width)),
            whole((4, width, width)),
            whole((4, width, width)),
            whole((CONV, width)),
        ],
        out_specs=[
            pl.BlockSpec((LENGTH, width), lambda i, m: (i, 0)),
            pl.BlockSpec((None, 2, LENGTH // 128, 128), lambda i, m: (i, 0, 0, 0)),
        ],
        scratch_shapes=[pltpu.VMEM((LEAD + LENGTH, width), jnp.float32)],
    )
    return pl.pallas_call(
        token_kernel,
        grid_spec=grid_spec,
        out_shape=[
            jax.ShapeDtypeStruct((rows, width), jnp.float32),
            jax.ShapeDtypeStruct((rows // LENGTH, 2, LENGTH // 128, 128), jnp.float32),
        ],
        cost_estimate=pl.CostEstimate(
            flops=4 * rows * D * width, transcendentals=rows * width, bytes_accessed=10 << 20
        ),
        name="token_path",
    )(
        me,
        own,
        left,
        right,
        far,
        gain.reshape(4, 1, width),
        inner_weight.reshape(4, width, width),
        gating_weight.reshape(4, width, width),
        taps,
    )


def finish_kernel(conv_ref, stats_ref, gain_ref, out_ref):
    width = conv_ref.shape[1]
    turn = pl.program_id(0)
    for n in range(conv_ref.shape[0] // 128):
        at = turn * (conv_ref.shape[0] // 128) + n
        rows = slice(n * 128, (n + 1) * 128)
        average = stats_ref[0, pl.ds(at, 1), :] / D
        variance = stats_ref[1, pl.ds(at, 1), :] / D - average * average
        spread = lax.rsqrt(variance + EPSILON_NORM)
        average = jnp.broadcast_to(average, (128, 128)).T
        spread = jnp.broadcast_to(spread, (128, 128)).T
        for lane in range(0, width, 128):
            part = slice(lane, lane + 128)
            scaled = (conv_ref[rows, part] - average) * spread * gain_ref[:, part]
            out_ref[rows, part] = scaled * jax.nn.sigmoid(scaled)


def finish(convolved, stats, channel_gain):
    rows, width = convolved.shape
    tile = 512
    return pl.pallas_call(
        finish_kernel,
        grid=(rows // tile,),
        in_specs=[
            pl.BlockSpec((tile, width), lambda i: (i, 0)),
            whole((2, rows // 128, 128)),
            whole((1, width)),
        ],
        out_specs=pl.BlockSpec((tile, width), lambda i: (i, 0)),
        out_shape=jax.ShapeDtypeStruct((rows, width), jnp.float32),
        cost_estimate=pl.CostEstimate(
            flops=8 * rows * width, transcendentals=rows * width, bytes_accessed=4 << 20
        ),
        name="finish",
    )(convolved, stats, channel_gain.reshape(1, width))


def attend_kernel(plane_ref, where_ref, conv_ref, gate_ref, *refs):
    near_ref, far_ref, upper_ref, lower_ref, out_ref, held_ref, sems = refs
    turn = pl.program_id(0)
    count = where_ref.shape[0]
    here = plane_ref[0]
    half = PROWS // 2

    @pl.when(turn == 0)
    def _():
        for n in range(count):
            owner = where_ref[n]
            away = lax.rem(owner // 8 - here + 8, 8)
            column = lax.rem(owner, 8)
            close = (away <= 1) | (away == 7)

            @pl.when(close)
            def _():
                k = jnp.where(away == 7, 1, 2 * away)
                at = pl.multiple_of(k * PROWS, PROWS)
                pltpu.make_async_copy(
                    near_ref.at[column, pl.ds(at, PROWS)], held_ref.at[n], sems.at[n]
                ).start()

            @pl.when(away == 4)
            def _():
                pltpu.make_async_copy(
                    upper_ref.at[column], held_ref.at[n, pl.ds(0, half)], sems.at[n]
                ).start()
                pltpu.make_async_copy(
                    lower_ref.at[column], held_ref.at[n, pl.ds(half, half)], sems.at[n]
                ).start()

            @pl.when(jnp.logical_not(close) & (away != 4))
            def _():
                k = jnp.where(away < 4, 2 * away - 3, 12 - 2 * away)
                at = pl.multiple_of(k * PROWS, PROWS)
                pltpu.make_async_copy(
                    far_ref.at[column, pl.ds(at, PROWS)], held_ref.at[n], sems.at[n]
                ).start()

    blocks = conv_ref.shape[0] // BLOCK
    weight = jax.nn.sigmoid(gate_ref[...])
    queries = conv_ref[...].astype(jnp.bfloat16)
    for n in range(blocks * PB):
        at = turn * blocks * PB + n
        pltpu.make_async_copy(
            far_ref.at[0, pl.ds(0, PROWS)], held_ref.at[at], sems.at[at]
        ).wait()
    scores = []
    for b in range(blocks):
        held = held_ref[pl.ds((turn * blocks + b) * PB, PB)].reshape(PB * PROWS, 2 * HEAD)
        rows = slice(b * BLOCK, (b + 1) * BLOCK)
        heads = jnp.concatenate([queries[rows, :HEAD], queries[rows, HEAD:]], axis=0)
        scores.append(
            lax.dot_general(
                heads,
                held[:, :HEAD],
                (((1,), (1,)), ((), ())),
                preferred_element_type=jnp.float32,
            )
            / math.sqrt(HEAD)
        )
    shares = []
    for b in range(blocks):
        raised = jnp.exp(scores[b] - jnp.max(scores[b], axis=1, keepdims=True))
        shares.append((raised / jnp.sum(raised, axis=1, keepdims=True)).astype(jnp.bfloat16))
    for b in range(blocks):
        held = held_ref[pl.ds((turn * blocks + b) * PB, PB)].reshape(PB * PROWS, 2 * HEAD)
        attended = jnp.dot(shares[b], held[:, HEAD:], preferred_element_type=jnp.float32)
        attended = jnp.concatenate([attended[:BLOCK], attended[BLOCK:]], axis=1)
        rows = slice(b * BLOCK, (b + 1) * BLOCK)
        out_ref[rows, :] = (conv_ref[rows, :] + weight * attended).astype(jnp.bfloat16)


def attend(plane, where, conv_out, retrieval_gate, groups):
    rows, width = conv_out.shape
    count = where.shape[0]
    tile = 512
    grid_spec = pltpu.PrefetchScalarGridSpec(
        num_scalar_prefetch=2,
        grid=(rows // tile,),
        in_specs=[
            pl.BlockSpec((tile, width), lambda i, *_: (i, 0)),
            whole((1, width)),
        ]
        + [pl.BlockSpec(memory_space=pl.ANY)] * len(groups),
        out_specs=pl.BlockSpec((tile, width), lambda i, *_: (i, 0)),
        scratch_shapes=[
            pltpu.VMEM((count, PROWS, 2 * HEAD), jnp.bfloat16),
            pltpu.SemaphoreType.DMA((count,)),
        ],
    )
    return pl.pallas_call(
        attend_kernel,
        grid_spec=grid_spec,
        out_shape=jax.ShapeDtypeStruct((rows, width), jnp.bfloat16),
        cost_estimate=pl.CostEstimate(
            flops=4 * rows * 2 * PB * PROWS * HEAD,
            transcendentals=rows * 2 * PB * PROWS,
            bytes_accessed=5 << 20,
        ),
        name="attend",
    )(plane, where, conv_out, retrieval_gate.reshape(1, width), *groups)


def pick_kernel(plane_ref, table_ref, own_ref, below_ref, above_ref, *refs):
    outs, sems = refs[:-1], refs[-1]
    here = plane_ref[0]
    half = PROWS // 2

    def slot(reader_plane, reader, owner_plane):
        at = lax.rem(here + reader_plane + 8, 8) * 8 + reader
        return table_ref[at, lax.rem(here + owner_plane + 8, 8)]

    for reader in range(8):
        for k, (source, owner_plane) in enumerate(((own_ref, 0), (below_ref, -1), (above_ref, 1))):
            pltpu.make_async_copy(
                source.at[slot(0, reader, owner_plane)],
                outs[0].at[reader, pl.ds(k * PROWS, PROWS)],
                sems.at[0],
            ).start()
        for source, side, at in ((below_ref, 1, 0), (above_ref, -1, half)):
            pltpu.make_async_copy(
                source.at[slot(3 * side, reader, -side), pl.ds(at, half)],
                outs[0].at[reader, pl.ds(3 * PROWS + at, half)],
                sems.at[0],
            ).start()
    for reader in range(8):
        for n, (source, side, steps) in enumerate(
            ((below_ref, 1, 1), (above_ref, -1, 1), (below_ref, 1, 2), (above_ref, -1, 2))
        ):
            pltpu.make_async_copy(
                source.at[slot(side * steps, reader, -side)],
                outs[1 + n].at[reader],
                sems.at[1 + n],
            ).start()
    for n, out in enumerate(outs):
        pltpu.make_async_copy(out, out, sems.at[n]).wait()


def pick(plane, table, own, below, above):
    shapes = [(8, 4 * PROWS)] + [(8, PROWS)] * 4
    return pl.pallas_call(
        pick_kernel,
        in_specs=[pl.BlockSpec(memory_space=pltpu.SMEM)] * 2
        + [pl.BlockSpec(memory_space=pltpu.VMEM)] * 3,
        out_specs=[pl.BlockSpec(memory_space=pl.ANY)] * len(shapes),
        scratch_shapes=[pltpu.SemaphoreType.DMA((len(shapes),))],
        out_shape=[
            jax.ShapeDtypeStruct((*shape, 2 * HEAD), jnp.bfloat16) for shape in shapes
        ],
        cost_estimate=pl.CostEstimate(flops=0, transcendentals=0, bytes_accessed=8 << 20),
        name="pick",
    )(plane, table, own, below, above)


def fill_kernel(*refs, at):
    first_ref, second_ref, out_ref, sems = refs[0], refs[1], refs[-2], refs[-1]
    copies = [
        pltpu.make_async_copy(
            ref, out_ref.at[:, pl.ds((at + n) * PROWS, PROWS)], sems.at[n]
        )
        for n, ref in enumerate((first_ref, second_ref))
    ]
    for copy in copies:
        copy.start()
    for copy in copies:
        copy.wait()


def fill(first, second, at, into=None):
    held = [] if into is None else [into]
    return pl.pallas_call(
        functools.partial(fill_kernel, at=at),
        in_specs=[pl.BlockSpec(memory_space=pltpu.VMEM)] * 2
        + [pl.BlockSpec(memory_space=pl.ANY)] * len(held),
        out_specs=pl.BlockSpec(memory_space=pl.ANY),
        scratch_shapes=[pltpu.SemaphoreType.DMA((2,))],
        out_shape=jax.ShapeDtypeStruct((8, 4 * PROWS, 2 * HEAD), jnp.bfloat16),
        input_output_aliases={2: 0} if held else {},
        cost_estimate=pl.CostEstimate(flops=0, transcendentals=0, bytes_accessed=2 << 20),
        name="fill",
    )(first, second, *held)


def shift(value, axis, step):
    return lax.ppermute(value, axis, ring(lax.axis_size(axis), step))


def exchange(value, axes):
    return lax.all_to_all(value, axes, split_axis=0, concat_axis=0, tiled=True)


def layer(
    tokens,
    token_gain,
    inner_weight,
    gating_weight,
    filter_taps,
    channel_gain,
    retrieval_gate,
    passage_store,
    passage_gain,
    keys_weight,
    values_weight,
    owners,
    local_slots,
):
    me = lax.axis_index("tp").astype(jnp.int32).reshape(1)
    plane = lax.axis_index("z").astype(jnp.int32).reshape(1)
    left = shift(tokens, "tp", 1)
    right = shift(tokens, "tp", -1)
    far = shift(tokens, "tp", 2)

    own = project_passages(passage_store, passage_gain, keys_weight, values_weight)
    own = own.reshape(-1, PROWS, 2 * HEAD)
    below = shift(own, "z", 1)
    above = shift(own, "z", -1)

    asked = owners.reshape(-1)
    slots = local_slots.reshape(-1)
    wanted = jnp.sum(
        jnp.where(asked[:, None] == jnp.arange(64, dtype=jnp.int32)[None, :], slots[:, None], 0),
        axis=0,
    )
    wanted = jnp.broadcast_to(wanted.reshape(1, 8, 8).transpose(0, 2, 1), (8, 8, 8))
    table = exchange(wanted.reshape(64, 8), ST)

    near, up1, down1, up2, down2 = pick(plane, table, own, below, above)
    side = ("y", "c")
    near = exchange(near, side)
    up1 = shift(up1, "z", 1)
    down1 = shift(down1, "z", -1)
    up2 = shift(up2, "z", 2)
    down2 = shift(down2, "z", -2)
    away = fill(up1, down1, 0)
    away = fill(up2, down2, 2, away)
    away = exchange(away, side)
    split = 3 * PROWS + PROWS // 2
    upper = shift(near[:, 3 * PROWS : split], "z", 3)
    lower = shift(near[:, split:], "z", -3)

    convolved, stats = token_path(
        me,
        tokens,
        left,
        right,
        far,
        token_gain,
        inner_weight,
        gating_weight,
        filter_taps,
    )
    stats = lax.psum(stats, "tp")
    stats = stats.transpose(1, 0, 2, 3).reshape(2, -1, 128)
    conv_out = finish(convolved, stats, channel_gain)
    return attend(plane, asked, conv_out, retrieval_gate, (near, away, upper, lower))


def solution(mesh):
    st, tp = mesh.devices.shape
    fine = Mesh(mesh.devices.reshape(st // 8, 4, 2, tp), ST + ("tp",))
    placed = (
        P(ST, "tp"),
        P(),
        P(None, "tp"),
        P(None, "tp"),
        P(None, "tp"),
        P("tp"),
        P("tp"),
        P(ST, None, None),
        P(),
        P(None, "tp"),
        P(None, "tp"),
        P(ST, None),
        P(ST, None),
    )
    return jax.shard_map(layer, mesh=fine, in_specs=placed, out_specs=P(ST, "tp"), check_vma=False)
```

```python
import functools
import math

import jax
import jax.numpy as jnp
from jax import lax
from jax.experimental import pallas as pl
from jax.experimental.pallas import tpu as pltpu
from jax.sharding import Mesh
from jax.sharding import PartitionSpec as P

D = 2048
HEAD = 256
CONV = 31
LENGTH = 512
BLOCK = 64
PB = 2
PROWS = 64
EPSILON = 1e-06
EPSILON_NORM = 1e-05
ST = ("z", "y", "c")
LEAD = 32
ROWS_CHUNK = 64
KEPT = 48
NEAR_ROWS = 4 * PROWS + 2 * (PROWS - KEPT)
AWAY_ROWS = 2 * PROWS + 2 * KEPT


def ring(size, step):
    return [(i, (i + step) % size) for i in range(size)]


def whole(shape):
    return pl.BlockSpec(shape, lambda *_: (0,) * len(shape))


def project_kernel(rows_ref, gain_ref, keys_ref, values_ref, out_ref):
    rows = rows_ref[...].astype(jnp.float32)
    inverse = lax.rsqrt(jnp.mean(rows * rows, axis=1, keepdims=True) + EPSILON)
    normed = (rows * inverse * gain_ref[...]).astype(jnp.bfloat16)
    out_ref[:, :HEAD] = jnp.dot(normed, keys_ref[...], preferred_element_type=jnp.float32).astype(
        jnp.bfloat16
    )
    out_ref[:, HEAD:] = jnp.dot(
        normed, values_ref[...], preferred_element_type=jnp.float32
    ).astype(jnp.bfloat16)


def project_passages(store, gain, keys_weight, values_weight):
    rows = store.reshape(-1, D)
    count = rows.shape[0]
    tile = 256
    return pl.pallas_call(
        project_kernel,
        grid=(count // tile,),
        in_specs=[
            pl.BlockSpec((tile, D), lambda i: (i, 0)),
            whole((1, D)),
            whole((D, HEAD)),
            whole((D, HEAD)),
        ],
        out_specs=pl.BlockSpec((tile, 2 * HEAD), lambda i: (i, 0)),
        out_shape=jax.ShapeDtypeStruct((count, 2 * HEAD), jnp.bfloat16),
        cost_estimate=pl.CostEstimate(
            flops=4 * count * D * HEAD, transcendentals=0, bytes_accessed=7 << 20
        ),
        name="project_passages",
    )(rows, gain.reshape(1, D), keys_weight, values_weight)


def token_kernel(
    me_ref,
    own_ref,
    left_ref,
    right_ref,
    far_ref,
    gain_ref,
    inner_ref,
    gating_ref,
    taps_ref,
    out_ref,
    stats_ref,
    padded_ref,
):
    me = me_ref[0]
    width = own_ref.shape[1]
    squares = jnp.zeros((LENGTH, 1), jnp.float32)
    inner = jnp.zeros((LENGTH, width), jnp.float32)
    gating = jnp.zeros((LENGTH, width), jnp.float32)
    for offset in range(4):
        at = lax.rem(me + offset, 4)
        if offset == 0:
            piece = own_ref[...].astype(jnp.float32)
        elif offset == 1:
            piece = right_ref[...].astype(jnp.float32)
        elif offset == 3:
            piece = left_ref[...].astype(jnp.float32)
        else:
            piece = far_ref[...].astype(jnp.float32)
        squares = squares + jnp.sum(piece * piece, axis=1, keepdims=True)
        scaled = (piece * gain_ref[at]).astype(jnp.bfloat16)
        inner = inner + jnp.dot(scaled, inner_ref[at], preferred_element_type=jnp.float32)
        gating = gating + jnp.dot(scaled, gating_ref[at], preferred_element_type=jnp.float32)
    inverse = lax.rsqrt(squares / D + EPSILON)
    gated = (inner * inverse * jax.nn.sigmoid(gating * inverse)).astype(jnp.bfloat16)
    padded_ref[:LEAD, :] = jnp.zeros((LEAD, width), jnp.float32)
    padded_ref[LEAD:, :] = gated.astype(jnp.float32)
    shift = LEAD - CONV + 1

    def step(n):
        base = n * ROWS_CHUNK
        sums = jnp.zeros((ROWS_CHUNK, 128), jnp.float32)
        square_sums = jnp.zeros((ROWS_CHUNK, 128), jnp.float32)
        for lane in range(0, width, 128):
            total = jnp.zeros((ROWS_CHUNK, 128), jnp.float32)
            for s in range(8):
                part = None
                for j in range(LEAD // 8 + 1):
                    tap = 8 * j + s - shift
                    if tap < 0 or tap >= CONV:
                        continue
                    height = ROWS_CHUNK + (8 if s else 0)
                    term = (
                        padded_ref[pl.ds(base + 8 * j, height), lane : lane + 128]
                        * taps_ref[tap : tap + 1, lane : lane + 128]
                    )
                    part = term if part is None else part + term
                total = total + part[s : s + ROWS_CHUNK]
            out_ref[pl.ds(base, ROWS_CHUNK), lane : lane + 128] = total
            sums = sums + total
            square_sums = square_sums + total * total
        return sums, square_sums

    for n in range(LENGTH // 128):
        pair = [step(2 * n + h) for h in range(2)]
        sums = jnp.concatenate([pair[0][0], pair[1][0]], axis=0)
        square_sums = jnp.concatenate([pair[0][1], pair[1][1]], axis=0)
        stats_ref[0, n : n + 1, :] = jnp.sum(sums.T, axis=0, keepdims=True)
        stats_ref[1, n : n + 1, :] = jnp.sum(square_sums.T, axis=0, keepdims=True)


def token_path(me, own, left, right, far, gain, inner_weight, gating_weight, taps):
    rows, width = own.shape
    grid_spec = pltpu.PrefetchScalarGridSpec(
        num_scalar_prefetch=1,
        grid=(rows // LENGTH,),
        in_specs=[pl.BlockSpec((LENGTH, width), lambda i, m: (i, 0))] * 4
        + [
            whole((4, 1, width)),
            whole((4, width, width)),
            whole((4, width, width)),
            whole((CONV, width)),
        ],
        out_specs=[
            pl.BlockSpec((LENGTH, width), lambda i, m: (i, 0)),
            pl.BlockSpec((None, 2, LENGTH // 128, 128), lambda i, m: (i, 0, 0, 0)),
        ],
        scratch_shapes=[pltpu.VMEM((LEAD + LENGTH, width), jnp.float32)],
    )
    return pl.pallas_call(
        token_kernel,
        grid_spec=grid_spec,
        out_shape=[
            jax.ShapeDtypeStruct((rows, width), jnp.float32),
            jax.ShapeDtypeStruct((rows // LENGTH, 2, LENGTH // 128, 128), jnp.float32),
        ],
        cost_estimate=pl.CostEstimate(
            flops=4 * rows * D * width, transcendentals=rows * width, bytes_accessed=10 << 20
        ),
        name="token_path",
    )(
        me,
        own,
        left,
        right,
        far,
        gain.reshape(4, 1, width),
        inner_weight.reshape(4, width, width),
        gating_weight.reshape(4, width, width),
        taps,
    )


def finish_kernel(conv_ref, stats_ref, gain_ref, out_ref):
    width = conv_ref.shape[1]
    turn = pl.program_id(0)
    for n in range(conv_ref.shape[0] // 128):
        at = turn * (conv_ref.shape[0] // 128) + n
        rows = slice(n * 128, (n + 1) * 128)
        average = stats_ref[0, pl.ds(at, 1), :] / D
        variance = stats_ref[1, pl.ds(at, 1), :] / D - average * average
        spread = lax.rsqrt(variance + EPSILON_NORM)
        average = jnp.broadcast_to(average, (128, 128)).T
        spread = jnp.broadcast_to(spread, (128, 128)).T
        for lane in range(0, width, 128):
            part = slice(lane, lane + 128)
            scaled = (conv_ref[rows, part] - average) * spread * gain_ref[:, part]
            out_ref[rows, part] = scaled * jax.nn.sigmoid(scaled)


def finish(convolved, stats, channel_gain):
    rows, width = convolved.shape
    tile = 512
    return pl.pallas_call(
        finish_kernel,
        grid=(rows // tile,),
        in_specs=[
            pl.BlockSpec((tile, width), lambda i: (i, 0)),
            whole((2, rows // 128, 128)),
            whole((1, width)),
        ],
        out_specs=pl.BlockSpec((tile, width), lambda i: (i, 0)),
        out_shape=jax.ShapeDtypeStruct((rows, width), jnp.float32),
        cost_estimate=pl.CostEstimate(
            flops=8 * rows * width, transcendentals=rows * width, bytes_accessed=4 << 20
        ),
        name="finish",
    )(convolved, stats, channel_gain.reshape(1, width))


def attend_kernel(plane_ref, where_ref, conv_ref, gate_ref, *refs):
    near_ref, far_ref, upper_ref, lower_ref, upper_rest_ref, lower_rest_ref = refs[:6]
    out_ref, held_ref, sems = refs[6:]
    turn = pl.program_id(0)
    count = where_ref.shape[0]
    here = plane_ref[0]
    half = PROWS // 2

    @pl.when(turn == 0)
    def _():
        for n in range(count):
            owner = where_ref[n]
            away = lax.rem(owner // 8 - here + 8, 8)
            column = lax.rem(owner, 8)
            close = (away <= 1) | (away == 7)

            @pl.when(close)
            def _():
                k = jnp.where(away == 7, 1, 2 * away)
                at = pl.multiple_of(k * PROWS, PROWS)
                pltpu.make_async_copy(
                    near_ref.at[column, pl.ds(at, PROWS)], held_ref.at[n], sems.at[n]
                ).start()

            @pl.when(away == 4)
            def _():
                pltpu.make_async_copy(
                    upper_ref.at[column], held_ref.at[n, pl.ds(0, half)], sems.at[n]
                ).start()
                pltpu.make_async_copy(
                    lower_ref.at[column], held_ref.at[n, pl.ds(half, half)], sems.at[n]
                ).start()

            @pl.when((away == 2) | (away == 6))
            def _():
                at = pl.multiple_of(jnp.where(away == 2, PROWS, 0), PROWS)
                pltpu.make_async_copy(
                    far_ref.at[column, pl.ds(at, PROWS)], held_ref.at[n], sems.at[n]
                ).start()

            for side, at, rest_ref in (
                (5, 2 * PROWS, upper_rest_ref),
                (3, 2 * PROWS + KEPT, lower_rest_ref),
            ):

                @pl.when(away == side)
                def _():
                    pltpu.make_async_copy(
                        far_ref.at[column, pl.ds(at, KEPT)],
                        held_ref.at[n, pl.ds(0, KEPT)],
                        sems.at[n],
                    ).start()
                    pltpu.make_async_copy(
                        rest_ref.at[column], held_ref.at[n, pl.ds(KEPT, PROWS - KEPT)], sems.at[n]
                    ).start()

    blocks = conv_ref.shape[0] // BLOCK
    weight = jax.nn.sigmoid(gate_ref[...])
    queries = conv_ref[...].astype(jnp.bfloat16)
    for n in range(blocks * PB):
        at = turn * blocks * PB + n
        pltpu.make_async_copy(
            far_ref.at[0, pl.ds(0, PROWS)], held_ref.at[at], sems.at[at]
        ).wait()
    scores = []
    for b in range(blocks):
        held = held_ref[pl.ds((turn * blocks + b) * PB, PB)].reshape(PB * PROWS, 2 * HEAD)
        rows = slice(b * BLOCK, (b + 1) * BLOCK)
        heads = jnp.concatenate([queries[rows, :HEAD], queries[rows, HEAD:]], axis=0)
        scores.append(
            lax.dot_general(
                heads,
                held[:, :HEAD],
                (((1,), (1,)), ((), ())),
                preferred_element_type=jnp.float32,
            )
            / math.sqrt(HEAD)
        )
    shares = []
    for b in range(blocks):
        raised = jnp.exp(scores[b] - jnp.max(scores[b], axis=1, keepdims=True))
        shares.append((raised / jnp.sum(raised, axis=1, keepdims=True)).astype(jnp.bfloat16))
    for b in range(blocks):
        held = held_ref[pl.ds((turn * blocks + b) * PB, PB)].reshape(PB * PROWS, 2 * HEAD)
        attended = jnp.dot(shares[b], held[:, HEAD:], preferred_element_type=jnp.float32)
        attended = jnp.concatenate([attended[:BLOCK], attended[BLOCK:]], axis=1)
        rows = slice(b * BLOCK, (b + 1) * BLOCK)
        out_ref[rows, :] = (conv_ref[rows, :] + weight * attended).astype(jnp.bfloat16)


def attend(plane, where, conv_out, retrieval_gate, groups):
    rows, width = conv_out.shape
    count = where.shape[0]
    tile = 512
    grid_spec = pltpu.PrefetchScalarGridSpec(
        num_scalar_prefetch=2,
        grid=(rows // tile,),
        in_specs=[
            pl.BlockSpec((tile, width), lambda i, *_: (i, 0)),
            whole((1, width)),
        ]
        + [pl.BlockSpec(memory_space=pl.ANY)] * len(groups),
        out_specs=pl.BlockSpec((tile, width), lambda i, *_: (i, 0)),
        scratch_shapes=[
            pltpu.VMEM((count, PROWS, 2 * HEAD), jnp.bfloat16),
            pltpu.SemaphoreType.DMA((count,)),
        ],
    )
    return pl.pallas_call(
        attend_kernel,
        grid_spec=grid_spec,
        out_shape=jax.ShapeDtypeStruct((rows, width), jnp.bfloat16),
        cost_estimate=pl.CostEstimate(
            flops=4 * rows * 2 * PB * PROWS * HEAD,
            transcendentals=rows * 2 * PB * PROWS,
            bytes_accessed=5 << 20,
        ),
        name="attend",
    )(plane, where, conv_out, retrieval_gate.reshape(1, width), *groups)


def pick_kernel(plane_ref, table_ref, own_ref, below_ref, above_ref, *refs):
    outs, sems = refs[:-1], refs[-1]
    here = plane_ref[0]
    half = PROWS // 2

    def slot(reader_plane, reader, owner_plane):
        at = lax.rem(here + reader_plane + 8, 8) * 8 + reader
        return table_ref[at, lax.rem(here + owner_plane + 8, 8)]

    for reader in range(8):
        at = 0
        for source, reader_plane, owner_plane, first, rows in (
            (own_ref, 0, 0, 0, PROWS),
            (below_ref, 0, -1, 0, PROWS),
            (above_ref, 0, 1, 0, PROWS),
            (below_ref, 3, -1, 0, half),
            (above_ref, -3, 1, half, half),
            (below_ref, 2, -1, KEPT, PROWS - KEPT),
            (above_ref, -2, 1, KEPT, PROWS - KEPT),
        ):
            pltpu.make_async_copy(
                source.at[slot(reader_plane, reader, owner_plane), pl.ds(first, rows)],
                outs[0].at[reader, pl.ds(at, rows)],
                sems.at[0],
            ).start()
            at += rows
    for reader in range(8):
        for n, (source, side, steps, rows) in enumerate(
            (
                (below_ref, 1, 1, PROWS),
                (above_ref, -1, 1, PROWS),
                (below_ref, 1, 2, KEPT),
                (above_ref, -1, 2, KEPT),
            )
        ):
            pltpu.make_async_copy(
                source.at[slot(side * steps, reader, -side), pl.ds(0, rows)],
                outs[1 + n].at[reader],
                sems.at[1 + n],
            ).start()
    for n, out in enumerate(outs):
        pltpu.make_async_copy(out, out, sems.at[n]).wait()


def pick(plane, table, own, below, above):
    shapes = [(8, NEAR_ROWS), (8, PROWS), (8, PROWS), (8, KEPT), (8, KEPT)]
    return pl.pallas_call(
        pick_kernel,
        in_specs=[pl.BlockSpec(memory_space=pltpu.SMEM)] * 2
        + [pl.BlockSpec(memory_space=pltpu.VMEM)] * 3,
        out_specs=[pl.BlockSpec(memory_space=pl.ANY)] * len(shapes),
        scratch_shapes=[pltpu.SemaphoreType.DMA((len(shapes),))],
        out_shape=[
            jax.ShapeDtypeStruct((*shape, 2 * HEAD), jnp.bfloat16) for shape in shapes
        ],
        cost_estimate=pl.CostEstimate(flops=0, transcendentals=0, bytes_accessed=8 << 20),
        name="pick",
    )(plane, table, own, below, above)


def fill_kernel(*refs, at):
    first_ref, second_ref, out_ref, sems = refs[0], refs[1], refs[-2], refs[-1]
    rows = first_ref.shape[1]
    copies = [
        pltpu.make_async_copy(ref, out_ref.at[:, pl.ds(at + n * rows, rows)], sems.at[n])
        for n, ref in enumerate((first_ref, second_ref))
    ]
    for copy in copies:
        copy.start()
    for copy in copies:
        copy.wait()


def fill(first, second, at, into=None):
    held = [] if into is None else [into]
    return pl.pallas_call(
        functools.partial(fill_kernel, at=at),
        in_specs=[pl.BlockSpec(memory_space=pltpu.VMEM)] * 2
        + [pl.BlockSpec(memory_space=pl.ANY)] * len(held),
        out_specs=pl.BlockSpec(memory_space=pl.ANY),
        scratch_shapes=[pltpu.SemaphoreType.DMA((2,))],
        out_shape=jax.ShapeDtypeStruct((8, AWAY_ROWS, 2 * HEAD), jnp.bfloat16),
        input_output_aliases={2: 0} if held else {},
        cost_estimate=pl.CostEstimate(flops=0, transcendentals=0, bytes_accessed=2 << 20),
        name="fill",
    )(first, second, *held)


def shift(value, axis, step):
    return lax.ppermute(value, axis, ring(lax.axis_size(axis), step))


def exchange(value, axes):
    return lax.all_to_all(value, axes, split_axis=0, concat_axis=0, tiled=True)


def layer(
    tokens,
    token_gain,
    inner_weight,
    gating_weight,
    filter_taps,
    channel_gain,
    retrieval_gate,
    passage_store,
    passage_gain,
    keys_weight,
    values_weight,
    owners,
    local_slots,
):
    me = lax.axis_index("tp").astype(jnp.int32).reshape(1)
    plane = lax.axis_index("z").astype(jnp.int32).reshape(1)
    left = shift(tokens, "tp", 1)
    right = shift(tokens, "tp", -1)
    far = shift(tokens, "tp", 2)

    own = project_passages(passage_store, passage_gain, keys_weight, values_weight)
    own = own.reshape(-1, PROWS, 2 * HEAD)
    below = shift(own, "z", 1)
    above = shift(own, "z", -1)

    asked = owners.reshape(-1)
    slots = local_slots.reshape(-1)
    wanted = jnp.sum(
        jnp.where(asked[:, None] == jnp.arange(64, dtype=jnp.int32)[None, :], slots[:, None], 0),
        axis=0,
    )
    wanted = jnp.broadcast_to(wanted.reshape(1, 8, 8).transpose(0, 2, 1), (8, 8, 8))
    table = exchange(wanted.reshape(64, 8), ST)

    near, up1, down1, up2, down2 = pick(plane, table, own, below, above)
    side = ("y", "c")
    near = exchange(near, side)
    up1 = shift(up1, "z", 1)
    down1 = shift(down1, "z", -1)
    up2 = shift(up2, "z", 2)
    down2 = shift(down2, "z", -2)
    away = fill(up1, down1, 0)
    away = fill(up2, down2, 2 * PROWS, away)
    away = exchange(away, side)
    half, rest = PROWS // 2, PROWS - KEPT
    at = 3 * PROWS
    upper = shift(near[:, at : at + half], "z", 3)
    lower = shift(near[:, at + half : at + 2 * half], "z", -3)
    at = 4 * PROWS
    upper_rest = shift(near[:, at : at + rest], "z", 2)
    lower_rest = shift(near[:, at + rest : at + 2 * rest], "z", -2)

    convolved, stats = token_path(
        me,
        tokens,
        left,
        right,
        far,
        token_gain,
        inner_weight,
        gating_weight,
        filter_taps,
    )
    stats = lax.psum(stats, "tp")
    stats = stats.transpose(1, 0, 2, 3).reshape(2, -1, 128)
    conv_out = finish(convolved, stats, channel_gain)
    return attend(plane, asked, conv_out, retrieval_gate, (near, away, upper, lower, upper_rest, lower_rest))


def solution(mesh):
    st, tp = mesh.devices.shape
    fine = Mesh(mesh.devices.reshape(st // 8, 4, 2, tp), ST + ("tp",))
    placed = (
        P(ST, "tp"),
        P(),
        P(None, "tp"),
        P(None, "tp"),
        P(None, "tp"),
        P("tp"),
        P("tp"),
        P(ST, None, None),
        P(),
        P(None, "tp"),
        P(None, "tp"),
        P(ST, None),
        P(ST, None),
    )
    return jax.shard_map(layer, mesh=fine, in_specs=placed, out_specs=P(ST, "tp"), check_vma=False)
```

```python
import functools
import math

import jax
import jax.numpy as jnp
from jax import lax
from jax.experimental import pallas as pl
from jax.experimental.pallas import tpu as pltpu
from jax.sharding import Mesh
from jax.sharding import PartitionSpec as P

D = 2048
HEAD = 256
CONV = 31
LENGTH = 512
BLOCK = 64
PB = 2
PROWS = 64
EPSILON = 1e-06
EPSILON_NORM = 1e-05
ST = ("z", "y", "c")
LEAD = 32
ROWS_CHUNK = 64
KEPT = 56
NEAR_ROWS = 4 * PROWS + 2 * (PROWS - KEPT)
AWAY_ROWS = 2 * PROWS + 2 * KEPT


def ring(size, step):
    return [(i, (i + step) % size) for i in range(size)]


def whole(shape):
    return pl.BlockSpec(shape, lambda *_: (0,) * len(shape))


def project_kernel(rows_ref, gain_ref, keys_ref, values_ref, out_ref):
    rows = rows_ref[...].astype(jnp.float32)
    inverse = lax.rsqrt(jnp.mean(rows * rows, axis=1, keepdims=True) + EPSILON)
    normed = (rows * inverse * gain_ref[...]).astype(jnp.bfloat16)
    out_ref[:, :HEAD] = jnp.dot(normed, keys_ref[...], preferred_element_type=jnp.float32).astype(
        jnp.bfloat16
    )
    out_ref[:, HEAD:] = jnp.dot(
        normed, values_ref[...], preferred_element_type=jnp.float32
    ).astype(jnp.bfloat16)


def project_passages(store, gain, keys_weight, values_weight):
    rows = store.reshape(-1, D)
    count = rows.shape[0]
    tile = 256
    return pl.pallas_call(
        project_kernel,
        grid=(count // tile,),
        in_specs=[
            pl.BlockSpec((tile, D), lambda i: (i, 0)),
            whole((1, D)),
            whole((D, HEAD)),
            whole((D, HEAD)),
        ],
        out_specs=pl.BlockSpec((tile, 2 * HEAD), lambda i: (i, 0)),
        out_shape=jax.ShapeDtypeStruct((count, 2 * HEAD), jnp.bfloat16),
        cost_estimate=pl.CostEstimate(
            flops=4 * count * D * HEAD, transcendentals=0, bytes_accessed=7 << 20
        ),
        name="project_passages",
    )(rows, gain.reshape(1, D), keys_weight, values_weight)


def token_kernel(
    me_ref,
    own_ref,
    left_ref,
    right_ref,
    far_ref,
    gain_ref,
    inner_ref,
    gating_ref,
    taps_ref,
    out_ref,
    stats_ref,
    padded_ref,
):
    me = me_ref[0]
    width = own_ref.shape[1]
    squares = jnp.zeros((LENGTH, 1), jnp.float32)
    inner = jnp.zeros((LENGTH, width), jnp.float32)
    gating = jnp.zeros((LENGTH, width), jnp.float32)
    for offset in range(4):
        at = lax.rem(me + offset, 4)
        if offset == 0:
            piece = own_ref[...].astype(jnp.float32)
        elif offset == 1:
            piece = right_ref[...].astype(jnp.float32)
        elif offset == 3:
            piece = left_ref[...].astype(jnp.float32)
        else:
            piece = far_ref[...].astype(jnp.float32)
        squares = squares + jnp.sum(piece * piece, axis=1, keepdims=True)
        scaled = (piece * gain_ref[at]).astype(jnp.bfloat16)
        inner = inner + jnp.dot(scaled, inner_ref[at], preferred_element_type=jnp.float32)
        gating = gating + jnp.dot(scaled, gating_ref[at], preferred_element_type=jnp.float32)
    inverse = lax.rsqrt(squares / D + EPSILON)
    gated = (inner * inverse * jax.nn.sigmoid(gating * inverse)).astype(jnp.bfloat16)
    padded_ref[:LEAD, :] = jnp.zeros((LEAD, width), jnp.float32)
    padded_ref[LEAD:, :] = gated.astype(jnp.float32)
    shift = LEAD - CONV + 1

    def step(n):
        base = n * ROWS_CHUNK
        sums = jnp.zeros((ROWS_CHUNK, 128), jnp.float32)
        square_sums = jnp.zeros((ROWS_CHUNK, 128), jnp.float32)
        for lane in range(0, width, 128):
            total = jnp.zeros((ROWS_CHUNK, 128), jnp.float32)
            for s in range(8):
                part = None
                for j in range(LEAD // 8 + 1):
                    tap = 8 * j + s - shift
                    if tap < 0 or tap >= CONV:
                        continue
                    height = ROWS_CHUNK + (8 if s else 0)
                    term = (
                        padded_ref[pl.ds(base + 8 * j, height), lane : lane + 128]
                        * taps_ref[tap : tap + 1, lane : lane + 128]
                    )
                    part = term if part is None else part + term
                total = total + part[s : s + ROWS_CHUNK]
            out_ref[pl.ds(base, ROWS_CHUNK), lane : lane + 128] = total
            sums = sums + total
            square_sums = square_sums + total * total
        return sums, square_sums

    for n in range(LENGTH // 128):
        pair = [step(2 * n + h) for h in range(2)]
        sums = jnp.concatenate([pair[0][0], pair[1][0]], axis=0)
        square_sums = jnp.concatenate([pair[0][1], pair[1][1]], axis=0)
        stats_ref[0, n : n + 1, :] = jnp.sum(sums.T, axis=0, keepdims=True)
        stats_ref[1, n : n + 1, :] = jnp.sum(square_sums.T, axis=0, keepdims=True)


def token_path(me, own, left, right, far, gain, inner_weight, gating_weight, taps):
    rows, width = own.shape
    grid_spec = pltpu.PrefetchScalarGridSpec(
        num_scalar_prefetch=1,
        grid=(rows // LENGTH,),
        in_specs=[pl.BlockSpec((LENGTH, width), lambda i, m: (i, 0))] * 4
        + [
            whole((4, 1, width)),
            whole((4, width, width)),
            whole((4, width, width)),
            whole((CONV, width)),
        ],
        out_specs=[
            pl.BlockSpec((LENGTH, width), lambda i, m: (i, 0)),
            pl.BlockSpec((None, 2, LENGTH // 128, 128), lambda i, m: (i, 0, 0, 0)),
        ],
        scratch_shapes=[pltpu.VMEM((LEAD + LENGTH, width), jnp.float32)],
    )
    return pl.pallas_call(
        token_kernel,
        grid_spec=grid_spec,
        out_shape=[
            jax.ShapeDtypeStruct((rows, width), jnp.float32),
            jax.ShapeDtypeStruct((rows // LENGTH, 2, LENGTH // 128, 128), jnp.float32),
        ],
        cost_estimate=pl.CostEstimate(
            flops=4 * rows * D * width, transcendentals=rows * width, bytes_accessed=10 << 20
        ),
        name="token_path",
    )(
        me,
        own,
        left,
        right,
        far,
        gain.reshape(4, 1, width),
        inner_weight.reshape(4, width, width),
        gating_weight.reshape(4, width, width),
        taps,
    )


def finish_kernel(conv_ref, stats_ref, gain_ref, out_ref):
    width = conv_ref.shape[1]
    turn = pl.program_id(0)
    for n in range(conv_ref.shape[0] // 128):
        at = turn * (conv_ref.shape[0] // 128) + n
        rows = slice(n * 128, (n + 1) * 128)
        average = stats_ref[0, pl.ds(at, 1), :] / D
        variance = stats_ref[1, pl.ds(at, 1), :] / D - average * average
        spread = lax.rsqrt(variance + EPSILON_NORM)
        average = jnp.broadcast_to(average, (128, 128)).T
        spread = jnp.broadcast_to(spread, (128, 128)).T
        for lane in range(0, width, 128):
            part = slice(lane, lane + 128)
            scaled = (conv_ref[rows, part] - average) * spread * gain_ref[:, part]
            out_ref[rows, part] = scaled * jax.nn.sigmoid(scaled)


def finish(convolved, stats, channel_gain):
    rows, width = convolved.shape
    tile = 512
    return pl.pallas_call(
        finish_kernel,
        grid=(rows // tile,),
        in_specs=[
            pl.BlockSpec((tile, width), lambda i: (i, 0)),
            whole((2, rows // 128, 128)),
            whole((1, width)),
        ],
        out_specs=pl.BlockSpec((tile, width), lambda i: (i, 0)),
        out_shape=jax.ShapeDtypeStruct((rows, width), jnp.float32),
        cost_estimate=pl.CostEstimate(
            flops=8 * rows * width, transcendentals=rows * width, bytes_accessed=4 << 20
        ),
        name="finish",
    )(convolved, stats, channel_gain.reshape(1, width))


def attend_kernel(plane_ref, where_ref, conv_ref, gate_ref, *refs):
    near_ref, far_ref, upper_ref, lower_ref, out_ref, held_ref, sems = refs
    turn = pl.program_id(0)
    count = where_ref.shape[0]
    here = plane_ref[0]
    half = PROWS // 2

    @pl.when(turn == 0)
    def _():
        for n in range(count):
            owner = where_ref[n]
            away = lax.rem(owner // 8 - here + 8, 8)
            column = lax.rem(owner, 8)
            close = (away <= 1) | (away == 7)

            @pl.when(close)
            def _():
                k = jnp.where(away == 7, 1, 2 * away)
                at = pl.multiple_of(k * PROWS, PROWS)
                pltpu.make_async_copy(
                    near_ref.at[column, pl.ds(at, PROWS)], held_ref.at[n], sems.at[n]
                ).start()

            @pl.when(away == 4)
            def _():
                pltpu.make_async_copy(
                    upper_ref.at[column, pl.ds(0, half)],
                    held_ref.at[n, pl.ds(0, half)],
                    sems.at[n],
                ).start()
                pltpu.make_async_copy(
                    lower_ref.at[column, pl.ds(0, half)],
                    held_ref.at[n, pl.ds(half, half)],
                    sems.at[n],
                ).start()

            @pl.when((away == 2) | (away == 6))
            def _():
                at = pl.multiple_of(jnp.where(away == 2, PROWS, 0), PROWS)
                pltpu.make_async_copy(
                    far_ref.at[column, pl.ds(at, PROWS)], held_ref.at[n], sems.at[n]
                ).start()

            for side, at, rest_ref in (
                (5, 2 * PROWS, upper_ref),
                (3, 2 * PROWS + KEPT, lower_ref),
            ):

                @pl.when(away == side)
                def _():
                    pltpu.make_async_copy(
                        far_ref.at[column, pl.ds(at, KEPT)],
                        held_ref.at[n, pl.ds(0, KEPT)],
                        sems.at[n],
                    ).start()
                    pltpu.make_async_copy(
                        rest_ref.at[column, pl.ds(half, PROWS - KEPT)],
                        held_ref.at[n, pl.ds(KEPT, PROWS - KEPT)],
                        sems.at[n],
                    ).start()

    blocks = conv_ref.shape[0] // BLOCK
    weight = jax.nn.sigmoid(gate_ref[...])
    queries = conv_ref[...].astype(jnp.bfloat16)
    for n in range(blocks * PB):
        at = turn * blocks * PB + n
        pltpu.make_async_copy(
            far_ref.at[0, pl.ds(0, PROWS)], held_ref.at[at], sems.at[at]
        ).wait()
    scores = []
    for b in range(blocks):
        held = held_ref[pl.ds((turn * blocks + b) * PB, PB)].reshape(PB * PROWS, 2 * HEAD)
        rows = slice(b * BLOCK, (b + 1) * BLOCK)
        heads = jnp.concatenate([queries[rows, :HEAD], queries[rows, HEAD:]], axis=0)
        scores.append(
            lax.dot_general(
                heads,
                held[:, :HEAD],
                (((1,), (1,)), ((), ())),
                preferred_element_type=jnp.float32,
            )
            / math.sqrt(HEAD)
        )
    shares = []
    for b in range(blocks):
        raised = jnp.exp(scores[b] - jnp.max(scores[b], axis=1, keepdims=True))
        shares.append((raised / jnp.sum(raised, axis=1, keepdims=True)).astype(jnp.bfloat16))
    for b in range(blocks):
        held = held_ref[pl.ds((turn * blocks + b) * PB, PB)].reshape(PB * PROWS, 2 * HEAD)
        attended = jnp.dot(shares[b], held[:, HEAD:], preferred_element_type=jnp.float32)
        attended = jnp.concatenate([attended[:BLOCK], attended[BLOCK:]], axis=1)
        rows = slice(b * BLOCK, (b + 1) * BLOCK)
        out_ref[rows, :] = (conv_ref[rows, :] + weight * attended).astype(jnp.bfloat16)


def attend(plane, where, conv_out, retrieval_gate, groups):
    rows, width = conv_out.shape
    count = where.shape[0]
    tile = 512
    grid_spec = pltpu.PrefetchScalarGridSpec(
        num_scalar_prefetch=2,
        grid=(rows // tile,),
        in_specs=[
            pl.BlockSpec((tile, width), lambda i, *_: (i, 0)),
            whole((1, width)),
        ]
        + [pl.BlockSpec(memory_space=pl.ANY)] * len(groups),
        out_specs=pl.BlockSpec((tile, width), lambda i, *_: (i, 0)),
        scratch_shapes=[
            pltpu.VMEM((count, PROWS, 2 * HEAD), jnp.bfloat16),
            pltpu.SemaphoreType.DMA((count,)),
        ],
    )
    return pl.pallas_call(
        attend_kernel,
        grid_spec=grid_spec,
        out_shape=jax.ShapeDtypeStruct((rows, width), jnp.bfloat16),
        cost_estimate=pl.CostEstimate(
            flops=4 * rows * 2 * PB * PROWS * HEAD,
            transcendentals=rows * 2 * PB * PROWS,
            bytes_accessed=5 << 20,
        ),
        name="attend",
    )(plane, where, conv_out, retrieval_gate.reshape(1, width), *groups)


def pick_kernel(plane_ref, table_ref, own_ref, below_ref, above_ref, *refs):
    outs, sems = refs[:-1], refs[-1]
    here = plane_ref[0]
    half = PROWS // 2

    def slot(reader_plane, reader, owner_plane):
        at = lax.rem(here + reader_plane + 8, 8) * 8 + reader
        return table_ref[at, lax.rem(here + owner_plane + 8, 8)]

    for reader in range(8):
        at = 0
        for source, reader_plane, owner_plane, first, rows in (
            (own_ref, 0, 0, 0, PROWS),
            (below_ref, 0, -1, 0, PROWS),
            (above_ref, 0, 1, 0, PROWS),
            (below_ref, 3, -1, 0, half),
            (own_ref, 3, 0, KEPT, PROWS - KEPT),
            (above_ref, -3, 1, half, half),
            (own_ref, -3, 0, KEPT, PROWS - KEPT),
        ):
            pltpu.make_async_copy(
                source.at[slot(reader_plane, reader, owner_plane), pl.ds(first, rows)],
                outs[0].at[reader, pl.ds(at, rows)],
                sems.at[0],
            ).start()
            at += rows
    for reader in range(8):
        for n, (source, side, steps, rows) in enumerate(
            (
                (below_ref, 1, 1, PROWS),
                (above_ref, -1, 1, PROWS),
                (below_ref, 1, 2, KEPT),
                (above_ref, -1, 2, KEPT),
            )
        ):
            pltpu.make_async_copy(
                source.at[slot(side * steps, reader, -side), pl.ds(0, rows)],
                outs[1 + n].at[reader],
                sems.at[1 + n],
            ).start()
    for n, out in enumerate(outs):
        pltpu.make_async_copy(out, out, sems.at[n]).wait()


def pick(plane, table, own, below, above):
    shapes = [(8, NEAR_ROWS), (8, PROWS), (8, PROWS), (8, KEPT), (8, KEPT)]
    return pl.pallas_call(
        pick_kernel,
        in_specs=[pl.BlockSpec(memory_space=pltpu.SMEM)] * 2
        + [pl.BlockSpec(memory_space=pltpu.VMEM)] * 3,
        out_specs=[pl.BlockSpec(memory_space=pl.ANY)] * len(shapes),
        scratch_shapes=[pltpu.SemaphoreType.DMA((len(shapes),))],
        out_shape=[
            jax.ShapeDtypeStruct((*shape, 2 * HEAD), jnp.bfloat16) for shape in shapes
        ],
        cost_estimate=pl.CostEstimate(flops=0, transcendentals=0, bytes_accessed=8 << 20),
        name="pick",
    )(plane, table, own, below, above)


def fill_kernel(*refs, at):
    first_ref, second_ref, out_ref, sems = refs[0], refs[1], refs[-2], refs[-1]
    rows = first_ref.shape[1]
    copies = [
        pltpu.make_async_copy(ref, out_ref.at[:, pl.ds(at + n * rows, rows)], sems.at[n])
        for n, ref in enumerate((first_ref, second_ref))
    ]
    for copy in copies:
        copy.start()
    for copy in copies:
        copy.wait()


def fill(first, second, at, into=None):
    held = [] if into is None else [into]
    return pl.pallas_call(
        functools.partial(fill_kernel, at=at),
        in_specs=[pl.BlockSpec(memory_space=pltpu.VMEM)] * 2
        + [pl.BlockSpec(memory_space=pl.ANY)] * len(held),
        out_specs=pl.BlockSpec(memory_space=pl.ANY),
        scratch_shapes=[pltpu.SemaphoreType.DMA((2,))],
        out_shape=jax.ShapeDtypeStruct((8, AWAY_ROWS, 2 * HEAD), jnp.bfloat16),
        input_output_aliases={2: 0} if held else {},
        cost_estimate=pl.CostEstimate(flops=0, transcendentals=0, bytes_accessed=2 << 20),
        name="fill",
    )(first, second, *held)


def shift(value, axis, step):
    return lax.ppermute(value, axis, ring(lax.axis_size(axis), step))


def exchange(value, axes):
    return lax.all_to_all(value, axes, split_axis=0, concat_axis=0, tiled=True)


def layer(
    tokens,
    token_gain,
    inner_weight,
    gating_weight,
    filter_taps,
    channel_gain,
    retrieval_gate,
    passage_store,
    passage_gain,
    keys_weight,
    values_weight,
    owners,
    local_slots,
):
    me = lax.axis_index("tp").astype(jnp.int32).reshape(1)
    plane = lax.axis_index("z").astype(jnp.int32).reshape(1)
    left = shift(tokens, "tp", 1)
    right = shift(tokens, "tp", -1)
    far = shift(tokens, "tp", 2)

    own = project_passages(passage_store, passage_gain, keys_weight, values_weight)
    own = own.reshape(-1, PROWS, 2 * HEAD)
    below = shift(own, "z", 1)
    above = shift(own, "z", -1)

    asked = owners.reshape(-1)
    slots = local_slots.reshape(-1)
    wanted = jnp.sum(
        jnp.where(asked[:, None] == jnp.arange(64, dtype=jnp.int32)[None, :], slots[:, None], 0),
        axis=0,
    )
    wanted = jnp.broadcast_to(wanted.reshape(1, 8, 8).transpose(0, 2, 1), (8, 8, 8))
    table = exchange(wanted.reshape(64, 8), ST)

    near, up1, down1, up2, down2 = pick(plane, table, own, below, above)
    side = ("y", "c")
    near = exchange(near, side)
    up1 = shift(up1, "z", 1)
    down1 = shift(down1, "z", -1)
    up2 = shift(up2, "z", 2)
    down2 = shift(down2, "z", -2)
    away = fill(up1, down1, 0)
    away = fill(up2, down2, 2 * PROWS, away)
    away = exchange(away, side)
    split = (3 * PROWS + NEAR_ROWS) // 2
    upper = shift(near[:, 3 * PROWS : split], "z", 3)
    lower = shift(near[:, split:], "z", -3)

    convolved, stats = token_path(
        me,
        tokens,
        left,
        right,
        far,
        token_gain,
        inner_weight,
        gating_weight,
        filter_taps,
    )
    stats = lax.psum(stats, "tp")
    stats = stats.transpose(1, 0, 2, 3).reshape(2, -1, 128)
    conv_out = finish(convolved, stats, channel_gain)
    return attend(plane, asked, conv_out, retrieval_gate, (near, away, upper, lower))


def solution(mesh):
    st, tp = mesh.devices.shape
    fine = Mesh(mesh.devices.reshape(st // 8, 4, 2, tp), ST + ("tp",))
    placed = (
        P(ST, "tp"),
        P(),
        P(None, "tp"),
        P(None, "tp"),
        P(None, "tp"),
        P("tp"),
        P("tp"),
        P(ST, None, None),
        P(),
        P(None, "tp"),
        P(None, "tp"),
        P(ST, None),
        P(ST, None),
    )
    return jax.shard_map(layer, mesh=fine, in_specs=placed, out_specs=P(ST, "tp"), check_vma=False)
```

```python
import functools
import math

import jax
import jax.numpy as jnp
from jax import lax
from jax.experimental import pallas as pl
from jax.experimental.pallas import tpu as pltpu
from jax.sharding import Mesh
from jax.sharding import PartitionSpec as P

D = 2048
HEAD = 256
CONV = 31
LENGTH = 512
BLOCK = 64
PB = 2
PROWS = 64
EPSILON = 1e-06
EPSILON_NORM = 1e-05
ST = ("z", "y", "c")
LEAD = 32
ROWS_CHUNK = 64
KEPT = 56
NEAR_ROWS = 4 * PROWS + 2 * (PROWS - KEPT)
AWAY_ROWS = 2 * PROWS + 2 * KEPT


def ring(size, step):
    return [(i, (i + step) % size) for i in range(size)]


def in_vmem(*values):
    return [pltpu.with_memory_space_constraint(value, pltpu.VMEM) for value in values]


def in_hbm(*values):
    return [pltpu.with_memory_space_constraint(value, pltpu.HBM) for value in values]


def whole(shape):
    return pl.BlockSpec(shape, lambda *_: (0,) * len(shape))


def project_kernel(rows_ref, gain_ref, keys_ref, values_ref, out_ref):
    rows = rows_ref[...].astype(jnp.float32)
    inverse = lax.rsqrt(jnp.mean(rows * rows, axis=1, keepdims=True) + EPSILON)
    normed = (rows * inverse * gain_ref[...]).astype(jnp.bfloat16)
    out_ref[:, :HEAD] = jnp.dot(normed, keys_ref[...], preferred_element_type=jnp.float32).astype(
        jnp.bfloat16
    )
    out_ref[:, HEAD:] = jnp.dot(
        normed, values_ref[...], preferred_element_type=jnp.float32
    ).astype(jnp.bfloat16)


def project_passages(store, gain, keys_weight, values_weight):
    rows = store.reshape(-1, D)
    count = rows.shape[0]
    tile = 256
    return pl.pallas_call(
        project_kernel,
        grid=(count // tile,),
        in_specs=[
            pl.BlockSpec((tile, D), lambda i: (i, 0)),
            whole((1, D)),
            whole((D, HEAD)),
            whole((D, HEAD)),
        ],
        out_specs=pl.BlockSpec((tile, 2 * HEAD), lambda i: (i, 0)),
        out_shape=jax.ShapeDtypeStruct((count, 2 * HEAD), jnp.bfloat16),
        cost_estimate=pl.CostEstimate(
            flops=4 * count * D * HEAD, transcendentals=0, bytes_accessed=7 << 20
        ),
        compiler_params=pltpu.CompilerParams(vmem_limit_bytes=16 << 20),
        name="project_passages",
    )(*in_hbm(rows), gain.reshape(1, D), *in_hbm(keys_weight, values_weight))


def token_kernel(
    me_ref,
    own_ref,
    left_ref,
    right_ref,
    far_ref,
    gain_ref,
    inner_ref,
    gating_ref,
    taps_ref,
    out_ref,
    stats_ref,
    padded_ref,
):
    me = me_ref[0]
    width = own_ref.shape[1]
    squares = jnp.zeros((LENGTH, 1), jnp.float32)
    inner = jnp.zeros((LENGTH, width), jnp.float32)
    gating = jnp.zeros((LENGTH, width), jnp.float32)
    for offset in range(4):
        at = lax.rem(me + offset, 4)
        if offset == 0:
            piece = own_ref[...].astype(jnp.float32)
        elif offset == 1:
            piece = right_ref[...].astype(jnp.float32)
        elif offset == 3:
            piece = left_ref[...].astype(jnp.float32)
        else:
            piece = far_ref[...].astype(jnp.float32)
        squares = squares + jnp.sum(piece * piece, axis=1, keepdims=True)
        scaled = (piece * gain_ref[at]).astype(jnp.bfloat16)
        inner = inner + jnp.dot(scaled, inner_ref[at], preferred_element_type=jnp.float32)
        gating = gating + jnp.dot(scaled, gating_ref[at], preferred_element_type=jnp.float32)
    inverse = lax.rsqrt(squares / D + EPSILON)
    gated = (inner * inverse * jax.nn.sigmoid(gating * inverse)).astype(jnp.bfloat16)
    padded_ref[:LEAD, :] = jnp.zeros((LEAD, width), jnp.float32)
    padded_ref[LEAD:, :] = gated.astype(jnp.float32)
    shift = LEAD - CONV + 1

    def step(n):
        base = n * ROWS_CHUNK
        sums = jnp.zeros((ROWS_CHUNK, 128), jnp.float32)
        square_sums = jnp.zeros((ROWS_CHUNK, 128), jnp.float32)
        for lane in range(0, width, 128):
            total = jnp.zeros((ROWS_CHUNK, 128), jnp.float32)
            for s in range(8):
                part = None
                for j in range(LEAD // 8 + 1):
                    tap = 8 * j + s - shift
                    if tap < 0 or tap >= CONV:
                        continue
                    height = ROWS_CHUNK + (8 if s else 0)
                    term = (
                        padded_ref[pl.ds(base + 8 * j, height), lane : lane + 128]
                        * taps_ref[tap : tap + 1, lane : lane + 128]
                    )
                    part = term if part is None else part + term
                total = total + part[s : s + ROWS_CHUNK]
            out_ref[pl.ds(base, ROWS_CHUNK), lane : lane + 128] = total
            sums = sums + total
            square_sums = square_sums + total * total
        return sums, square_sums

    for n in range(LENGTH // 128):
        pair = [step(2 * n + h) for h in range(2)]
        sums = jnp.concatenate([pair[0][0], pair[1][0]], axis=0)
        square_sums = jnp.concatenate([pair[0][1], pair[1][1]], axis=0)
        stats_ref[0, n : n + 1, :] = jnp.sum(sums.T, axis=0, keepdims=True)
        stats_ref[1, n : n + 1, :] = jnp.sum(square_sums.T, axis=0, keepdims=True)


def token_path(me, own, left, right, far, gain, inner_weight, gating_weight, taps):
    rows, width = own.shape
    grid_spec = pltpu.PrefetchScalarGridSpec(
        num_scalar_prefetch=1,
        grid=(rows // LENGTH,),
        in_specs=[pl.BlockSpec((LENGTH, width), lambda i, m: (i, 0))] * 4
        + [
            whole((4, 1, width)),
            whole((4, width, width)),
            whole((4, width, width)),
            whole((CONV, width)),
        ],
        out_specs=[
            pl.BlockSpec((LENGTH, width), lambda i, m: (i, 0)),
            pl.BlockSpec((None, 2, LENGTH // 128, 128), lambda i, m: (i, 0, 0, 0)),
        ],
        scratch_shapes=[pltpu.VMEM((LEAD + LENGTH, width), jnp.float32)],
    )
    return pl.pallas_call(
        token_kernel,
        grid_spec=grid_spec,
        out_shape=[
            pltpu.HBM((rows, width), jnp.float32),
            jax.ShapeDtypeStruct((rows // LENGTH, 2, LENGTH // 128, 128), jnp.float32),
        ],
        cost_estimate=pl.CostEstimate(
            flops=4 * rows * D * width, transcendentals=rows * width, bytes_accessed=10 << 20
        ),
        compiler_params=pltpu.CompilerParams(vmem_limit_bytes=40 << 20),
        name="token_path",
    )(
        me,
        *in_hbm(
            own,
            left,
            right,
            far,
            gain.reshape(4, 1, width),
            inner_weight.reshape(4, width, width),
            gating_weight.reshape(4, width, width),
            taps,
        ),
    )


def finish_kernel(conv_ref, stats_ref, gain_ref, out_ref):
    width = conv_ref.shape[1]
    turn = pl.program_id(0)
    for n in range(conv_ref.shape[0] // 128):
        at = turn * (conv_ref.shape[0] // 128) + n
        rows = slice(n * 128, (n + 1) * 128)
        average = stats_ref[0, pl.ds(at, 1), :] / D
        variance = stats_ref[1, pl.ds(at, 1), :] / D - average * average
        spread = lax.rsqrt(variance + EPSILON_NORM)
        average = jnp.broadcast_to(average, (128, 128)).T
        spread = jnp.broadcast_to(spread, (128, 128)).T
        for lane in range(0, width, 128):
            part = slice(lane, lane + 128)
            scaled = (conv_ref[rows, part] - average) * spread * gain_ref[:, part]
            out_ref[rows, part] = scaled * jax.nn.sigmoid(scaled)


def finish(convolved, stats, channel_gain):
    rows, width = convolved.shape
    tile = 512
    return pl.pallas_call(
        finish_kernel,
        grid=(rows // tile,),
        in_specs=[
            pl.BlockSpec((tile, width), lambda i: (i, 0)),
            whole((2, rows // 128, 128)),
            whole((1, width)),
        ],
        out_specs=pl.BlockSpec((tile, width), lambda i: (i, 0)),
        out_shape=pltpu.HBM((rows, width), jnp.float32),
        cost_estimate=pl.CostEstimate(
            flops=8 * rows * width, transcendentals=rows * width, bytes_accessed=4 << 20
        ),
        compiler_params=pltpu.CompilerParams(vmem_limit_bytes=14 << 20),
        name="finish",
    )(*in_hbm(convolved), stats, channel_gain.reshape(1, width))


def attend_kernel(plane_ref, where_ref, conv_ref, gate_ref, *refs):
    near_ref, far_ref, upper_ref, lower_ref, out_ref, held_ref, sems = refs
    turn = pl.program_id(0)
    count = where_ref.shape[0]
    here = plane_ref[0]
    half = PROWS // 2

    @pl.when(turn == 0)
    def _():
        for n in range(count):
            owner = where_ref[n]
            away = lax.rem(owner // 8 - here + 8, 8)
            column = lax.rem(owner, 8)
            close = (away <= 1) | (away == 7)

            @pl.when(close)
            def _():
                k = jnp.where(away == 7, 1, 2 * away)
                at = pl.multiple_of(k * PROWS, PROWS)
                pltpu.make_async_copy(
                    near_ref.at[column, pl.ds(at, PROWS)], held_ref.at[n], sems.at[n]
                ).start()

            @pl.when(away == 4)
            def _():
                pltpu.make_async_copy(
                    upper_ref.at[column, pl.ds(0, half)],
                    held_ref.at[n, pl.ds(0, half)],
                    sems.at[n],
                ).start()
                pltpu.make_async_copy(
                    lower_ref.at[column, pl.ds(0, half)],
                    held_ref.at[n, pl.ds(half, half)],
                    sems.at[n],
                ).start()

            @pl.when((away == 2) | (away == 6))
            def _():
                at = pl.multiple_of(jnp.where(away == 2, PROWS, 0), PROWS)
                pltpu.make_async_copy(
                    far_ref.at[column, pl.ds(at, PROWS)], held_ref.at[n], sems.at[n]
                ).start()

            for side, at, rest_ref in (
                (5, 2 * PROWS, upper_ref),
                (3, 2 * PROWS + KEPT, lower_ref),
            ):

                @pl.when(away == side)
                def _():
                    pltpu.make_async_copy(
                        far_ref.at[column, pl.ds(at, KEPT)],
                        held_ref.at[n, pl.ds(0, KEPT)],
                        sems.at[n],
                    ).start()
                    pltpu.make_async_copy(
                        rest_ref.at[column, pl.ds(half, PROWS - KEPT)],
                        held_ref.at[n, pl.ds(KEPT, PROWS - KEPT)],
                        sems.at[n],
                    ).start()

    blocks = conv_ref.shape[0] // BLOCK
    weight = jax.nn.sigmoid(gate_ref[...])
    queries = conv_ref[...].astype(jnp.bfloat16)
    for n in range(blocks * PB):
        at = turn * blocks * PB + n
        pltpu.make_async_copy(
            far_ref.at[0, pl.ds(0, PROWS)], held_ref.at[at], sems.at[at]
        ).wait()
    scores = []
    for b in range(blocks):
        held = held_ref[pl.ds((turn * blocks + b) * PB, PB)].reshape(PB * PROWS, 2 * HEAD)
        rows = slice(b * BLOCK, (b + 1) * BLOCK)
        heads = jnp.concatenate([queries[rows, :HEAD], queries[rows, HEAD:]], axis=0)
        scores.append(
            lax.dot_general(
                heads,
                held[:, :HEAD],
                (((1,), (1,)), ((), ())),
                preferred_element_type=jnp.float32,
            )
            / math.sqrt(HEAD)
        )
    shares = []
    for b in range(blocks):
        raised = jnp.exp(scores[b] - jnp.max(scores[b], axis=1, keepdims=True))
        shares.append((raised / jnp.sum(raised, axis=1, keepdims=True)).astype(jnp.bfloat16))
    for b in range(blocks):
        held = held_ref[pl.ds((turn * blocks + b) * PB, PB)].reshape(PB * PROWS, 2 * HEAD)
        attended = jnp.dot(shares[b], held[:, HEAD:], preferred_element_type=jnp.float32)
        attended = jnp.concatenate([attended[:BLOCK], attended[BLOCK:]], axis=1)
        rows = slice(b * BLOCK, (b + 1) * BLOCK)
        out_ref[rows, :] = (conv_ref[rows, :] + weight * attended).astype(jnp.bfloat16)


def attend(plane, where, conv_out, retrieval_gate, groups):
    rows, width = conv_out.shape
    count = where.shape[0]
    tile = 512
    grid_spec = pltpu.PrefetchScalarGridSpec(
        num_scalar_prefetch=2,
        grid=(rows // tile,),
        in_specs=[
            pl.BlockSpec((tile, width), lambda i, *_: (i, 0)),
            whole((1, width)),
        ]
        + [pl.BlockSpec(memory_space=pl.ANY)] * len(groups),
        out_specs=pl.BlockSpec((tile, width), lambda i, *_: (i, 0)),
        scratch_shapes=[
            pltpu.VMEM((count, PROWS, 2 * HEAD), jnp.bfloat16),
            pltpu.SemaphoreType.DMA((count,)),
        ],
    )
    return pl.pallas_call(
        attend_kernel,
        grid_spec=grid_spec,
        out_shape=jax.ShapeDtypeStruct((rows, width), jnp.bfloat16),
        cost_estimate=pl.CostEstimate(
            flops=4 * rows * 2 * PB * PROWS * HEAD,
            transcendentals=rows * 2 * PB * PROWS,
            bytes_accessed=5 << 20,
        ),
        compiler_params=pltpu.CompilerParams(vmem_limit_bytes=16 << 20),
        name="attend",
    )(plane, where, *in_hbm(conv_out), retrieval_gate.reshape(1, width), *in_vmem(*groups))


def pick_kernel(plane_ref, table_ref, own_ref, below_ref, above_ref, *refs):
    outs, sems = refs[:-1], refs[-1]
    here = plane_ref[0]
    half = PROWS // 2

    def slot(reader_plane, reader, owner_plane):
        at = lax.rem(here + reader_plane + 8, 8) * 8 + reader
        return table_ref[at, lax.rem(here + owner_plane + 8, 8)]

    for reader in range(8):
        at = 0
        for source, reader_plane, owner_plane, first, rows in (
            (own_ref, 0, 0, 0, PROWS),
            (below_ref, 0, -1, 0, PROWS),
            (above_ref, 0, 1, 0, PROWS),
            (below_ref, 3, -1, 0, half),
            (own_ref, 3, 0, KEPT, PROWS - KEPT),
            (above_ref, -3, 1, half, half),
            (own_ref, -3, 0, KEPT, PROWS - KEPT),
        ):
            pltpu.make_async_copy(
                source.at[slot(reader_plane, reader, owner_plane), pl.ds(first, rows)],
                outs[0].at[reader, pl.ds(at, rows)],
                sems.at[0],
            ).start()
            at += rows
    for reader in range(8):
        for n, (source, side, steps, rows) in enumerate(
            (
                (below_ref, 1, 1, PROWS),
                (above_ref, -1, 1, PROWS),
                (below_ref, 1, 2, KEPT),
                (above_ref, -1, 2, KEPT),
            )
        ):
            pltpu.make_async_copy(
                source.at[slot(side * steps, reader, -side), pl.ds(0, rows)],
                outs[1 + n].at[reader],
                sems.at[1 + n],
            ).start()
    for n, out in enumerate(outs):
        pltpu.make_async_copy(out, out, sems.at[n]).wait()


def pick(plane, table, own, below, above):
    shapes = [(8, NEAR_ROWS), (8, PROWS), (8, PROWS), (8, KEPT), (8, KEPT)]
    return pl.pallas_call(
        pick_kernel,
        in_specs=[pl.BlockSpec(memory_space=pltpu.SMEM)] * 2
        + [pl.BlockSpec(memory_space=pl.ANY)] * 3,
        out_specs=[pl.BlockSpec(memory_space=pl.ANY)] * len(shapes),
        scratch_shapes=[pltpu.SemaphoreType.DMA((len(shapes),))],
        out_shape=[
            pltpu.HBM((*shape, 2 * HEAD), jnp.bfloat16) for shape in shapes
        ],
        cost_estimate=pl.CostEstimate(flops=0, transcendentals=0, bytes_accessed=8 << 20),
        compiler_params=pltpu.CompilerParams(vmem_limit_bytes=2 << 20),
        name="pick",
    )(plane, table, *in_vmem(own, below, above))


def fill_kernel(*refs, at):
    first_ref, second_ref, out_ref, sems = refs[0], refs[1], refs[-2], refs[-1]
    rows = first_ref.shape[1]
    copies = [
        pltpu.make_async_copy(ref, out_ref.at[:, pl.ds(at + n * rows, rows)], sems.at[n])
        for n, ref in enumerate((first_ref, second_ref))
    ]
    for copy in copies:
        copy.start()
    for copy in copies:
        copy.wait()


def fill(first, second, at, into=None):
    held = [] if into is None else [into]
    return pl.pallas_call(
        functools.partial(fill_kernel, at=at),
        in_specs=[pl.BlockSpec(memory_space=pl.ANY)] * (2 + len(held)),
        out_specs=pl.BlockSpec(memory_space=pl.ANY),
        scratch_shapes=[pltpu.SemaphoreType.DMA((2,))],
        out_shape=pltpu.HBM((8, AWAY_ROWS, 2 * HEAD), jnp.bfloat16),
        input_output_aliases={2: 0} if held else {},
        cost_estimate=pl.CostEstimate(flops=0, transcendentals=0, bytes_accessed=2 << 20),
        compiler_params=pltpu.CompilerParams(vmem_limit_bytes=2 << 20),
        name="fill",
    )(*in_vmem(first, second), *in_hbm(*held))


def shift(value, axis, step):
    return lax.ppermute(value, axis, ring(lax.axis_size(axis), step))


def exchange(value, axes):
    return lax.all_to_all(value, axes, split_axis=0, concat_axis=0, tiled=True)


def layer(
    tokens,
    token_gain,
    inner_weight,
    gating_weight,
    filter_taps,
    channel_gain,
    retrieval_gate,
    passage_store,
    passage_gain,
    keys_weight,
    values_weight,
    owners,
    local_slots,
):
    me = lax.axis_index("tp").astype(jnp.int32).reshape(1)
    plane = lax.axis_index("z").astype(jnp.int32).reshape(1)
    left = shift(tokens, "tp", 1)
    right = shift(tokens, "tp", -1)
    far = shift(tokens, "tp", 2)

    own = project_passages(passage_store, passage_gain, keys_weight, values_weight)
    own = own.reshape(-1, PROWS, 2 * HEAD)
    below = shift(own, "z", 1)
    above = shift(own, "z", -1)

    asked = owners.reshape(-1)
    slots = local_slots.reshape(-1)
    wanted = jnp.sum(
        jnp.where(asked[:, None] == jnp.arange(64, dtype=jnp.int32)[None, :], slots[:, None], 0),
        axis=0,
    )
    wanted = jnp.broadcast_to(wanted.reshape(1, 8, 8).transpose(0, 2, 1), (8, 8, 8))
    table = exchange(wanted.reshape(64, 8), ST)

    near, up1, down1, up2, down2 = pick(plane, table, own, below, above)
    side = ("y", "c")
    near = exchange(near, side)
    up1 = shift(up1, "z", 1)
    down1 = shift(down1, "z", -1)
    up2 = shift(up2, "z", 2)
    down2 = shift(down2, "z", -2)
    away = fill(up1, down1, 0)
    away = fill(up2, down2, 2 * PROWS, away)
    away = exchange(away, side)
    split = (3 * PROWS + NEAR_ROWS) // 2
    upper = shift(near[:, 3 * PROWS : split], "z", 3)
    lower = shift(near[:, split:], "z", -3)

    convolved, stats = token_path(
        me,
        tokens,
        left,
        right,
        far,
        token_gain,
        inner_weight,
        gating_weight,
        filter_taps,
    )
    stats = lax.psum(stats, "tp")
    stats = stats.transpose(1, 0, 2, 3).reshape(2, -1, 128)
    conv_out = finish(convolved, stats, channel_gain)
    return attend(plane, asked, conv_out, retrieval_gate, (near, away, upper, lower))


def solution(mesh):
    st, tp = mesh.devices.shape
    fine = Mesh(mesh.devices.reshape(st // 8, 4, 2, tp), ST + ("tp",))
    placed = (
        P(ST, "tp"),
        P(),
        P(None, "tp"),
        P(None, "tp"),
        P(None, "tp"),
        P("tp"),
        P("tp"),
        P(ST, None, None),
        P(),
        P(None, "tp"),
        P(None, "tp"),
        P(ST, None),
        P(ST, None),
    )
    return jax.shard_map(layer, mesh=fine, in_specs=placed, out_specs=P(ST, "tp"), check_vma=False)
```

```python
import functools
import math

import jax
import jax.numpy as jnp
from jax import lax
from jax.experimental import pallas as pl
from jax.experimental.pallas import tpu as pltpu
from jax.sharding import Mesh
from jax.sharding import PartitionSpec as P

D = 2048
HEAD = 256
CONV = 31
LENGTH = 512
BLOCK = 64
PB = 2
PROWS = 64
EPSILON = 1e-06
EPSILON_NORM = 1e-05
ST = ("z", "y", "c")
LEAD = 32
ROWS_CHUNK = 64
KEPT = 56
NEAR_ROWS = 4 * PROWS + 2 * (PROWS - KEPT)
AWAY_ROWS = 2 * PROWS + 2 * KEPT


def ring(size, step):
    return [(i, (i + step) % size) for i in range(size)]


def in_vmem(*values):
    return [pltpu.with_memory_space_constraint(value, pltpu.VMEM) for value in values]


def in_hbm(*values):
    return [pltpu.with_memory_space_constraint(value, pltpu.HBM) for value in values]


def whole(shape):
    return pl.BlockSpec(shape, lambda *_: (0,) * len(shape))


def project_kernel(rows_ref, gain_ref, keys_ref, values_ref, out_ref):
    rows = rows_ref[...].astype(jnp.float32)
    inverse = lax.rsqrt(jnp.mean(rows * rows, axis=1, keepdims=True) + EPSILON)
    normed = (rows * inverse * gain_ref[...]).astype(jnp.bfloat16)
    out_ref[:, :HEAD] = jnp.dot(normed, keys_ref[...], preferred_element_type=jnp.float32).astype(
        jnp.bfloat16
    )
    out_ref[:, HEAD:] = jnp.dot(
        normed, values_ref[...], preferred_element_type=jnp.float32
    ).astype(jnp.bfloat16)


def project_passages(store, gain, keys_weight, values_weight, part):
    rows = store.reshape(-1, D)
    count = rows.shape[0] // 2
    tile = 256
    first = part * (count // tile)
    return pl.pallas_call(
        project_kernel,
        grid=(count // tile,),
        in_specs=[
            pl.BlockSpec((tile, D), lambda i: (i + first, 0)),
            whole((1, D)),
            whole((D, HEAD)),
            whole((D, HEAD)),
        ],
        out_specs=pl.BlockSpec((tile, 2 * HEAD), lambda i: (i, 0)),
        out_shape=jax.ShapeDtypeStruct((count, 2 * HEAD), jnp.bfloat16),
        cost_estimate=pl.CostEstimate(
            flops=4 * count * D * HEAD, transcendentals=0, bytes_accessed=4 << 20
        ),
        compiler_params=pltpu.CompilerParams(vmem_limit_bytes=16 << 20),
        name="project_passages",
    )(*in_hbm(rows), gain.reshape(1, D), *in_hbm(keys_weight, values_weight))


def token_kernel(
    me_ref,
    own_ref,
    left_ref,
    right_ref,
    far_ref,
    gain_ref,
    inner_ref,
    gating_ref,
    taps_ref,
    out_ref,
    stats_ref,
    padded_ref,
):
    me = me_ref[0]
    width = own_ref.shape[1]
    squares = jnp.zeros((LENGTH, 1), jnp.float32)
    inner = jnp.zeros((LENGTH, width), jnp.float32)
    gating = jnp.zeros((LENGTH, width), jnp.float32)
    for offset in range(4):
        at = lax.rem(me + offset, 4)
        if offset == 0:
            piece = own_ref[...].astype(jnp.float32)
        elif offset == 1:
            piece = right_ref[...].astype(jnp.float32)
        elif offset == 3:
            piece = left_ref[...].astype(jnp.float32)
        else:
            piece = far_ref[...].astype(jnp.float32)
        squares = squares + jnp.sum(piece * piece, axis=1, keepdims=True)
        scaled = (piece * gain_ref[at]).astype(jnp.bfloat16)
        inner = inner + jnp.dot(scaled, inner_ref[at], preferred_element_type=jnp.float32)
        gating = gating + jnp.dot(scaled, gating_ref[at], preferred_element_type=jnp.float32)
    inverse = lax.rsqrt(squares / D + EPSILON)
    gated = (inner * inverse * jax.nn.sigmoid(gating * inverse)).astype(jnp.bfloat16)
    padded_ref[:LEAD, :] = jnp.zeros((LEAD, width), jnp.float32)
    padded_ref[LEAD:, :] = gated.astype(jnp.float32)
    shift = LEAD - CONV + 1

    def step(n):
        base = n * ROWS_CHUNK
        sums = jnp.zeros((ROWS_CHUNK, 128), jnp.float32)
        square_sums = jnp.zeros((ROWS_CHUNK, 128), jnp.float32)
        for lane in range(0, width, 128):
            total = jnp.zeros((ROWS_CHUNK, 128), jnp.float32)
            for s in range(8):
                part = None
                for j in range(LEAD // 8 + 1):
                    tap = 8 * j + s - shift
                    if tap < 0 or tap >= CONV:
                        continue
                    height = ROWS_CHUNK + (8 if s else 0)
                    term = (
                        padded_ref[pl.ds(base + 8 * j, height), lane : lane + 128]
                        * taps_ref[tap : tap + 1, lane : lane + 128]
                    )
                    part = term if part is None else part + term
                total = total + part[s : s + ROWS_CHUNK]
            out_ref[pl.ds(base, ROWS_CHUNK), lane : lane + 128] = total
            sums = sums + total
            square_sums = square_sums + total * total
        return sums, square_sums

    for n in range(LENGTH // 128):
        pair = [step(2 * n + h) for h in range(2)]
        sums = jnp.concatenate([pair[0][0], pair[1][0]], axis=0)
        square_sums = jnp.concatenate([pair[0][1], pair[1][1]], axis=0)
        stats_ref[0, n : n + 1, :] = jnp.sum(sums.T, axis=0, keepdims=True)
        stats_ref[1, n : n + 1, :] = jnp.sum(square_sums.T, axis=0, keepdims=True)


def token_path(me, own, left, right, far, gain, inner_weight, gating_weight, taps):
    rows, width = own.shape
    grid_spec = pltpu.PrefetchScalarGridSpec(
        num_scalar_prefetch=1,
        grid=(rows // LENGTH,),
        in_specs=[pl.BlockSpec((LENGTH, width), lambda i, m: (i, 0))] * 4
        + [
            whole((4, 1, width)),
            whole((4, width, width)),
            whole((4, width, width)),
            whole((CONV, width)),
        ],
        out_specs=[
            pl.BlockSpec((LENGTH, width), lambda i, m: (i, 0)),
            pl.BlockSpec((None, 2, LENGTH // 128, 128), lambda i, m: (i, 0, 0, 0)),
        ],
        scratch_shapes=[pltpu.VMEM((LEAD + LENGTH, width), jnp.float32)],
    )
    return pl.pallas_call(
        token_kernel,
        grid_spec=grid_spec,
        out_shape=[
            pltpu.HBM((rows, width), jnp.float32),
            jax.ShapeDtypeStruct((rows // LENGTH, 2, LENGTH // 128, 128), jnp.float32),
        ],
        cost_estimate=pl.CostEstimate(
            flops=4 * rows * D * width, transcendentals=rows * width, bytes_accessed=10 << 20
        ),
        compiler_params=pltpu.CompilerParams(vmem_limit_bytes=40 << 20),
        name="token_path",
    )(
        me,
        *in_hbm(
            own,
            left,
            right,
            far,
            gain.reshape(4, 1, width),
            inner_weight.reshape(4, width, width),
            gating_weight.reshape(4, width, width),
            taps,
        ),
    )


def finish_kernel(conv_ref, stats_ref, gain_ref, out_ref):
    width = conv_ref.shape[1]
    turn = pl.program_id(0)
    for n in range(conv_ref.shape[0] // 128):
        at = turn * (conv_ref.shape[0] // 128) + n
        rows = slice(n * 128, (n + 1) * 128)
        average = stats_ref[0, pl.ds(at, 1), :] / D
        variance = stats_ref[1, pl.ds(at, 1), :] / D - average * average
        spread = lax.rsqrt(variance + EPSILON_NORM)
        average = jnp.broadcast_to(average, (128, 128)).T
        spread = jnp.broadcast_to(spread, (128, 128)).T
        for lane in range(0, width, 128):
            part = slice(lane, lane + 128)
            scaled = (conv_ref[rows, part] - average) * spread * gain_ref[:, part]
            out_ref[rows, part] = scaled * jax.nn.sigmoid(scaled)


def finish(convolved, stats, channel_gain):
    rows, width = convolved.shape
    tile = 512
    return pl.pallas_call(
        finish_kernel,
        grid=(rows // tile,),
        in_specs=[
            pl.BlockSpec((tile, width), lambda i: (i, 0)),
            whole((2, rows // 128, 128)),
            whole((1, width)),
        ],
        out_specs=pl.BlockSpec((tile, width), lambda i: (i, 0)),
        out_shape=pltpu.HBM((rows, width), jnp.float32),
        cost_estimate=pl.CostEstimate(
            flops=8 * rows * width, transcendentals=rows * width, bytes_accessed=4 << 20
        ),
        compiler_params=pltpu.CompilerParams(vmem_limit_bytes=14 << 20),
        name="finish",
    )(*in_hbm(convolved), stats, channel_gain.reshape(1, width))


def attend_kernel(plane_ref, where_ref, conv_ref, gate_ref, *refs):
    near_ref, far_ref, upper_ref, lower_ref, out_ref, held_ref, sems = refs
    turn = pl.program_id(0)
    count = where_ref.shape[0]
    here = plane_ref[0]
    half = PROWS // 2

    @pl.when(turn == 0)
    def _():
        for n in range(count):
            owner = where_ref[n]
            away = lax.rem(owner // 8 - here + 8, 8)
            column = lax.rem(owner, 8)
            close = (away <= 1) | (away == 7)

            @pl.when(close)
            def _():
                k = jnp.where(away == 7, 1, 2 * away)
                at = pl.multiple_of(k * PROWS, PROWS)
                pltpu.make_async_copy(
                    near_ref.at[column, pl.ds(at, PROWS)], held_ref.at[n], sems.at[n]
                ).start()

            @pl.when(away == 4)
            def _():
                pltpu.make_async_copy(
                    upper_ref.at[column, pl.ds(0, half)],
                    held_ref.at[n, pl.ds(0, half)],
                    sems.at[n],
                ).start()
                pltpu.make_async_copy(
                    lower_ref.at[column, pl.ds(0, half)],
                    held_ref.at[n, pl.ds(half, half)],
                    sems.at[n],
                ).start()

            @pl.when((away == 2) | (away == 6))
            def _():
                at = pl.multiple_of(jnp.where(away == 2, PROWS, 0), PROWS)
                pltpu.make_async_copy(
                    far_ref.at[column, pl.ds(at, PROWS)], held_ref.at[n], sems.at[n]
                ).start()

            for side, at, rest_ref in (
                (5, 2 * PROWS, upper_ref),
                (3, 2 * PROWS + KEPT, lower_ref),
            ):

                @pl.when(away == side)
                def _():
                    pltpu.make_async_copy(
                        far_ref.at[column, pl.ds(at, KEPT)],
                        held_ref.at[n, pl.ds(0, KEPT)],
                        sems.at[n],
                    ).start()
                    pltpu.make_async_copy(
                        rest_ref.at[column, pl.ds(half, PROWS - KEPT)],
                        held_ref.at[n, pl.ds(KEPT, PROWS - KEPT)],
                        sems.at[n],
                    ).start()

    blocks = conv_ref.shape[0] // BLOCK
    weight = jax.nn.sigmoid(gate_ref[...])
    queries = conv_ref[...].astype(jnp.bfloat16)
    for n in range(blocks * PB):
        at = turn * blocks * PB + n
        pltpu.make_async_copy(
            far_ref.at[0, pl.ds(0, PROWS)], held_ref.at[at], sems.at[at]
        ).wait()
    scores = []
    for b in range(blocks):
        held = held_ref[pl.ds((turn * blocks + b) * PB, PB)].reshape(PB * PROWS, 2 * HEAD)
        rows = slice(b * BLOCK, (b + 1) * BLOCK)
        heads = jnp.concatenate([queries[rows, :HEAD], queries[rows, HEAD:]], axis=0)
        scores.append(
            lax.dot_general(
                heads,
                held[:, :HEAD],
                (((1,), (1,)), ((), ())),
                preferred_element_type=jnp.float32,
            )
            / math.sqrt(HEAD)
        )
    shares = []
    for b in range(blocks):
        raised = jnp.exp(scores[b] - jnp.max(scores[b], axis=1, keepdims=True))
        shares.append((raised / jnp.sum(raised, axis=1, keepdims=True)).astype(jnp.bfloat16))
    for b in range(blocks):
        held = held_ref[pl.ds((turn * blocks + b) * PB, PB)].reshape(PB * PROWS, 2 * HEAD)
        attended = jnp.dot(shares[b], held[:, HEAD:], preferred_element_type=jnp.float32)
        attended = jnp.concatenate([attended[:BLOCK], attended[BLOCK:]], axis=1)
        rows = slice(b * BLOCK, (b + 1) * BLOCK)
        out_ref[rows, :] = (conv_ref[rows, :] + weight * attended).astype(jnp.bfloat16)


def attend(plane, where, conv_out, retrieval_gate, groups):
    rows, width = conv_out.shape
    count = where.shape[0]
    tile = 512
    grid_spec = pltpu.PrefetchScalarGridSpec(
        num_scalar_prefetch=2,
        grid=(rows // tile,),
        in_specs=[
            pl.BlockSpec((tile, width), lambda i, *_: (i, 0)),
            whole((1, width)),
        ]
        + [pl.BlockSpec(memory_space=pl.ANY)] * len(groups),
        out_specs=pl.BlockSpec((tile, width), lambda i, *_: (i, 0)),
        scratch_shapes=[
            pltpu.VMEM((count, PROWS, 2 * HEAD), jnp.bfloat16),
            pltpu.SemaphoreType.DMA((count,)),
        ],
    )
    return pl.pallas_call(
        attend_kernel,
        grid_spec=grid_spec,
        out_shape=jax.ShapeDtypeStruct((rows, width), jnp.bfloat16),
        cost_estimate=pl.CostEstimate(
            flops=4 * rows * 2 * PB * PROWS * HEAD,
            transcendentals=rows * 2 * PB * PROWS,
            bytes_accessed=5 << 20,
        ),
        compiler_params=pltpu.CompilerParams(vmem_limit_bytes=16 << 20),
        name="attend",
    )(plane, where, *in_hbm(conv_out), retrieval_gate.reshape(1, width), *in_hbm(*groups))


def pick_kernel(plane_ref, table_ref, *refs):
    (own, below, above), refs = (refs[0:2], refs[2:4], refs[4:6]), refs[6:]
    outs, sems = refs[:-1], refs[-1]
    here = plane_ref[0]
    half = PROWS // 2

    def slot(reader_plane, reader, owner_plane):
        at = lax.rem(here + reader_plane + 8, 8) * 8 + reader
        return table_ref[at, lax.rem(here + owner_plane + 8, 8)]

    def send(sources, taken, first, rows, target, n):
        size = sources[0].shape[0]
        for part, source in enumerate(sources):

            @pl.when((taken < size) if part == 0 else (taken >= size))
            def _():
                pltpu.make_async_copy(
                    source.at[taken - part * size, pl.ds(first, rows)], target, sems.at[n]
                ).start()

    for reader in range(8):
        for n, (source, side, steps, rows) in enumerate(
            (
                (below, 1, 1, PROWS),
                (above, -1, 1, PROWS),
                (below, 1, 2, KEPT),
                (above, -1, 2, KEPT),
            )
        ):
            taken = slot(side * steps, reader, -side)
            send(source, taken, 0, rows, outs[1 + n].at[reader], 1 + n)
    for reader in range(8):
        at = 0
        for source, reader_plane, owner_plane, first, rows in (
            (own, 0, 0, 0, PROWS),
            (below, 0, -1, 0, PROWS),
            (above, 0, 1, 0, PROWS),
            (below, 3, -1, 0, half),
            (own, 3, 0, KEPT, PROWS - KEPT),
            (above, -3, 1, half, half),
            (own, -3, 0, KEPT, PROWS - KEPT),
        ):
            taken = slot(reader_plane, reader, owner_plane)
            send(source, taken, first, rows, outs[0].at[reader, pl.ds(at, rows)], 0)
            at += rows
    for n, out in enumerate(outs):
        pltpu.make_async_copy(out, out, sems.at[n]).wait()


def pick(plane, table, *sources):
    shapes = [(8, NEAR_ROWS), (8, PROWS), (8, PROWS), (8, KEPT), (8, KEPT)]
    return pl.pallas_call(
        pick_kernel,
        in_specs=[pl.BlockSpec(memory_space=pltpu.SMEM)] * 2
        + [pl.BlockSpec(memory_space=pl.ANY)] * len(sources),
        out_specs=[pl.BlockSpec(memory_space=pl.ANY)] * len(shapes),
        scratch_shapes=[pltpu.SemaphoreType.DMA((len(shapes),))],
        out_shape=[pltpu.HBM((*shape, 2 * HEAD), jnp.bfloat16) for shape in shapes],
        cost_estimate=pl.CostEstimate(flops=0, transcendentals=0, bytes_accessed=8 << 20),
        compiler_params=pltpu.CompilerParams(vmem_limit_bytes=2 << 20),
        name="pick",
    )(plane, table, *in_vmem(*sources))


def fill_kernel(*refs, at):
    first_ref, second_ref = refs[:2]
    out_ref, stores = refs[-2:]
    rows = first_ref.shape[1]
    copies = [
        pltpu.make_async_copy(ref, out_ref.at[:, pl.ds(at + n * rows, rows)], stores.at[n])
        for n, ref in enumerate((first_ref, second_ref))
    ]
    for copy in copies:
        copy.start()
    for copy in copies:
        copy.wait()


def staged_fill_kernel(first_ref, second_ref, into_ref, out_ref, held_ref, loads, stores, *, at):
    del into_ref
    size, rows, _ = first_ref.shape
    count = size // 2
    parts = [(n, h) for h in range(2) for n in range(2)]

    def load(n, h):
        source = (first_ref, second_ref)[n].at[pl.ds(h * count, count)]
        return pltpu.make_async_copy(source, held_ref.at[n, h], loads.at[n, h])

    def store(n, h):
        target = out_ref.at[pl.ds(h * count, count), pl.ds(at + n * rows, rows)]
        return pltpu.make_async_copy(held_ref.at[n, h], target, stores.at[n, h])

    for part in parts:
        load(*part).start()
    for part in parts:
        load(*part).wait()
        store(*part).start()
    for part in parts:
        store(*part).wait()


def fill(first, second, at, into=None):
    size, rows, width = first.shape
    if into is None:
        kernel, held = fill_kernel, in_vmem(first, second)
        scratch = [pltpu.SemaphoreType.DMA((2,))]
    else:
        kernel, held = staged_fill_kernel, in_hbm(first, second, into)
        scratch = [pltpu.VMEM((2, 2, size // 2, rows, width), first.dtype)] + [
            pltpu.SemaphoreType.DMA((2, 2))
        ] * 2
    return pl.pallas_call(
        functools.partial(kernel, at=at),
        in_specs=[pl.BlockSpec(memory_space=pl.ANY)] * len(held),
        out_specs=pl.BlockSpec(memory_space=pl.ANY),
        scratch_shapes=scratch,
        out_shape=pltpu.HBM((size, AWAY_ROWS, width), first.dtype),
        input_output_aliases={} if into is None else {2: 0},
        cost_estimate=pl.CostEstimate(flops=0, transcendentals=0, bytes_accessed=2 << 20),
        compiler_params=pltpu.CompilerParams(vmem_limit_bytes=4 << 20),
        name="fill",
    )(*held)


def shift(value, axis, step):
    return lax.ppermute(value, axis, ring(lax.axis_size(axis), step))


def exchange(value, axes):
    return lax.all_to_all(value, axes, split_axis=0, concat_axis=0, tiled=True)


def layer(
    tokens,
    token_gain,
    inner_weight,
    gating_weight,
    filter_taps,
    channel_gain,
    retrieval_gate,
    passage_store,
    passage_gain,
    keys_weight,
    values_weight,
    owners,
    local_slots,
):
    me = lax.axis_index("tp").astype(jnp.int32).reshape(1)
    plane = lax.axis_index("z").astype(jnp.int32).reshape(1)
    left = shift(tokens, "tp", 1)
    right = shift(tokens, "tp", -1)
    far = shift(tokens, "tp", 2)

    sources = [[], [], []]
    for part in range(2):
        own = project_passages(
            passage_store, passage_gain, keys_weight, values_weight, part
        )
        own = own.reshape(-1, PROWS, 2 * HEAD)
        sources[0].append(own)
        sources[1].append(shift(own, "z", 1))
        sources[2].append(shift(own, "z", -1))

    asked = owners.reshape(-1)
    slots = local_slots.reshape(-1)
    wanted = jnp.sum(
        jnp.where(asked[:, None] == jnp.arange(64, dtype=jnp.int32)[None, :], slots[:, None], 0),
        axis=0,
    )
    wanted = jnp.broadcast_to(wanted.reshape(1, 8, 8).transpose(0, 2, 1), (8, 8, 8))
    table = exchange(wanted.reshape(64, 8), ST)

    near, up1, down1, up2, down2 = pick(plane, table, *sum(sources, []))
    side = ("y", "c")
    near = exchange(near, side)
    up1 = shift(up1, "z", 1)
    down1 = shift(down1, "z", -1)
    up2 = shift(up2, "z", 2)
    down2 = shift(down2, "z", -2)
    away = fill(up1, down1, 0)
    away = fill(up2, down2, 2 * PROWS, away)
    away = exchange(away, side)
    split = (3 * PROWS + NEAR_ROWS) // 2
    upper = shift(near[:, 3 * PROWS : split], "z", 3)
    lower = shift(near[:, split:], "z", -3)

    convolved, stats = token_path(
        me,
        tokens,
        left,
        right,
        far,
        token_gain,
        inner_weight,
        gating_weight,
        filter_taps,
    )
    stats = lax.psum(stats, "tp")
    stats = stats.transpose(1, 0, 2, 3).reshape(2, -1, 128)
    conv_out = finish(convolved, stats, channel_gain)
    return attend(plane, asked, conv_out, retrieval_gate, (near, away, upper, lower))


def solution(mesh):
    st, tp = mesh.devices.shape
    fine = Mesh(mesh.devices.reshape(st // 8, 4, 2, tp), ST + ("tp",))
    placed = (
        P(ST, "tp"),
        P(),
        P(None, "tp"),
        P(None, "tp"),
        P(None, "tp"),
        P("tp"),
        P("tp"),
        P(ST, None, None),
        P(),
        P(None, "tp"),
        P(None, "tp"),
        P(ST, None),
        P(ST, None),
    )
    return jax.shard_map(layer, mesh=fine, in_specs=placed, out_specs=P(ST, "tp"), check_vma=False)
```

```python
import functools
import math

import jax
import jax.numpy as jnp
from jax import lax
from jax.experimental import pallas as pl
from jax.experimental.pallas import tpu as pltpu
from jax.sharding import Mesh
from jax.sharding import PartitionSpec as P

D = 2048
HEAD = 256
CONV = 31
LENGTH = 512
BLOCK = 64
PB = 2
PROWS = 64
EPSILON = 1e-06
EPSILON_NORM = 1e-05
ST = ("z", "y", "c")
LEAD = 32
ROWS_CHUNK = 64
KEPT = 56
NEAR_ROWS = 4 * PROWS + 2 * (PROWS - KEPT)
AWAY_ROWS = 2 * PROWS + 2 * KEPT


def ring(size, step):
    return [(i, (i + step) % size) for i in range(size)]


def in_vmem(*values):
    return [pltpu.with_memory_space_constraint(value, pltpu.VMEM) for value in values]


def in_hbm(*values):
    return [pltpu.with_memory_space_constraint(value, pltpu.HBM) for value in values]


def whole(shape):
    return pl.BlockSpec(shape, lambda *_: (0,) * len(shape))


def project_kernel(rows_ref, gain_ref, keys_ref, values_ref, out_ref):
    rows = rows_ref[...].astype(jnp.float32)
    inverse = lax.rsqrt(jnp.mean(rows * rows, axis=1, keepdims=True) + EPSILON)
    normed = (rows * inverse * gain_ref[...]).astype(jnp.bfloat16)
    out_ref[:, :HEAD] = jnp.dot(normed, keys_ref[...], preferred_element_type=jnp.float32).astype(
        jnp.bfloat16
    )
    out_ref[:, HEAD:] = jnp.dot(
        normed, values_ref[...], preferred_element_type=jnp.float32
    ).astype(jnp.bfloat16)


def project_passages(store, gain, keys_weight, values_weight, part):
    rows = store.reshape(-1, D)
    count = rows.shape[0] // 2
    tile = 256
    first = part * (count // tile)
    return pl.pallas_call(
        project_kernel,
        grid=(count // tile,),
        in_specs=[
            pl.BlockSpec((tile, D), lambda i: (i + first, 0)),
            whole((1, D)),
            whole((D, HEAD)),
            whole((D, HEAD)),
        ],
        out_specs=pl.BlockSpec((tile, 2 * HEAD), lambda i: (i, 0)),
        out_shape=jax.ShapeDtypeStruct((count, 2 * HEAD), jnp.bfloat16),
        cost_estimate=pl.CostEstimate(
            flops=4 * count * D * HEAD, transcendentals=0, bytes_accessed=4 << 20
        ),
        compiler_params=pltpu.CompilerParams(vmem_limit_bytes=16 << 20),
        name="project_passages",
    )(*in_hbm(rows), gain.reshape(1, D), *in_hbm(keys_weight, values_weight))


def token_kernel(
    me_ref,
    own_ref,
    left_ref,
    right_ref,
    far_ref,
    gain_ref,
    inner_ref,
    gating_ref,
    taps_ref,
    out_ref,
    stats_ref,
    padded_ref,
    inner_held,
    gating_held,
    sems,
):
    me = me_ref[0]
    begin = pl.program_id(0) == 0

    def load(n, offset):
        at = lax.rem(me + offset, 4)
        source, target = ((inner_ref, inner_held), (gating_ref, gating_held))[n]
        return pltpu.make_async_copy(source.at[at], target.at[offset], sems.at[n, offset])

    @pl.when(begin)
    def _():
        for offset in range(4):
            for n in range(2):
                load(n, offset).start()

    width = own_ref.shape[1]
    squares = jnp.zeros((LENGTH, 1), jnp.float32)
    inner = jnp.zeros((LENGTH, width), jnp.float32)
    gating = jnp.zeros((LENGTH, width), jnp.float32)
    for offset in range(4):
        at = lax.rem(me + offset, 4)
        if offset == 0:
            piece = own_ref[...].astype(jnp.float32)
        elif offset == 1:
            piece = right_ref[...].astype(jnp.float32)
        elif offset == 3:
            piece = left_ref[...].astype(jnp.float32)
        else:
            piece = far_ref[...].astype(jnp.float32)
        squares = squares + jnp.sum(piece * piece, axis=1, keepdims=True)
        scaled = (piece * gain_ref[at]).astype(jnp.bfloat16)

        @pl.when(begin)
        def _():
            for n in range(2):
                load(n, offset).wait()

        inner = inner + jnp.dot(scaled, inner_held[offset], preferred_element_type=jnp.float32)
        gating = gating + jnp.dot(scaled, gating_held[offset], preferred_element_type=jnp.float32)
    inverse = lax.rsqrt(squares / D + EPSILON)
    gated = (inner * inverse * jax.nn.sigmoid(gating * inverse)).astype(jnp.bfloat16)
    padded_ref[:LEAD, :] = jnp.zeros((LEAD, width), jnp.float32)
    padded_ref[LEAD:, :] = gated.astype(jnp.float32)
    shift = LEAD - CONV + 1

    def step(n):
        base = n * ROWS_CHUNK
        sums = jnp.zeros((ROWS_CHUNK, 128), jnp.float32)
        square_sums = jnp.zeros((ROWS_CHUNK, 128), jnp.float32)
        for lane in range(0, width, 128):
            total = jnp.zeros((ROWS_CHUNK, 128), jnp.float32)
            for s in range(8):
                part = None
                for j in range(LEAD // 8 + 1):
                    tap = 8 * j + s - shift
                    if tap < 0 or tap >= CONV:
                        continue
                    height = ROWS_CHUNK + (8 if s else 0)
                    term = (
                        padded_ref[pl.ds(base + 8 * j, height), lane : lane + 128]
                        * taps_ref[tap : tap + 1, lane : lane + 128]
                    )
                    part = term if part is None else part + term
                total = total + part[s : s + ROWS_CHUNK]
            out_ref[pl.ds(base, ROWS_CHUNK), lane : lane + 128] = total
            sums = sums + total
            square_sums = square_sums + total * total
        return sums, square_sums

    for n in range(LENGTH // 128):
        pair = [step(2 * n + h) for h in range(2)]
        sums = jnp.concatenate([pair[0][0], pair[1][0]], axis=0)
        square_sums = jnp.concatenate([pair[0][1], pair[1][1]], axis=0)
        stats_ref[0, n : n + 1, :] = jnp.sum(sums.T, axis=0, keepdims=True)
        stats_ref[1, n : n + 1, :] = jnp.sum(square_sums.T, axis=0, keepdims=True)


def token_path(me, own, left, right, far, gain, inner_weight, gating_weight, taps):
    rows, width = own.shape
    grid_spec = pltpu.PrefetchScalarGridSpec(
        num_scalar_prefetch=1,
        grid=(rows // LENGTH,),
        in_specs=[pl.BlockSpec((LENGTH, width), lambda i, m: (i, 0))] * 4
        + [
            whole((4, 1, width)),
            pl.BlockSpec(memory_space=pl.ANY),
            pl.BlockSpec(memory_space=pl.ANY),
            whole((CONV, width)),
        ],
        out_specs=[
            pl.BlockSpec((LENGTH, width), lambda i, m: (i, 0)),
            pl.BlockSpec((None, 2, LENGTH // 128, 128), lambda i, m: (i, 0, 0, 0)),
        ],
        scratch_shapes=[
            pltpu.VMEM((LEAD + LENGTH, width), jnp.float32),
            pltpu.VMEM((4, width, width), jnp.bfloat16),
            pltpu.VMEM((4, width, width), jnp.bfloat16),
            pltpu.SemaphoreType.DMA((2, 4)),
        ],
    )
    return pl.pallas_call(
        token_kernel,
        grid_spec=grid_spec,
        out_shape=[
            pltpu.HBM((rows, width), jnp.float32),
            jax.ShapeDtypeStruct((rows // LENGTH, 2, LENGTH // 128, 128), jnp.float32),
        ],
        cost_estimate=pl.CostEstimate(
            flops=4 * rows * D * width, transcendentals=rows * width, bytes_accessed=10 << 20
        ),
        compiler_params=pltpu.CompilerParams(vmem_limit_bytes=40 << 20),
        name="token_path",
    )(
        me,
        *in_hbm(
            own,
            left,
            right,
            far,
            gain.reshape(4, 1, width),
            inner_weight.reshape(4, width, width),
            gating_weight.reshape(4, width, width),
            taps,
        ),
    )


def finish_kernel(conv_ref, stats_ref, gain_ref, out_ref):
    width = conv_ref.shape[1]
    turn = pl.program_id(0)
    for n in range(conv_ref.shape[0] // 128):
        at = turn * (conv_ref.shape[0] // 128) + n
        rows = slice(n * 128, (n + 1) * 128)
        average = stats_ref[0, pl.ds(at, 1), :] / D
        variance = stats_ref[1, pl.ds(at, 1), :] / D - average * average
        spread = lax.rsqrt(variance + EPSILON_NORM)
        average = jnp.broadcast_to(average, (128, 128)).T
        spread = jnp.broadcast_to(spread, (128, 128)).T
        for lane in range(0, width, 128):
            part = slice(lane, lane + 128)
            scaled = (conv_ref[rows, part] - average) * spread * gain_ref[:, part]
            out_ref[rows, part] = scaled * jax.nn.sigmoid(scaled)


def finish(convolved, stats, channel_gain):
    rows, width = convolved.shape
    tile = 512
    return pl.pallas_call(
        finish_kernel,
        grid=(rows // tile,),
        in_specs=[
            pl.BlockSpec((tile, width), lambda i: (i, 0)),
            whole((2, rows // 128, 128)),
            whole((1, width)),
        ],
        out_specs=pl.BlockSpec((tile, width), lambda i: (i, 0)),
        out_shape=pltpu.HBM((rows, width), jnp.float32),
        cost_estimate=pl.CostEstimate(
            flops=8 * rows * width, transcendentals=rows * width, bytes_accessed=4 << 20
        ),
        compiler_params=pltpu.CompilerParams(vmem_limit_bytes=14 << 20),
        name="finish",
    )(*in_hbm(convolved), stats, channel_gain.reshape(1, width))


def attend_kernel(plane_ref, where_ref, conv_ref, gate_ref, *refs):
    near_ref, far_ref, upper_ref, lower_ref, out_ref, held_ref, sems = refs
    turn = pl.program_id(0)
    count = where_ref.shape[0]
    here = plane_ref[0]
    half = PROWS // 2

    @pl.when(turn == 0)
    def _():
        for n in range(count):
            owner = where_ref[n]
            away = lax.rem(owner // 8 - here + 8, 8)
            column = lax.rem(owner, 8)
            close = (away <= 1) | (away == 7)

            @pl.when(close)
            def _():
                k = jnp.where(away == 7, 1, 2 * away)
                at = pl.multiple_of(k * PROWS, PROWS)
                pltpu.make_async_copy(
                    near_ref.at[column, pl.ds(at, PROWS)], held_ref.at[n], sems.at[n]
                ).start()

            @pl.when(away == 4)
            def _():
                pltpu.make_async_copy(
                    upper_ref.at[column, pl.ds(0, half)],
                    held_ref.at[n, pl.ds(0, half)],
                    sems.at[n],
                ).start()
                pltpu.make_async_copy(
                    lower_ref.at[column, pl.ds(0, half)],
                    held_ref.at[n, pl.ds(half, half)],
                    sems.at[n],
                ).start()

            @pl.when((away == 2) | (away == 6))
            def _():
                at = pl.multiple_of(jnp.where(away == 2, PROWS, 0), PROWS)
                pltpu.make_async_copy(
                    far_ref.at[column, pl.ds(at, PROWS)], held_ref.at[n], sems.at[n]
                ).start()

            for side, at, rest_ref in (
                (5, 2 * PROWS, upper_ref),
                (3, 2 * PROWS + KEPT, lower_ref),
            ):

                @pl.when(away == side)
                def _():
                    pltpu.make_async_copy(
                        far_ref.at[column, pl.ds(at, KEPT)],
                        held_ref.at[n, pl.ds(0, KEPT)],
                        sems.at[n],
                    ).start()
                    pltpu.make_async_copy(
                        rest_ref.at[column, pl.ds(half, PROWS - KEPT)],
                        held_ref.at[n, pl.ds(KEPT, PROWS - KEPT)],
                        sems.at[n],
                    ).start()

    blocks = conv_ref.shape[0] // BLOCK
    weight = jax.nn.sigmoid(gate_ref[...])
    queries = conv_ref[...].astype(jnp.bfloat16)
    for n in range(blocks * PB):
        at = turn * blocks * PB + n
        pltpu.make_async_copy(
            far_ref.at[0, pl.ds(0, PROWS)], held_ref.at[at], sems.at[at]
        ).wait()
    scores = []
    for b in range(blocks):
        held = held_ref[pl.ds((turn * blocks + b) * PB, PB)].reshape(PB * PROWS, 2 * HEAD)
        rows = slice(b * BLOCK, (b + 1) * BLOCK)
        heads = jnp.concatenate([queries[rows, :HEAD], queries[rows, HEAD:]], axis=0)
        scores.append(
            lax.dot_general(
                heads,
                held[:, :HEAD],
                (((1,), (1,)), ((), ())),
                preferred_element_type=jnp.float32,
            )
            / math.sqrt(HEAD)
        )
    shares = []
    for b in range(blocks):
        raised = jnp.exp(scores[b] - jnp.max(scores[b], axis=1, keepdims=True))
        shares.append((raised / jnp.sum(raised, axis=1, keepdims=True)).astype(jnp.bfloat16))
    for b in range(blocks):
        held = held_ref[pl.ds((turn * blocks + b) * PB, PB)].reshape(PB * PROWS, 2 * HEAD)
        attended = jnp.dot(shares[b], held[:, HEAD:], preferred_element_type=jnp.float32)
        attended = jnp.concatenate([attended[:BLOCK], attended[BLOCK:]], axis=1)
        rows = slice(b * BLOCK, (b + 1) * BLOCK)
        out_ref[rows, :] = (conv_ref[rows, :] + weight * attended).astype(jnp.bfloat16)


def attend(plane, where, conv_out, retrieval_gate, groups):
    rows, width = conv_out.shape
    count = where.shape[0]
    tile = 512
    grid_spec = pltpu.PrefetchScalarGridSpec(
        num_scalar_prefetch=2,
        grid=(rows // tile,),
        in_specs=[
            pl.BlockSpec((tile, width), lambda i, *_: (i, 0)),
            whole((1, width)),
        ]
        + [pl.BlockSpec(memory_space=pl.ANY)] * len(groups),
        out_specs=pl.BlockSpec((tile, width), lambda i, *_: (i, 0)),
        scratch_shapes=[
            pltpu.VMEM((count, PROWS, 2 * HEAD), jnp.bfloat16),
            pltpu.SemaphoreType.DMA((count,)),
        ],
    )
    return pl.pallas_call(
        attend_kernel,
        grid_spec=grid_spec,
        out_shape=jax.ShapeDtypeStruct((rows, width), jnp.bfloat16),
        cost_estimate=pl.CostEstimate(
            flops=4 * rows * 2 * PB * PROWS * HEAD,
            transcendentals=rows * 2 * PB * PROWS,
            bytes_accessed=5 << 20,
        ),
        compiler_params=pltpu.CompilerParams(vmem_limit_bytes=16 << 20),
        name="attend",
    )(plane, where, *in_hbm(conv_out), retrieval_gate.reshape(1, width), *in_hbm(*groups))


def pick_kernel(plane_ref, table_ref, *refs):
    (own, below, above), refs = (refs[0:2], refs[2:4], refs[4:6]), refs[6:]
    outs, sems = refs[:-1], refs[-1]
    here = plane_ref[0]
    half = PROWS // 2

    def slot(reader_plane, reader, owner_plane):
        return table_ref[
            lax.rem(here + reader_plane + 8, 8), reader * 8 + lax.rem(here + owner_plane + 8, 8)
        ]

    def send(sources, taken, first, rows, target, n):
        size = sources[0].shape[0]
        for part, source in enumerate(sources):

            @pl.when((taken < size) if part == 0 else (taken >= size))
            def _():
                pltpu.make_async_copy(
                    source.at[taken - part * size, pl.ds(first, rows)], target, sems.at[n]
                ).start()

    for reader in range(8):
        for n, (source, side, steps, rows) in enumerate(
            (
                (below, 1, 1, PROWS),
                (above, -1, 1, PROWS),
                (below, 1, 2, KEPT),
                (above, -1, 2, KEPT),
            )
        ):
            taken = slot(side * steps, reader, -side)
            send(source, taken, 0, rows, outs[1 + n].at[reader], 1 + n)
    for reader in range(8):
        at = 0
        for source, reader_plane, owner_plane, first, rows in (
            (own, 0, 0, 0, PROWS),
            (below, 0, -1, 0, PROWS),
            (above, 0, 1, 0, PROWS),
            (below, 3, -1, 0, half),
            (own, 3, 0, KEPT, PROWS - KEPT),
            (above, -3, 1, half, half),
            (own, -3, 0, KEPT, PROWS - KEPT),
        ):
            taken = slot(reader_plane, reader, owner_plane)
            send(source, taken, first, rows, outs[0].at[reader, pl.ds(at, rows)], 0)
            at += rows
    for n, out in enumerate(outs):
        pltpu.make_async_copy(out, out, sems.at[n]).wait()


def pick(plane, table, *sources):
    shapes = [(8, NEAR_ROWS), (8, PROWS), (8, PROWS), (8, KEPT), (8, KEPT)]
    return pl.pallas_call(
        pick_kernel,
        in_specs=[pl.BlockSpec(memory_space=pltpu.SMEM)] * 2
        + [pl.BlockSpec(memory_space=pl.ANY)] * len(sources),
        out_specs=[pl.BlockSpec(memory_space=pl.ANY)] * len(shapes),
        scratch_shapes=[pltpu.SemaphoreType.DMA((len(shapes),))],
        out_shape=[pltpu.HBM((*shape, 2 * HEAD), jnp.bfloat16) for shape in shapes],
        cost_estimate=pl.CostEstimate(flops=0, transcendentals=0, bytes_accessed=8 << 20),
        compiler_params=pltpu.CompilerParams(vmem_limit_bytes=2 << 20),
        name="pick",
    )(plane, table, *in_vmem(*sources))


def fill_kernel(*refs, at):
    first_ref, second_ref = refs[:2]
    out_ref, stores = refs[-2:]
    rows = first_ref.shape[1]
    copies = [
        pltpu.make_async_copy(ref, out_ref.at[:, pl.ds(at + n * rows, rows)], stores.at[n])
        for n, ref in enumerate((first_ref, second_ref))
    ]
    for copy in copies:
        copy.start()
    for copy in copies:
        copy.wait()


def staged_fill_kernel(first_ref, second_ref, into_ref, out_ref, held_ref, loads, stores, *, at):
    del into_ref
    size, rows, _ = first_ref.shape
    count = size // 2
    parts = [(n, h) for h in range(2) for n in range(2)]

    def load(n, h):
        source = (first_ref, second_ref)[n].at[pl.ds(h * count, count)]
        return pltpu.make_async_copy(source, held_ref.at[n, h], loads.at[n, h])

    def store(n, h):
        target = out_ref.at[pl.ds(h * count, count), pl.ds(at + n * rows, rows)]
        return pltpu.make_async_copy(held_ref.at[n, h], target, stores.at[n, h])

    for part in parts:
        load(*part).start()
    for part in parts:
        load(*part).wait()
        store(*part).start()
    for part in parts:
        store(*part).wait()


def fill(first, second, at, into=None):
    size, rows, width = first.shape
    if into is None:
        kernel, held = fill_kernel, in_vmem(first, second)
        scratch = [pltpu.SemaphoreType.DMA((2,))]
    else:
        kernel, held = staged_fill_kernel, in_hbm(first, second, into)
        scratch = [pltpu.VMEM((2, 2, size // 2, rows, width), first.dtype)] + [
            pltpu.SemaphoreType.DMA((2, 2))
        ] * 2
    return pl.pallas_call(
        functools.partial(kernel, at=at),
        in_specs=[pl.BlockSpec(memory_space=pl.ANY)] * len(held),
        out_specs=pl.BlockSpec(memory_space=pl.ANY),
        scratch_shapes=scratch,
        out_shape=pltpu.HBM((size, AWAY_ROWS, width), first.dtype),
        input_output_aliases={} if into is None else {2: 0},
        cost_estimate=pl.CostEstimate(flops=0, transcendentals=0, bytes_accessed=2 << 20),
        compiler_params=pltpu.CompilerParams(vmem_limit_bytes=4 << 20),
        name="fill",
    )(*held)


def shift(value, axis, step):
    return lax.ppermute(value, axis, ring(lax.axis_size(axis), step))


def exchange(value, axes):
    return lax.all_to_all(value, axes, split_axis=0, concat_axis=0, tiled=True)


def layer(
    tokens,
    token_gain,
    inner_weight,
    gating_weight,
    filter_taps,
    channel_gain,
    retrieval_gate,
    passage_store,
    passage_gain,
    keys_weight,
    values_weight,
    owners,
    local_slots,
):
    me = lax.axis_index("tp").astype(jnp.int32).reshape(1)
    plane = lax.axis_index("z").astype(jnp.int32).reshape(1)
    left = shift(tokens, "tp", 1)
    right = shift(tokens, "tp", -1)
    far = shift(tokens, "tp", 2)

    sources = [[], [], []]
    for part in range(2):
        own = project_passages(
            passage_store, passage_gain, keys_weight, values_weight, part
        )
        own = own.reshape(-1, PROWS, 2 * HEAD)
        sources[0].append(own)
        sources[1].append(shift(own, "z", 1))
        sources[2].append(shift(own, "z", -1))

    asked = owners.reshape(-1)
    slots = local_slots.reshape(-1)
    wanted = jnp.sum(
        jnp.where(asked[:, None] == jnp.arange(64, dtype=jnp.int32)[None, :], slots[:, None], 0),
        axis=0,
    )
    wanted = exchange(wanted.reshape(8, 8).T, ("y", "c"))
    table = exchange(jnp.broadcast_to(wanted.reshape(1, 64), (8, 64)), "z")

    near, up1, down1, up2, down2 = pick(plane, table, *sum(sources, []))
    side = ("y", "c")
    near = exchange(near, side)
    up1 = shift(up1, "z", 1)
    down1 = shift(down1, "z", -1)
    up2 = shift(up2, "z", 2)
    down2 = shift(down2, "z", -2)
    away = fill(up1, down1, 0)
    away = fill(up2, down2, 2 * PROWS, away)
    away = exchange(away, side)
    split = (3 * PROWS + NEAR_ROWS) // 2
    upper = shift(near[:, 3 * PROWS : split], "z", 3)
    lower = shift(near[:, split:], "z", -3)

    convolved, stats = token_path(
        me,
        tokens,
        left,
        right,
        far,
        token_gain,
        inner_weight,
        gating_weight,
        filter_taps,
    )
    stats = lax.psum(stats, "tp")
    stats = stats.transpose(1, 0, 2, 3).reshape(2, -1, 128)
    conv_out = finish(convolved, stats, channel_gain)
    return attend(plane, asked, conv_out, retrieval_gate, (near, away, upper, lower))


def solution(mesh):
    st, tp = mesh.devices.shape
    fine = Mesh(mesh.devices.reshape(st // 8, 4, 2, tp), ST + ("tp",))
    placed = (
        P(ST, "tp"),
        P(),
        P(None, "tp"),
        P(None, "tp"),
        P(None, "tp"),
        P("tp"),
        P("tp"),
        P(ST, None, None),
        P(),
        P(None, "tp"),
        P(None, "tp"),
        P(ST, None),
        P(ST, None),
    )
    return jax.shard_map(layer, mesh=fine, in_specs=placed, out_specs=P(ST, "tp"), check_vma=False)
```

```python
import functools
import math

import jax
import jax.numpy as jnp
from jax import lax
from jax.experimental import pallas as pl
from jax.experimental.pallas import tpu as pltpu
from jax.sharding import Mesh
from jax.sharding import PartitionSpec as P

D = 2048
HEAD = 256
CONV = 31
LENGTH = 512
BLOCK = 64
PB = 2
PROWS = 64
EPSILON = 1e-06
EPSILON_NORM = 1e-05
ST = ("z", "y", "c")
LEAD = 32
ROWS_CHUNK = 64
KEPT = 56
NEAR_ROWS = 4 * PROWS + 2 * (PROWS - KEPT)
AWAY_ROWS = 2 * PROWS + 2 * KEPT


def ring(size, step):
    return [(i, (i + step) % size) for i in range(size)]


def in_vmem(*values):
    return [pltpu.with_memory_space_constraint(value, pltpu.VMEM) for value in values]


def in_hbm(*values):
    return [pltpu.with_memory_space_constraint(value, pltpu.HBM) for value in values]


def whole(shape):
    return pl.BlockSpec(shape, lambda *_: (0,) * len(shape))


def project_kernel(rows_ref, gain_ref, keys_ref, values_ref, out_ref):
    rows = rows_ref[...].astype(jnp.float32)
    inverse = lax.rsqrt(jnp.mean(rows * rows, axis=1, keepdims=True) + EPSILON)
    normed = (rows * inverse * gain_ref[...]).astype(jnp.bfloat16)
    out_ref[:, :HEAD] = jnp.dot(normed, keys_ref[...], preferred_element_type=jnp.float32).astype(
        jnp.bfloat16
    )
    out_ref[:, HEAD:] = jnp.dot(
        normed, values_ref[...], preferred_element_type=jnp.float32
    ).astype(jnp.bfloat16)


def project_passages(store, gain, keys_weight, values_weight, part):
    rows = store.reshape(-1, D)
    count = rows.shape[0] // 2
    tile = 256
    first = part * (count // tile)
    return pl.pallas_call(
        project_kernel,
        grid=(count // tile,),
        in_specs=[
            pl.BlockSpec((tile, D), lambda i: (i + first, 0)),
            whole((1, D)),
            whole((D, HEAD)),
            whole((D, HEAD)),
        ],
        out_specs=pl.BlockSpec((tile, 2 * HEAD), lambda i: (i, 0)),
        out_shape=jax.ShapeDtypeStruct((count, 2 * HEAD), jnp.bfloat16),
        cost_estimate=pl.CostEstimate(
            flops=4 * count * D * HEAD, transcendentals=0, bytes_accessed=4 << 20
        ),
        compiler_params=pltpu.CompilerParams(vmem_limit_bytes=16 << 20),
        name="project_passages",
    )(*in_hbm(rows, gain.reshape(1, D), keys_weight, values_weight))


def token_kernel(
    me_ref,
    own_ref,
    left_ref,
    right_ref,
    far_ref,
    gain_ref,
    inner_ref,
    gating_ref,
    taps_ref,
    out_ref,
    stats_ref,
    padded_ref,
):
    me = me_ref[0]
    width = own_ref.shape[1]
    squares = jnp.zeros((LENGTH, 1), jnp.float32)
    inner = jnp.zeros((LENGTH, width), jnp.float32)
    gating = jnp.zeros((LENGTH, width), jnp.float32)
    for offset in range(4):
        at = lax.rem(me + offset, 4)
        if offset == 0:
            piece = own_ref[...].astype(jnp.float32)
        elif offset == 1:
            piece = right_ref[...].astype(jnp.float32)
        elif offset == 3:
            piece = left_ref[...].astype(jnp.float32)
        else:
            piece = far_ref[...].astype(jnp.float32)
        squares = squares + jnp.sum(piece * piece, axis=1, keepdims=True)
        scaled = (piece * gain_ref[at]).astype(jnp.bfloat16)
        inner = inner + jnp.dot(scaled, inner_ref[at], preferred_element_type=jnp.float32)
        gating = gating + jnp.dot(scaled, gating_ref[at], preferred_element_type=jnp.float32)
    inverse = lax.rsqrt(squares / D + EPSILON)
    gated = (inner * inverse * jax.nn.sigmoid(gating * inverse)).astype(jnp.bfloat16)
    padded_ref[:LEAD, :] = jnp.zeros((LEAD, width), jnp.float32)
    padded_ref[LEAD:, :] = gated.astype(jnp.float32)
    shift = LEAD - CONV + 1

    def step(n):
        base = n * ROWS_CHUNK
        sums = jnp.zeros((ROWS_CHUNK, 128), jnp.float32)
        square_sums = jnp.zeros((ROWS_CHUNK, 128), jnp.float32)
        for lane in range(0, width, 128):
            total = jnp.zeros((ROWS_CHUNK, 128), jnp.float32)
            for s in range(8):
                part = None
                for j in range(LEAD // 8 + 1):
                    tap = 8 * j + s - shift
                    if tap < 0 or tap >= CONV:
                        continue
                    height = ROWS_CHUNK + (8 if s else 0)
                    term = (
                        padded_ref[pl.ds(base + 8 * j, height), lane : lane + 128]
                        * taps_ref[tap : tap + 1, lane : lane + 128]
                    )
                    part = term if part is None else part + term
                total = total + part[s : s + ROWS_CHUNK]
            out_ref[pl.ds(base, ROWS_CHUNK), lane : lane + 128] = total
            sums = sums + total
            square_sums = square_sums + total * total
        return sums, square_sums

    for n in range(LENGTH // 128):
        pair = [step(2 * n + h) for h in range(2)]
        sums = jnp.concatenate([pair[0][0], pair[1][0]], axis=0)
        square_sums = jnp.concatenate([pair[0][1], pair[1][1]], axis=0)
        stats_ref[0, n : n + 1, :] = jnp.sum(sums.T, axis=0, keepdims=True)
        stats_ref[1, n : n + 1, :] = jnp.sum(square_sums.T, axis=0, keepdims=True)


def token_path(me, own, left, right, far, gain, inner_weight, gating_weight, taps):
    rows, width = own.shape
    grid_spec = pltpu.PrefetchScalarGridSpec(
        num_scalar_prefetch=1,
        grid=(rows // LENGTH,),
        in_specs=[pl.BlockSpec((LENGTH, width), lambda i, m: (i, 0))] * 4
        + [
            whole((4, 1, width)),
            whole((4, width, width)),
            whole((4, width, width)),
            whole((CONV, width)),
        ],
        out_specs=[
            pl.BlockSpec((LENGTH, width), lambda i, m: (i, 0)),
            pl.BlockSpec((None, 2, LENGTH // 128, 128), lambda i, m: (i, 0, 0, 0)),
        ],
        scratch_shapes=[pltpu.VMEM((LEAD + LENGTH, width), jnp.float32)],
    )
    return pl.pallas_call(
        token_kernel,
        grid_spec=grid_spec,
        out_shape=[
            pltpu.HBM((rows, width), jnp.float32),
            jax.ShapeDtypeStruct((rows // LENGTH, 2, LENGTH // 128, 128), jnp.float32),
        ],
        cost_estimate=pl.CostEstimate(
            flops=4 * rows * D * width, transcendentals=rows * width, bytes_accessed=10 << 20
        ),
        compiler_params=pltpu.CompilerParams(vmem_limit_bytes=40 << 20),
        name="token_path",
    )(
        me,
        *in_hbm(
            own,
            left,
            right,
            far,
            gain.reshape(4, 1, width),
            inner_weight.reshape(4, width, width),
            gating_weight.reshape(4, width, width),
            taps,
        ),
    )


def finish_kernel(conv_ref, stats_ref, gain_ref, out_ref):
    width = conv_ref.shape[1]
    turn = pl.program_id(0)
    for n in range(conv_ref.shape[0] // 128):
        at = turn * (conv_ref.shape[0] // 128) + n
        rows = slice(n * 128, (n + 1) * 128)
        average = stats_ref[0, pl.ds(at, 1), :] / D
        variance = stats_ref[1, pl.ds(at, 1), :] / D - average * average
        spread = lax.rsqrt(variance + EPSILON_NORM)
        average = jnp.broadcast_to(average, (128, 128)).T
        spread = jnp.broadcast_to(spread, (128, 128)).T
        for lane in range(0, width, 128):
            part = slice(lane, lane + 128)
            scaled = (conv_ref[rows, part] - average) * spread * gain_ref[:, part]
            out_ref[rows, part] = scaled * jax.nn.sigmoid(scaled)


def finish(convolved, stats, channel_gain):
    rows, width = convolved.shape
    tile = 512
    return pl.pallas_call(
        finish_kernel,
        grid=(rows // tile,),
        in_specs=[
            pl.BlockSpec((tile, width), lambda i: (i, 0)),
            whole((2, rows // 128, 128)),
            whole((1, width)),
        ],
        out_specs=pl.BlockSpec((tile, width), lambda i: (i, 0)),
        out_shape=pltpu.VMEM((rows, width), jnp.float32),
        cost_estimate=pl.CostEstimate(
            flops=8 * rows * width, transcendentals=rows * width, bytes_accessed=4 << 20
        ),
        compiler_params=pltpu.CompilerParams(vmem_limit_bytes=14 << 20),
        name="finish",
    )(*in_hbm(convolved), stats, channel_gain.reshape(1, width))


def attend_kernel(plane_ref, where_ref, conv_ref, gate_ref, *refs):
    near_ref, far_ref, upper_ref, lower_ref, out_ref, held_ref, sems = refs
    turn = pl.program_id(0)
    count = where_ref.shape[0]
    here = plane_ref[0]
    half = PROWS // 2

    @pl.when(turn == 0)
    def _():
        for n in range(count):
            owner = where_ref[n]
            away = lax.rem(owner // 8 - here + 8, 8)
            column = lax.rem(owner, 8)
            close = (away <= 1) | (away == 7)

            @pl.when(close)
            def _():
                k = jnp.where(away == 7, 1, 2 * away)
                at = pl.multiple_of(k * PROWS, PROWS)
                pltpu.make_async_copy(
                    near_ref.at[column, pl.ds(at, PROWS)], held_ref.at[n], sems.at[n]
                ).start()

            @pl.when(away == 4)
            def _():
                pltpu.make_async_copy(
                    upper_ref.at[column, pl.ds(0, half)],
                    held_ref.at[n, pl.ds(0, half)],
                    sems.at[n],
                ).start()
                pltpu.make_async_copy(
                    lower_ref.at[column, pl.ds(0, half)],
                    held_ref.at[n, pl.ds(half, half)],
                    sems.at[n],
                ).start()

            @pl.when((away == 2) | (away == 6))
            def _():
                at = pl.multiple_of(jnp.where(away == 2, PROWS, 0), PROWS)
                pltpu.make_async_copy(
                    far_ref.at[column, pl.ds(at, PROWS)], held_ref.at[n], sems.at[n]
                ).start()

            for side, at, rest_ref in (
                (5, 2 * PROWS, upper_ref),
                (3, 2 * PROWS + KEPT, lower_ref),
            ):

                @pl.when(away == side)
                def _():
                    pltpu.make_async_copy(
                        far_ref.at[column, pl.ds(at, KEPT)],
                        held_ref.at[n, pl.ds(0, KEPT)],
                        sems.at[n],
                    ).start()
                    pltpu.make_async_copy(
                        rest_ref.at[column, pl.ds(half, PROWS - KEPT)],
                        held_ref.at[n, pl.ds(KEPT, PROWS - KEPT)],
                        sems.at[n],
                    ).start()

    blocks = conv_ref.shape[0] // BLOCK
    weight = jax.nn.sigmoid(gate_ref[...])
    queries = conv_ref[...].astype(jnp.bfloat16)
    for n in range(blocks * PB):
        at = turn * blocks * PB + n
        pltpu.make_async_copy(
            far_ref.at[0, pl.ds(0, PROWS)], held_ref.at[at], sems.at[at]
        ).wait()
    scores = []
    for b in range(blocks):
        held = held_ref[pl.ds((turn * blocks + b) * PB, PB)].reshape(PB * PROWS, 2 * HEAD)
        rows = slice(b * BLOCK, (b + 1) * BLOCK)
        heads = jnp.concatenate([queries[rows, :HEAD], queries[rows, HEAD:]], axis=0)
        scores.append(
            lax.dot_general(
                heads,
                held[:, :HEAD],
                (((1,), (1,)), ((), ())),
                preferred_element_type=jnp.float32,
            )
            / math.sqrt(HEAD)
        )
    shares = []
    for b in range(blocks):
        raised = jnp.exp(scores[b] - jnp.max(scores[b], axis=1, keepdims=True))
        shares.append((raised / jnp.sum(raised, axis=1, keepdims=True)).astype(jnp.bfloat16))
    for b in range(blocks):
        held = held_ref[pl.ds((turn * blocks + b) * PB, PB)].reshape(PB * PROWS, 2 * HEAD)
        attended = jnp.dot(shares[b], held[:, HEAD:], preferred_element_type=jnp.float32)
        attended = jnp.concatenate([attended[:BLOCK], attended[BLOCK:]], axis=1)
        rows = slice(b * BLOCK, (b + 1) * BLOCK)
        out_ref[rows, :] = (conv_ref[rows, :] + weight * attended).astype(jnp.bfloat16)


def attend(plane, where, conv_out, retrieval_gate, groups):
    rows, width = conv_out.shape
    count = where.shape[0]
    tile = rows
    grid_spec = pltpu.PrefetchScalarGridSpec(
        num_scalar_prefetch=2,
        grid=(rows // tile,),
        in_specs=[
            pl.BlockSpec((tile, width), lambda i, *_: (i, 0)),
            whole((1, width)),
        ]
        + [pl.BlockSpec(memory_space=pl.ANY)] * len(groups),
        out_specs=pl.BlockSpec((tile, width), lambda i, *_: (i, 0)),
        scratch_shapes=[
            pltpu.VMEM((count, PROWS, 2 * HEAD), jnp.bfloat16),
            pltpu.SemaphoreType.DMA((count,)),
        ],
    )
    return pl.pallas_call(
        attend_kernel,
        grid_spec=grid_spec,
        out_shape=jax.ShapeDtypeStruct((rows, width), jnp.bfloat16),
        cost_estimate=pl.CostEstimate(
            flops=4 * rows * 2 * PB * PROWS * HEAD,
            transcendentals=rows * 2 * PB * PROWS,
            bytes_accessed=5 << 20,
        ),
        compiler_params=pltpu.CompilerParams(vmem_limit_bytes=16 << 20),
        name="attend",
    )(plane, where, *in_vmem(conv_out), retrieval_gate.reshape(1, width), *in_hbm(*groups[:2]), *in_vmem(*groups[2:]))


def pick_kernel(plane_ref, table_ref, *refs):
    (own, below, above), refs = (refs[0:2], refs[2:4], refs[4:6]), refs[6:]
    outs, sems = refs[:-1], refs[-1]
    here = plane_ref[0]
    half = PROWS // 2

    def slot(reader_plane, reader, owner_plane):
        at = lax.rem(here + reader_plane + 8, 8) * 8 + reader
        return table_ref[at, lax.rem(here + owner_plane + 8, 8)]

    def send(sources, taken, first, rows, target, n):
        size = sources[0].shape[0]
        for part, source in enumerate(sources):

            @pl.when((taken < size) if part == 0 else (taken >= size))
            def _():
                pltpu.make_async_copy(
                    source.at[taken - part * size, pl.ds(first, rows)], target, sems.at[n]
                ).start()

    for reader in range(8):
        for n, (source, side, steps, rows) in enumerate(
            (
                (below, 1, 1, PROWS),
                (above, -1, 1, PROWS),
                (below, 1, 2, KEPT),
                (above, -1, 2, KEPT),
            )
        ):
            taken = slot(side * steps, reader, -side)
            send(source, taken, 0, rows, outs[1 + n].at[reader], 1 + n)
    for reader in range(8):
        at = 0
        for source, reader_plane, owner_plane, first, rows in (
            (own, 0, 0, 0, PROWS),
            (below, 0, -1, 0, PROWS),
            (above, 0, 1, 0, PROWS),
            (below, 3, -1, 0, half),
            (own, 3, 0, KEPT, PROWS - KEPT),
            (above, -3, 1, half, half),
            (own, -3, 0, KEPT, PROWS - KEPT),
        ):
            taken = slot(reader_plane, reader, owner_plane)
            send(source, taken, first, rows, outs[0].at[reader, pl.ds(at, rows)], 0)
            at += rows
    for n, out in enumerate(outs):
        pltpu.make_async_copy(out, out, sems.at[n]).wait()


def pick(plane, table, *sources):
    shapes = [(8, NEAR_ROWS), (8, PROWS), (8, PROWS), (8, KEPT), (8, KEPT)]
    return pl.pallas_call(
        pick_kernel,
        in_specs=[pl.BlockSpec(memory_space=pltpu.SMEM)] * 2
        + [pl.BlockSpec(memory_space=pl.ANY)] * len(sources),
        out_specs=[pl.BlockSpec(memory_space=pl.ANY)] * len(shapes),
        scratch_shapes=[pltpu.SemaphoreType.DMA((len(shapes),))],
        out_shape=[pltpu.HBM((*shape, 2 * HEAD), jnp.bfloat16) for shape in shapes],
        cost_estimate=pl.CostEstimate(flops=0, transcendentals=0, bytes_accessed=8 << 20),
        compiler_params=pltpu.CompilerParams(vmem_limit_bytes=2 << 20),
        name="pick",
    )(plane, table, *in_vmem(*sources))


def fill_kernel(*refs, at):
    first_ref, second_ref = refs[:2]
    out_ref, stores = refs[-2:]
    rows = first_ref.shape[1]
    copies = [
        pltpu.make_async_copy(ref, out_ref.at[:, pl.ds(at + n * rows, rows)], stores.at[n])
        for n, ref in enumerate((first_ref, second_ref))
    ]
    for copy in copies:
        copy.start()
    for copy in copies:
        copy.wait()


def staged_fill_kernel(first_ref, second_ref, into_ref, out_ref, held_ref, loads, stores, *, at):
    del into_ref
    size, rows, _ = first_ref.shape
    count = size // 2
    parts = [(n, h) for h in range(2) for n in range(2)]

    def load(n, h):
        source = (first_ref, second_ref)[n].at[pl.ds(h * count, count)]
        return pltpu.make_async_copy(source, held_ref.at[n, h], loads.at[n, h])

    def store(n, h):
        target = out_ref.at[pl.ds(h * count, count), pl.ds(at + n * rows, rows)]
        return pltpu.make_async_copy(held_ref.at[n, h], target, stores.at[n, h])

    for part in parts:
        load(*part).start()
    for part in parts:
        load(*part).wait()
        store(*part).start()
    for part in parts:
        store(*part).wait()


def fill(first, second, at, into=None):
    size, rows, width = first.shape
    if into is None:
        kernel, held = fill_kernel, in_vmem(first, second)
        scratch = [pltpu.SemaphoreType.DMA((2,))]
    else:
        kernel, held = staged_fill_kernel, in_hbm(first, second, into)
        scratch = [pltpu.VMEM((2, 2, size // 2, rows, width), first.dtype)] + [
            pltpu.SemaphoreType.DMA((2, 2))
        ] * 2
    return pl.pallas_call(
        functools.partial(kernel, at=at),
        in_specs=[pl.BlockSpec(memory_space=pl.ANY)] * len(held),
        out_specs=pl.BlockSpec(memory_space=pl.ANY),
        scratch_shapes=scratch,
        out_shape=pltpu.HBM((size, AWAY_ROWS, width), first.dtype),
        input_output_aliases={} if into is None else {2: 0},
        cost_estimate=pl.CostEstimate(flops=0, transcendentals=0, bytes_accessed=2 << 20),
        compiler_params=pltpu.CompilerParams(vmem_limit_bytes=4 << 20),
        name="fill",
    )(*held)


def shift(value, axis, step):
    return lax.ppermute(value, axis, ring(lax.axis_size(axis), step))


def exchange(value, axes):
    return lax.all_to_all(value, axes, split_axis=0, concat_axis=0, tiled=True)


def layer(
    tokens,
    token_gain,
    inner_weight,
    gating_weight,
    filter_taps,
    channel_gain,
    retrieval_gate,
    passage_store,
    passage_gain,
    keys_weight,
    values_weight,
    owners,
    local_slots,
):
    me = lax.axis_index("tp").astype(jnp.int32).reshape(1)
    plane = lax.axis_index("z").astype(jnp.int32).reshape(1)
    left = shift(tokens, "tp", 1)
    right = shift(tokens, "tp", -1)
    far = shift(tokens, "tp", 2)

    sources = [[], [], []]
    for part in range(2):
        own = project_passages(
            passage_store, passage_gain, keys_weight, values_weight, part
        )
        own = own.reshape(-1, PROWS, 2 * HEAD)
        sources[0].append(own)
        sources[1].append(shift(own, "z", 1))
        sources[2].append(shift(own, "z", -1))

    asked = owners.reshape(-1)
    slots = local_slots.reshape(-1)
    wanted = jnp.sum(
        jnp.where(asked[:, None] == jnp.arange(64, dtype=jnp.int32)[None, :], slots[:, None], 0),
        axis=0,
    )
    wanted = jnp.broadcast_to(wanted.reshape(1, 8, 8).transpose(0, 2, 1), (8, 8, 8))
    table = exchange(wanted.reshape(64, 8), ST)

    near, up1, down1, up2, down2 = pick(plane, table, *sum(sources, []))
    side = ("y", "c")
    near = exchange(near, side)
    up1 = shift(up1, "z", 1)
    down1 = shift(down1, "z", -1)
    up2 = shift(up2, "z", 2)
    down2 = shift(down2, "z", -2)
    away = fill(up1, down1, 0)
    away = fill(up2, down2, 2 * PROWS, away)
    away = exchange(away, side)
    split = (3 * PROWS + NEAR_ROWS) // 2
    upper = shift(near[:, 3 * PROWS : split], "z", 3)
    lower = shift(near[:, split:], "z", -3)

    convolved, stats = token_path(
        me,
        tokens,
        left,
        right,
        far,
        token_gain,
        inner_weight,
        gating_weight,
        filter_taps,
    )
    stats = lax.psum(stats, "tp")
    stats = stats.transpose(1, 0, 2, 3).reshape(2, -1, 128)
    conv_out = finish(convolved, stats, channel_gain)
    return attend(plane, asked, conv_out, retrieval_gate, (near, away, upper, lower))


def solution(mesh):
    st, tp = mesh.devices.shape
    fine = Mesh(mesh.devices.reshape(st // 8, 4, 2, tp), ST + ("tp",))
    placed = (
        P(ST, "tp"),
        P(),
        P(None, "tp"),
        P(None, "tp"),
        P(None, "tp"),
        P("tp"),
        P("tp"),
        P(ST, None, None),
        P(),
        P(None, "tp"),
        P(None, "tp"),
        P(ST, None),
        P(ST, None),
    )
    return jax.shard_map(layer, mesh=fine, in_specs=placed, out_specs=P(ST, "tp"), check_vma=False)
```
